256 devices in a mesh: ep: 64 (over z, y, core), tp: 4 (over x).
Axes of the slice: x: 4, y: 4, z: 8, core: 2. Of those that a mesh axis runs over, the one named last changes fastest.
Arguments:
- tokens: bfloat16 [1024, 2048], P('ep'), may hold values from -6 to 6
- norm_gain: bfloat16 [2048], replicated, may hold values from 0.099609375 to 1.8984375
- query_weight: bfloat16 [2048, 1024], P('ep', 'tp'), may hold values from -0.125 to 0.125
- key_weight: bfloat16 [2048, 1024], P('ep', 'tp'), may hold values from -0.125 to 0.125
- value_weight: bfloat16 [2048, 2048], P('ep', 'tp'), may hold values from -0.125 to 0.125
- outgate_weight: bfloat16 [2048, 2048], P('ep', 'tp'), may hold values from -0.125 to 0.125
- beta_weight: bfloat16 [2048, 16], replicated, may hold values from -0.125 to 0.125
- decay_weight: bfloat16 [2048, 16], replicated, may hold values from -0.125 to 0.125
- decay_rate: float32 [16], P('tp'), may hold values from 0.02 to 6
- decay_bias: float32 [16], P('tp'), may hold values from -3 to 3
- head_gain: bfloat16 [128], replicated, may hold values from 0.099609375 to 1.8984375
- recurrent: float32 [1024, 16, 128, 128], P('ep', 'tp'), may hold values from -3 to 3
- output_weight: bfloat16 [2048, 2048], P('tp', 'ep'), may hold values from -0.125 to 0.125
- ffn_gain: bfloat16 [2048], replicated, may hold values from 0.099609375 to 1.8984375
- routes: int32 [1024, 4], P('ep'), may hold values from 0 to 63, all different within a row; in each aligned block of 16 rows (0 to 15, 16 to 31, ...) at most 2 rows name the same one
- route_weight: float32 [1024, 4], P('ep'), may hold values from 0.1 to 1
- expert_gate: bfloat16 [64, 2048, 512], P('ep', None, 'tp'), may hold values from -0.125 to 0.125
- expert_up: bfloat16 [64, 2048, 512], P('ep', None, 'tp'), may hold values from -0.125 to 0.125
- expert_down: bfloat16 [64, 512, 2048], P('ep', 'tp'), may hold values from -0.25 to 0.25
- shared_gate: bfloat16 [2048, 512], P('ep', 'tp'), may hold values from -0.125 to 0.125
- shared_up: bfloat16 [2048, 512], P('ep', 'tp'), may hold values from -0.125 to 0.125
- shared_down: bfloat16 [512, 2048], P('tp', 'ep'), may hold values from -0.25 to 0.25
- branch_gate: bfloat16 [2048], replicated, may hold values from -0.125 to 0.125
Outputs:
- layer_out: bfloat16 [1024, 2048], P('ep')
- new_state: float32 [1024, 16, 128, 128], P('ep', 'tp')
The draws below stay inside these ranges and needn't reach their ends.
Inputs may be any that keep to these rules, and one draw needn't show every extreme that they name: `routes`: each row names 4 different experts. Among the rows of one aligned block of 16 rows no expert is named more than 2 times, and some block reaches it: one expert is named exactly 2 times there.
All inputs are finite; a program needn't handle non-finite values.
Results may differ from the reference program's by a relative error of at most 0.019.
Values may be sent and summed in bfloat16 or wider, within the bound.
A program may use at most 64 MiB of HBM per device.

```python
import math
import jax
import jax.numpy as jnp
import numpy as np
from jax import lax

D = 2048
DK = 128
DV = 128
HK = 8
HV = 16
D_EXPERT = 512
D_SHARED = 512
TOPK = 4
SEQ_DEV = 16
SEQS = 1024
EXPERTS = 64
CAP = 2
N_EP = 64
N_TP = 4


def levels(stream_key, dims, shards, smallest, high):
    def one(position, blocks):
        draws = jax.random.uniform(jax.random.fold_in(jax.random.fold_in(stream_key, 6), position), (blocks,), jnp.float32, smallest / len(shards), high / len(shards))
        return jnp.repeat(jnp.exp(draws), dims[position] // blocks).reshape((-1,) + (1,) * (len(dims) - position - 1))

    level = one(*shards[0])
    for cut in shards[1:]:
        level = level * one(*cut)
    return level


def routed_block(stream_key, own, number, rows, number_of, top, most, slope):
    sequence = jax.random.permutation(stream_key, number_of)
    heavy_load, ordinary = shares(number_of, rows * top, most, slope, True), shares(number_of, rows * top, most, slope, False)
    places = jnp.arange(number_of)

    def named(sizes, turn):
        used = int((sizes > 0).sum())
        fixed = max(1, used // 4)
        shifted = fixed + (places - fixed + turn * (used - fixed)) % max(1, number_of - fixed)
        return jnp.zeros((number_of,), jnp.int32).at[sequence[jnp.where(places < fixed, places, shifted)]].set(jnp.asarray(sizes, jnp.int32))

    sizes = jnp.where(number % 4 == 0, named(heavy_load, number // 4), named(ordinary, number - number // 4 - 1))
    mixed = jax.random.permutation(jax.random.fold_in(own, 3), number_of)
    source_of, taker = mixed[0:number_of // 2 * 2:2], mixed[1:number_of // 2 * 2:2]
    margin = jnp.minimum(sizes[source_of] - 1, most - sizes[taker]) // 2
    margin = jnp.where((source_of == sequence[0]) | (taker == sequence[0]) | (sizes[taker] == 0), 0, jnp.maximum(margin, 0))
    shifted = jax.random.randint(jax.random.fold_in(own, 4), (number_of // 2,), 0, 1 << 20) % (margin + 1)
    sizes = sizes.at[source_of].add(-shifted).at[taker].add(shifted)
    items = jnp.searchsorted(jnp.cumsum(sizes), jnp.arange(rows * top), side="right").astype(jnp.int32)
    table = items.reshape(top, rows).T
    table = table[jax.random.permutation(jax.random.fold_in(own, 1), rows)]
    turn = jax.random.randint(jax.random.fold_in(own, 2), (rows, 1), 0, top)
    return jnp.take_along_axis(table, (jnp.arange(top)[None, :] + turn) % top, axis=1)


def shares(count, total, most, lean, full):
    loads = [(1 << 20) // math.isqrt(standing ** lean) + 1 for standing in range(1, count + 1)]
    largest = most if full else min(most, max(-(-total // count), total * loads[0] // sum(loads)))
    least = 1 if total - largest >= count - 1 else 0
    given, rest = [largest] + [least] * (count - 1), total - largest - least * (count - 1)
    while rest > 0:
        free = [i for i in range(1, count) if given[i] < largest] or [i for i in range(1, count) if given[i] < most]
        pool, left = sum([loads[i] for i in free]), rest
        for i in free:
            extra = min(most - given[i], max(1, left * loads[i] // pool), rest)
            given[i] = given[i] + extra
            rest = rest - extra
    return np.array(given)


def noise(stream_key, extent, deviation, reach, pieces=(), held_as=jnp.bfloat16):
    values = jax.random.normal(stream_key, extent, jnp.float32) * deviation
    if len(pieces) > 0:
        values = levels(stream_key, extent, pieces, -0.22, 0.18) * values
    return jnp.clip(values, min=-reach, max=reach).astype(held_as)


def setup_inputs(seed: int = 0) -> dict:
    key_of = jax.random.split(jax.random.key(seed), 24)
    tokens = noise(key_of[0], (SEQS, D), 1.0, 6.0, ((0, 64),))
    norm_gain = jnp.clip(1.0 + 0.18 * jax.random.normal(key_of[1], (D,), jnp.float32), 0.099609375, 1.8984375).astype(jnp.bfloat16)
    query_weight = noise(key_of[2], (D, HK * DK), D ** -0.5, 0.125, ((0, 64), (1, 4)))
    key_weight = noise(key_of[3], (D, HK * DK), D ** -0.5, 0.125, ((0, 64), (1, 4)))
    value_weight = noise(key_of[4], (D, HV * DV), D ** -0.5, 0.125, ((0, 64), (1, 4)))
    outgate_weight = noise(key_of[5], (D, HV * DV), D ** -0.5, 0.125, ((0, 64), (1, 4)))
    beta_weight = noise(key_of[6], (D, HV), D ** -0.5, 0.125)
    decay_weight = noise(key_of[7], (D, HV), D ** -0.5, 0.125)
    decay_rate = jnp.clip(jnp.exp(math.log(6.0) - 5.7037825 * jax.random.uniform(key_of[8], (HV,), jnp.float32) ** levels(key_of[8], (HV,), ((0, 4),), -0.2, 0.2)), 0.02, 6.0)
    decay_bias = noise(key_of[9], (HV,), 1.0, 3.0, ((0, 4),), jnp.float32)
    head_gain = jnp.clip(1.0 + 0.18 * jax.random.normal(key_of[10], (DV,), jnp.float32), 0.099609375, 1.8984375).astype(jnp.bfloat16)
    recurrent = noise(key_of[11], (SEQS, HV, DK, DV), 0.5, 3.0, ((0, 64), (1, 4)), jnp.float32)
    output_weight = noise(key_of[12], (HV * DV, D), (HV * DV) ** -0.5, 0.125, ((0, 4), (1, 64)))
    ffn_gain = jnp.clip(1.0 + 0.18 * jax.random.normal(key_of[13], (D,), jnp.float32), 0.099609375, 1.8984375).astype(jnp.bfloat16)
    routes_keys = jax.random.split(jax.random.fold_in(key_of[14], 1), SEQS // SEQ_DEV)
    routes_turns = jax.random.permutation(jax.random.fold_in(key_of[14], 3), SEQS // SEQ_DEV)
    routes = jax.vmap(lambda own, number: routed_block(jax.random.fold_in(key_of[14], 2), own, number, SEQ_DEV, EXPERTS, TOPK, CAP, 2))(routes_keys, routes_turns).reshape((SEQS, TOPK))
    route_weight = jnp.clip(jnp.exp(math.log(1.0) - 2.3025851 * jax.random.uniform(key_of[15], (SEQS, TOPK), jnp.float32) ** levels(key_of[15], (SEQS, TOPK), ((0, 64),), -0.2, 0.2)), 0.1, 1.0)
    expert_gate = noise(key_of[16], (EXPERTS, D, D_EXPERT), D ** -0.5, 0.125, ((0, 64), (2, 4)))
    expert_up = noise(key_of[17], (EXPERTS, D, D_EXPERT), D ** -0.5, 0.125, ((0, 64), (2, 4)))
    expert_down = noise(key_of[18], (EXPERTS, D_EXPERT, D), D_EXPERT ** -0.5, 0.25, ((0, 64), (1, 4)))
    shared_gate = noise(key_of[19], (D, D_SHARED), D ** -0.5, 0.125, ((0, 64), (1, 4)))
    shared_up = noise(key_of[20], (D, D_SHARED), D ** -0.5, 0.125, ((0, 64), (1, 4)))
    shared_down = noise(key_of[21], (D_SHARED, D), D_SHARED ** -0.5, 0.25, ((0, 4), (1, 64)))
    branch_gate = noise(key_of[22], (D,), D ** -0.5, 0.125)
    return dict(tokens=tokens, norm_gain=norm_gain, query_weight=query_weight, key_weight=key_weight, value_weight=value_weight, outgate_weight=outgate_weight, beta_weight=beta_weight, decay_weight=decay_weight, decay_rate=decay_rate, decay_bias=decay_bias, head_gain=head_gain, recurrent=recurrent, output_weight=output_weight, ffn_gain=ffn_gain, routes=routes, route_weight=route_weight, expert_gate=expert_gate, expert_up=expert_up, expert_down=expert_down, shared_gate=shared_gate, shared_up=shared_up, shared_down=shared_down, branch_gate=branch_gate)


EPS = 1e-06
ROUTED_SCALE = 2.5

def rms_scale(values, gain):
    values = values.astype(jnp.float32)
    return values * lax.rsqrt(lax.optimization_barrier(jnp.mean(values * values, axis=-1, keepdims=True)) + EPS) * gain.astype(jnp.float32)

def unit_rows(values):
    return values * lax.rsqrt(lax.optimization_barrier(jnp.sum(values * values, axis=-1, keepdims=True)) + EPS)

def grouped_product(left, right, groups):
    inner = left.shape[1] // groups
    running = jnp.zeros((left.shape[0], right.shape[1]), jnp.float32)
    for index in range(groups):
        partial_product = jnp.dot(left[:, index * inner:(index + 1) * inner], right[index * inner:(index + 1) * inner], preferred_element_type=jnp.float32)
        running = running + partial_product.astype(jnp.bfloat16).astype(jnp.float32)
    return running

def reference(tokens, norm_gain, query_weight, key_weight, value_weight, outgate_weight, beta_weight, decay_weight, decay_rate, decay_bias, head_gain, recurrent, output_weight, ffn_gain, routes, route_weight, expert_gate, expert_up, expert_down, shared_gate, shared_up, shared_down, branch_gate):
    seqs, width = tokens.shape
    heads, key_dim, value_dim = (recurrent.shape[1], recurrent.shape[2], recurrent.shape[3])
    key_heads = query_weight.shape[1] // key_dim
    normed = rms_scale(tokens, norm_gain).astype(jnp.bfloat16)
    query_proj = jnp.dot(normed, query_weight, preferred_element_type=jnp.float32).astype(jnp.bfloat16)
    key_proj = jnp.dot(normed, key_weight, preferred_element_type=jnp.float32).astype(jnp.bfloat16)
    value_proj = jnp.dot(normed, value_weight, preferred_element_type=jnp.float32).astype(jnp.bfloat16)
    gate_proj = jnp.dot(normed, outgate_weight, preferred_element_type=jnp.float32).astype(jnp.bfloat16)
    beta_logit = jnp.dot(normed, beta_weight, preferred_element_type=jnp.float32)
    decay_logit = jnp.dot(normed, decay_weight, preferred_element_type=jnp.float32)
    repeat_count = heads // key_heads
    queries = unit_rows(jax.nn.silu(query_proj.astype(jnp.float32)).reshape(seqs, key_heads, key_dim))
    queries = jnp.repeat(queries, repeat_count, axis=1) * key_dim ** (-0.5)
    key_rows = unit_rows(jax.nn.silu(key_proj.astype(jnp.float32)).reshape(seqs, key_heads, key_dim))
    key_rows = jnp.repeat(key_rows, repeat_count, axis=1)
    value_rows = jax.nn.silu(value_proj.astype(jnp.float32)).reshape(seqs, heads, value_dim)
    strength = jax.nn.sigmoid(beta_logit)
    retain = jnp.exp(-decay_rate[None, :] * jax.nn.softplus(decay_logit + decay_bias[None, :]))
    decayed = recurrent * retain[:, :, None, None]
    predicted = jnp.einsum('shde,shd->she', decayed, key_rows, precision=lax.Precision.HIGHEST)
    correction = strength[:, :, None] * (value_rows - predicted)
    new_state = decayed + key_rows[:, :, :, None] * correction[:, :, None, :]
    readout = jnp.einsum('shde,shd->she', new_state, queries, precision=lax.Precision.HIGHEST)
    out_gate = jax.nn.silu(gate_proj.astype(jnp.float32)).reshape(seqs, heads, value_dim)
    heads_out = (rms_scale(readout, head_gain) * out_gate).astype(jnp.bfloat16).reshape(seqs, heads * value_dim)
    mix = grouped_product(heads_out, output_weight, N_TP)
    residual = (tokens.astype(jnp.float32) + mix).astype(jnp.bfloat16)
    ffn_in = rms_scale(residual, ffn_gain).astype(jnp.bfloat16)
    topk = routes.shape[1]
    seq_local = seqs // N_EP
    experts_total = expert_gate.shape[0]
    pair_count = seq_local * topk
    pair_ids = routes.reshape(N_EP, pair_count).astype(jnp.int32)
    onehot = (pair_ids[:, :, None] == jnp.arange(experts_total).astype(jnp.int32)[None, None, :]).astype(jnp.int32)
    slots = lax.optimization_barrier(jnp.sum((jnp.cumsum(onehot, axis=1) - onehot) * onehot, axis=2)).astype(jnp.int32)
    target = (pair_ids * CAP + slots).astype(jnp.int32)
    source_rows = jnp.repeat(ffn_in.reshape(N_EP, seq_local, width), topk, axis=1)
    buffer = jnp.zeros((N_EP, experts_total * CAP, width), jnp.bfloat16)
    source_index = jnp.arange(N_EP).astype(jnp.int32)[:, None]
    buffer = buffer.at[source_index, target].set(source_rows)
    buffer = buffer.reshape(N_EP, experts_total, CAP, width).transpose(1, 0, 2, 3).reshape(experts_total, N_EP * CAP, width)

    def expert_rows(operands):
        rows_in, gate_matrix, up_matrix, down_matrix = operands
        gate_part = jnp.dot(rows_in, gate_matrix, preferred_element_type=jnp.float32)
        up_part = jnp.dot(rows_in, up_matrix, preferred_element_type=jnp.float32)
        act = (jax.nn.silu(gate_part) * up_part).astype(jnp.bfloat16)
        return grouped_product(act, down_matrix, N_TP).astype(jnp.bfloat16)
    results = lax.map(expert_rows, (buffer, expert_gate, expert_up, expert_down))
    results = results.reshape(experts_total, N_EP, CAP, width).transpose(1, 0, 2, 3).reshape(N_EP, experts_total * CAP, width)
    pair_out = jnp.take_along_axis(results, target[:, :, None], axis=1).astype(jnp.float32)
    scaled = route_weight / lax.optimization_barrier(jnp.sum(route_weight, axis=1, keepdims=True)) * ROUTED_SCALE
    moe = lax.optimization_barrier(jnp.sum(pair_out.reshape(seqs, topk, width) * scaled[:, :, None], axis=1))
    shared_g = jnp.dot(ffn_in, shared_gate, preferred_element_type=jnp.float32)
    shared_u = jnp.dot(ffn_in, shared_up, preferred_element_type=jnp.float32)
    shared_act = (jax.nn.silu(shared_g) * shared_u).astype(jnp.bfloat16)
    shared_out = grouped_product(shared_act, shared_down, N_TP)
    branch = jax.nn.sigmoid(jnp.dot(ffn_in, branch_gate, preferred_element_type=jnp.float32))
    layer_out = (residual.astype(jnp.float32) + moe + branch[:, None] * shared_out).astype(jnp.bfloat16)
    return (layer_out, new_state)
```

```python
import functools

import jax
import jax.numpy as jnp
from jax import lax
from jax.experimental import pallas as pl
from jax.experimental.pallas import tpu as pltpu
from jax.sharding import PartitionSpec as P

EPS = 1e-06
ROUTED_SCALE = 2.5
NZ, NY, NC = 8, 4, 2
MESH = pl.DeviceIdType.MESH
BF = jnp.bfloat16
F32 = jnp.float32


def silu(v):
    return v / (1.0 + jnp.exp(-v))


def sigmoid(v):
    return 1.0 / (1.0 + jnp.exp(-v))


def rms(values, gain):
    return (
        values
        * lax.rsqrt(jnp.mean(values * values, axis=-1, keepdims=True) + EPS)
        * gain
    )


def unit(v):
    return v * lax.rsqrt(jnp.sum(v * v, axis=-1, keepdims=True) + EPS)


def attn_kernel(
    tokens, norm_gain, wq, wk, wv, wg, bw, dw, rate, bias, head_gain, rec, ow, ffn_gain,
    residual_out, ffn_out, state_out,
    state, wbuf, tok_src, tokbuf, psend, prec, obuf, mix_send, mix_rec,
    kt, qt, vals, rs_ref, corr, ro,
    load_sem, w_s, w_r, wf_s, wf_r, t_s, t_r, p_s, p_r, o1_s, o1_r, o2_s, o2_r, o3_s, o3_r, m_s, m_r,
    st_sem,
):
    e = lax.axis_index("ep")
    x = lax.axis_index("tp")
    nx = lax.axis_size("tp")
    z, yc = e // (NY * NC), e % (NY * NC)
    y, c = yc // NC, yc % NC
    partner = e + 1 - 2 * c
    zdev = lambda d: ((z + d) % NZ) * (NY * NC) + yc
    ydev = lambda d: z * (NY * NC) + ((y + d) % NY) * NC + c

    def rcopy(src, dst, ss, rs, ep, tp):
        return pltpu.make_async_remote_copy(
            src_ref=src, dst_ref=dst, send_sem=ss, recv_sem=rs, device_id=(ep, tp), device_id_type=MESH
        )

    barrier = pltpu.get_barrier_semaphore()
    for d in range(1, NZ):
        pl.semaphore_signal(barrier, inc=1, device_id=(zdev(d), x), device_id_type=MESH)
    for d in range(1, NY):
        pl.semaphore_signal(barrier, inc=1, device_id=(ydev(d), x), device_id_type=MESH)
    pl.semaphore_signal(barrier, inc=1, device_id=(partner, x), device_id_type=MESH)
    for d in range(1, nx):
        pl.semaphore_signal(barrier, inc=1, device_id=(e, (x + d) % nx), device_id_type=MESH)

    loads = []
    at = 0
    for i, w in enumerate((wq, wk, wv, wg)):
        n = w.shape[1]
        loads.append(pltpu.make_async_copy(w, wbuf.at[yc, :, at : at + n], load_sem.at[i]))
        at += n
    for l in loads:
        l.start()
    load_state = pltpu.make_async_copy(rec, state, load_sem.at[4])
    load_state.start()

    normed = rms(tokens[...].astype(F32), norm_gain[...].astype(F32)).astype(BF)
    kz = tokbuf.shape[2]
    for i in range(NZ):
        tok_src[i] = normed[:, i * kz : (i + 1) * kz]
    n_own = ow.shape[1]
    eye = (
        lax.broadcasted_iota(jnp.int32, (n_own, n_own), 0)
        == lax.broadcasted_iota(jnp.int32, (n_own, n_own), 1)
    ).astype(BF)
    obuf[e] = lax.dot_general(
        eye, ow[...], (((1,), (1,)), ((), ())), preferred_element_type=F32
    ).astype(BF)
    for l in loads:
        l.wait()
    pl.semaphore_wait(barrier, (NZ - 1) + (NY - 1) + 1 + (nx - 1))

    toks = [
        rcopy(tok_src.at[(z + d) % NZ], tokbuf.at[d], t_s.at[d], t_r.at[d], zdev(d), x)
        for d in range(1, NZ)
    ]
    for cp in toks:
        cp.start()
    ws = [rcopy(wbuf.at[yc], wbuf.at[yc], w_s.at[d], w_r.at[d], ydev(d), x) for d in range(1, NY)]
    for cp in ws:
        cp.start()
    fwd = [rcopy(wbuf.at[yc], wbuf.at[yc], wf_s.at[0], wf_r.at[0], partner, x)]
    fwd[0].start()
    o1 = [rcopy(obuf.at[e], obuf.at[e], o1_s.at[d], o1_r.at[d], zdev(d), x) for d in range(1, NZ)]
    for cp in o1:
        cp.start()
    tokbuf[0] = tok_src[z]

    bl = jnp.dot(normed, bw[...], preferred_element_type=F32)
    dl = jnp.dot(normed, dw[...], preferred_element_type=F32)
    lanes = lax.broadcasted_iota(jnp.int32, bl.shape, 1)
    heads = rec.shape[1]
    retain, strength = [], []
    for h in range(heads):
        mine = lanes == x * heads + h
        b = jnp.sum(jnp.where(mine, bl, 0.0), axis=1, keepdims=True)
        g = jnp.sum(jnp.where(mine, dl, 0.0), axis=1, keepdims=True) + bias[0, h]
        soft = jnp.maximum(g, 0.0) + jnp.log1p(jnp.exp(-jnp.abs(g)))
        strength.append(sigmoid(b))
        retain.append(jnp.exp(-rate[0, h] * soft))
    lane = lax.broadcasted_iota(jnp.int32, rs_ref.shape, 1)
    packed = jnp.zeros(rs_ref.shape, F32)
    for h in range(heads):
        packed = jnp.where(lane == h, retain[h], packed)
        packed = jnp.where(lane == heads + h, strength[h], packed)

    for d in range(1, NY):
        ws[d - 1].wait_recv()
        j = ((y + NY - d) % NY) * NC + c
        cp = rcopy(wbuf.at[j], wbuf.at[j], wf_s.at[d], wf_r.at[d], partner, x)
        cp.start()
        fwd.append(cp)
    for cp in toks:
        cp.wait_recv()
    for cp in fwd:
        cp.wait_recv()
    cols = wbuf.shape[2]
    seqs = tokens.shape[0]
    partial = jnp.dot(
        tokbuf[...].reshape(NZ * seqs, kz), wbuf[...].reshape(kz, cols), preferred_element_type=F32
    ).astype(BF)
    psend[...] = partial.reshape(NZ, seqs, cols)
    sums = [
        rcopy(psend.at[d], prec.at[d], p_s.at[d], p_r.at[d], zdev(NZ - d), x) for d in range(1, NZ)
    ]
    for d in (4, 3, 5, 2, 6, 1, 7):
        sums[d - 1].start()

    o2, o3 = [], []
    for d in range(NZ):
        if d:
            o1[d - 1].wait_recv()
        j = ((z + NZ - d) % NZ) * (NY * NC) + yc
        for dy in range(1, NY):
            cp = rcopy(obuf.at[j], obuf.at[j], o2_s.at[dy, d], o2_r.at[dy, d], ydev(dy), x)
            cp.start()
            o2.append((dy, d, cp))
        cp = rcopy(obuf.at[j], obuf.at[j], o3_s.at[0, d], o3_r.at[0, d], partner, x)
        cp.start()
        o3.append(cp)

    for cp in sums:
        cp.wait_recv()
    total = psend[0].astype(F32)
    for d in range(1, NZ):
        total = total + prec[d].astype(F32)
    proj = total.astype(BF).astype(F32)

    for dy, d, cp in o2:
        cp.wait_recv()
        j = ((z + NZ - d) % NZ) * (NY * NC) + ((y + NY - dy) % NY) * NC + c
        f = rcopy(obuf.at[j], obuf.at[j], o3_s.at[dy, d], o3_r.at[dy, d], partner, x)
        f.start()
        o3.append(f)

    dk = rec.shape[2]
    dv = rec.shape[3]
    khs = wq.shape[1] // dk
    per = heads // khs
    qs, ks, kq = [], [], []
    for i in range(khs):
        q = unit(silu(proj[:, i * dk : (i + 1) * dk])) * dk ** (-0.5)
        k = unit(silu(proj[:, (khs + i) * dk : (khs + i + 1) * dk]))
        kt[i] = k.T
        qt[i] = q.T
        kq.append(jnp.sum(k * q, axis=1, keepdims=True))
    for i in range(khs):
        packed = jnp.where(lane == 2 * heads + i, kq[i], packed)
    rs_ref[...] = packed
    vbase = 2 * khs * dk
    for h in range(heads):
        vals[h] = silu(proj[:, vbase + h * dv : vbase + (h + 1) * dv])
    gate = proj[:, vbase + heads * dv :]
    load_state.wait()

    def column(ref, i, s):
        t = ref[i]
        pick = lax.broadcasted_iota(jnp.int32, t.shape, 1) == s
        return jnp.sum(jnp.where(pick, t, 0.0), axis=1, keepdims=True)

    def read_one(s, carry):
        rowrs = rs_ref[pl.ds(s, 1), :]
        for i in range(khs):
            kcol = column(kt, i, s)
            qcol = column(qt, i, s)
            dotkq = rowrs[:, 2 * heads + i : 2 * heads + i + 1]
            for h in range(i * per, (i + 1) * per):
                st = state[s, h]
                ret = rowrs[:, h : h + 1]
                pred = jnp.sum(st * kcol, axis=0, keepdims=True) * ret
                base = jnp.sum(st * qcol, axis=0, keepdims=True) * ret
                cor = rowrs[:, heads + h : heads + h + 1] * (
                    vals[h, pl.ds(s, 1), :] - pred
                )
                corr[h, pl.ds(s, 1), :] = cor
                ro[h, pl.ds(s, 1), :] = base + dotkq * cor
        return carry

    lax.fori_loop(0, seqs, read_one, 0)

    hg = head_gain[...].astype(F32)
    parts = []
    for h in range(heads):
        parts.append(
            rms(ro[h], hg) * silu(gate[:, h * dv : (h + 1) * dv])
        )
    heads_out = jnp.concatenate(parts, axis=1).astype(BF)
    for cp in o3:
        cp.wait_recv()
    width = tokens.shape[1]
    mix_send[...] = lax.dot_general(
        heads_out,
        obuf[...].reshape(width, heads * dv),
        (((1,), (1,)), ((), ())),
        preferred_element_type=F32,
    ).astype(BF)
    mixes = [
        rcopy(mix_send, mix_rec.at[d], m_s.at[d], m_r.at[d], e, (x + d) % nx) for d in range(1, nx)
    ]
    for cp in mixes:
        cp.start()

    def write_one(s, carry):
        rowrs = rs_ref[pl.ds(s, 1), :]
        for i in range(khs):
            kcol = column(kt, i, s)
            for h in range(i * per, (i + 1) * per):
                state[s, h] = state[s, h] * rowrs[:, h : h + 1] + kcol * corr[h, pl.ds(s, 1), :]
        return carry

    lax.fori_loop(0, seqs, write_one, 0)
    store_state = pltpu.make_async_copy(state, state_out, st_sem)
    store_state.start()

    mixed = mix_send[...].astype(F32)
    for d in range(1, nx):
        mixes[d - 1].wait_recv()
        mixed = mixed + mix_rec[d].astype(F32)
    residual = (tokens[...].astype(F32) + mixed).astype(BF)
    residual_out[...] = residual
    ffn_out[...] = rms(residual.astype(F32), ffn_gain[...].astype(F32)).astype(BF)

    for group in (toks, ws, o1, fwd, sums, [t[2] for t in o2], o3, mixes):
        for cp in group:
            cp.wait_send()
    store_state.wait()


def attention(tokens, norm_gain, wq, wk, wv, wg, bw, dw, rate, bias, head_gain, rec, ow, ffn_gain):
    nx = lax.axis_size("tp")
    seqs, width = tokens.shape
    heads, dk, dv = rec.shape[1:]
    cols = wq.shape[1] + wk.shape[1] + wv.shape[1] + wg.shape[1]
    rows = wq.shape[0]
    kz = rows * NY * NC
    vmem = pl.BlockSpec(memory_space=pltpu.VMEM)
    smem = pl.BlockSpec(memory_space=pltpu.SMEM)
    hbm = pl.BlockSpec(memory_space=pl.ANY)
    dma = pltpu.SemaphoreType.DMA
    ep = NZ * NY * NC
    khs = wq.shape[1] // dk
    return pl.pallas_call(
        attn_kernel,
        out_shape=(
            jax.ShapeDtypeStruct((seqs, width), BF),
            jax.ShapeDtypeStruct((seqs, width), BF),
            jax.ShapeDtypeStruct(rec.shape, F32),
        ),
        in_specs=[vmem, vmem, hbm, hbm, hbm, hbm, vmem, vmem, smem, smem, vmem, hbm, vmem, vmem],
        out_specs=(vmem, vmem, hbm),
        scratch_shapes=[
            pltpu.VMEM(rec.shape, F32),
            pltpu.VMEM((NY * NC, rows, cols), BF),
            pltpu.VMEM((NZ, seqs, kz), BF),
            pltpu.VMEM((NZ, seqs, kz), BF),
            pltpu.VMEM((NZ, seqs, cols), BF),
            pltpu.VMEM((NZ, seqs, cols), BF),
            pltpu.VMEM((ep, ow.shape[1], ow.shape[0]), BF),
            pltpu.VMEM((seqs, width), BF),
            pltpu.VMEM((nx, seqs, width), BF),
            pltpu.VMEM((khs, dk, seqs), F32),
            pltpu.VMEM((khs, dk, seqs), F32),
            pltpu.VMEM((heads, seqs, dv), F32),
            pltpu.VMEM((seqs, 128), F32),
            pltpu.VMEM((heads, seqs, dv), F32),
            pltpu.VMEM((heads, seqs, dv), F32),
            dma((5,)),
            dma((NY,)), dma((NY,)), dma((NY,)), dma((NY,)),
            dma((NZ,)), dma((NZ,)), dma((NZ,)), dma((NZ,)),
            dma((NZ,)), dma((NZ,)),
            dma((NY, NZ)), dma((NY, NZ)), dma((NY, NZ)), dma((NY, NZ)),
            dma((nx,)), dma((nx,)),
            dma,
        ],
        compiler_params=pltpu.CompilerParams(
            collective_id=1, has_side_effects=True, vmem_limit_bytes=40 * 1024 * 1024
        ),
        name="attention",
    )(
        tokens, norm_gain.reshape(1, -1), wq, wk, wv, wg, bw, dw, rate.reshape(1, -1), bias.reshape(1, -1),
        head_gain.reshape(1, -1), rec, ow, ffn_gain.reshape(1, -1),
    )


def side_by_side(arrays, axis, dim, along):
    both = jnp.concatenate(arrays, axis=along)
    whole, at, outs = (lax.all_gather(both, axis, axis=dim, tiled=True), 0, [])
    for a in arrays:
        outs.append(lax.slice_in_dim(whole, at, at + a.shape[along], axis=along))
        at += a.shape[along]
    return tuple(outs)


def copy_for_each(array, axis):
    copies = jnp.broadcast_to(array, (lax.axis_size(axis), *array.shape))
    return lax.all_to_all(copies, axis, split_axis=0, concat_axis=0, tiled=True)


def laid_out(pieces, dim):
    dims = list(pieces.shape[1:])
    dims[dim] *= pieces.shape[0]
    return jnp.moveaxis(pieces, 0, dim).reshape(dims)


def collect(array, axis, dim):
    pieces = copy_for_each(array, axis)
    return laid_out(pieces, dim)


def over_copies(array, axis):
    everything = copy_for_each(array, axis)
    return jnp.sum(everything.astype(jnp.float32), axis=0)


def in_blocks(array, dim, peers):
    dims = array.shape
    pieces = array.reshape(*dims[:dim], peers, dims[dim] // peers, *dims[dim + 1 :])
    return jnp.moveaxis(pieces, dim, 0)


def summed_on_arrival(array, axis, dim):
    pieces = in_blocks(array, dim, lax.axis_size(axis))
    arrived = lax.all_to_all(pieces, axis, split_axis=0, concat_axis=0, tiled=True)
    return arrived.astype(jnp.float32).sum(axis=0)


def rms_scale(values, gain):
    values = values.astype(jnp.float32)
    return (
        values
        * lax.rsqrt(jnp.mean(values * values, axis=-1, keepdims=True) + EPS)
        * gain.astype(jnp.float32)
    )


def per_device(
    tokens,
    norm_gain,
    query_weight,
    key_weight,
    value_weight,
    outgate_weight,
    beta_weight,
    decay_weight,
    decay_rate,
    decay_bias,
    head_gain,
    recurrent,
    output_weight,
    ffn_gain,
    routes,
    route_weight,
    expert_gate,
    expert_up,
    expert_down,
    shared_gate,
    shared_up,
    shared_down,
    branch_gate,
):
    ep_count = lax.axis_size("ep")
    tp_count = lax.axis_size("tp")
    seq_local, width = tokens.shape
    residual, ffn_in, new_state = attention(
        tokens, norm_gain, query_weight, key_weight, value_weight, outgate_weight, beta_weight,
        decay_weight, decay_rate, decay_bias, head_gain, recurrent, output_weight, ffn_gain,
    )
    pieces = side_by_side((shared_gate, shared_up), "ep", 0, 1)
    token_block = ffn_in
    shared_g = jnp.dot(token_block, pieces[0], preferred_element_type=jnp.float32)
    shared_u = jnp.dot(token_block, pieces[1], preferred_element_type=jnp.float32)
    shared_act = (jax.nn.silu(shared_g) * shared_u).astype(jnp.bfloat16)
    shared_partial = jnp.dot(
        shared_act, collect(shared_down, "ep", 1), preferred_element_type=jnp.float32
    )
    shared_out = over_copies(
        shared_partial.astype(jnp.bfloat16).astype(jnp.float32).astype(jnp.bfloat16), "tp"
    ).astype(jnp.float32)
    topk = routes.shape[1]
    pair_count = seq_local * topk
    capacity = 2 * ((pair_count + ep_count - 1) // ep_count)
    expert_ids = routes.reshape(pair_count)
    onehot = (expert_ids[:, None] == jnp.arange(ep_count)[None, :]).astype(jnp.float32)
    earlier = (jnp.arange(pair_count)[:, None] > jnp.arange(pair_count)[None, :]).astype(
        jnp.float32
    )
    slots = jnp.sum(jnp.dot(earlier, onehot) * onehot, axis=1).astype(jnp.int32)
    target = expert_ids * capacity + slots
    placement_matrix = (target[:, None] == jnp.arange(ep_count * capacity)[None, :]).astype(
        jnp.bfloat16
    )
    dispatch_matrix = jnp.sum(
        placement_matrix.reshape(seq_local, topk, ep_count * capacity).astype(jnp.float32), axis=1
    ).astype(jnp.bfloat16)
    outgoing = jnp.dot(dispatch_matrix.T, ffn_in, preferred_element_type=jnp.float32).astype(
        jnp.bfloat16
    )
    outgoing = outgoing.reshape(ep_count, capacity, width)
    share_cols = width // tp_count
    received = lax.all_to_all(outgoing, "ep", split_axis=0, concat_axis=0, tiled=True)
    flat_rows = received.reshape(-1, width)
    gate_part = jnp.dot(flat_rows, expert_gate[0], preferred_element_type=jnp.float32)
    up_part = jnp.dot(flat_rows, expert_up[0], preferred_element_type=jnp.float32)
    act = (jax.nn.silu(gate_part) * up_part).astype(jnp.bfloat16)
    partial_rows = (
        jnp.dot(act, expert_down[0], preferred_element_type=jnp.float32)
        .astype(jnp.bfloat16)
        .astype(jnp.float32)
    )
    part_cols = summed_on_arrival(partial_rows.astype(jnp.bfloat16), "tp", 1).astype(jnp.bfloat16)
    returned = lax.all_to_all(
        part_cols.reshape(received.shape[0], received.shape[1], share_cols),
        "ep",
        split_axis=0,
        concat_axis=0,
        tiled=True,
    )
    scaled = route_weight / jnp.sum(route_weight, axis=1, keepdims=True) * ROUTED_SCALE
    branch = jax.nn.sigmoid(jnp.dot(ffn_in, branch_gate, preferred_element_type=jnp.float32))
    col_begin = lax.axis_index("tp") * share_cols
    pair_out = jnp.dot(
        placement_matrix,
        returned.reshape(ep_count * capacity, share_cols),
        preferred_element_type=jnp.float32,
    )
    moe_cols = jnp.sum(pair_out.reshape(seq_local, topk, share_cols) * scaled[:, :, None], axis=1)
    resid_part = lax.dynamic_slice_in_dim(residual, col_begin, share_cols, 1).astype(jnp.float32)
    shared_part = lax.dynamic_slice_in_dim(shared_out, col_begin, share_cols, 1)
    out_cols = (resid_part + moe_cols + branch[:, None] * shared_part).astype(jnp.bfloat16)
    layer_out = collect(out_cols, "tp", 1)
    return (layer_out, new_state)


def solution(mesh):
    return jax.shard_map(
        per_device,
        mesh=mesh,
        in_specs=(
            P("ep", None),
            P(),
            P("ep", "tp"),
            P("ep", "tp"),
            P("ep", "tp"),
            P("ep", "tp"),
            P(),
            P(),
            P("tp"),
            P("tp"),
            P(),
            P("ep", "tp", None, None),
            P("tp", "ep"),
            P(),
            P("ep", None),
            P("ep", None),
            P("ep", None, "tp"),
            P("ep", None, "tp"),
            P("ep", "tp", None),
            P("ep", "tp"),
            P("ep", "tp"),
            P("tp", "ep"),
            P(),
        ),
        out_specs=(P("ep", None), P("ep", "tp", None, None)),
        check_vma=False,
    )
```

```python
import jax
import jax.numpy as jnp
from jax import lax
from jax.experimental import pallas as pl
from jax.experimental.pallas import tpu as pltpu
from jax.sharding import PartitionSpec as P

EPS = 1e-06
ROUTED_SCALE = 2.5
NZ, NY, NC = 8, 4, 2
YC = NY * NC
EP = NZ * YC
SLOTS = 2
LANES = 128
MESH = pl.DeviceIdType.MESH
BF = jnp.bfloat16
F32 = jnp.float32
I32 = jnp.int32


def silu(v):
    return v / (1.0 + jnp.exp(-v))


def sigmoid(v):
    return 1.0 / (1.0 + jnp.exp(-v))


def rms(values, gain):
    return values * lax.rsqrt(jnp.mean(values * values, axis=-1, keepdims=True) + EPS) * gain


def unit(v):
    return v * lax.rsqrt(jnp.sum(v * v, axis=-1, keepdims=True) + EPS)


def iota(shape, dim):
    return lax.broadcasted_iota(I32, shape, dim)


def nt_dot(a, b):
    return lax.dot_general(a, b, (((1,), (1,)), ((), ())), preferred_element_type=F32)


def layer_kernel(
    tokens_h, norm_gain_h, wq, wk, wv, wg, bw_h, dw_h, rate_h, bias_h, head_gain_h, rec, ow_h, ffn_gain_h,
    routes_h, rweight_h, eg_h, eu_h, ed_h, sg_h, su_h, sd_h, branch_h,
    out_ref, keys_out, corr_out, retain_out,
    tokens, norm_gain, bw, dw, rate, bias, head_gain, ffn_gain, routes, rweight, branch_gate,
    state, wbuf, tok_src, tokbuf, psend, prec, obuf, sbuf, mix_send, mix_rec,
    kt, qt, vals, rs_ref, ro,
    egu, dsrc, dbuf, chunks, res_chunks, dsend, xrows, rowsf, act_all, outf, rsend, rrecv, sh_send, sh_rec, fin,
    load_sem, w_s, w_r, wf_s, wf_r, t_s, t_r, p_s, p_r, o1_s, o1_r, o2_s, o2_r, o3_s, o3_r,
    s1_s, s1_r, s2_s, s2_r, s3_s, s3_r, m_s, m_r, ed_s, ed_r, d_s, d_r, x_s, x_r, a_s, a_r, r_s, r_r,
    h_s, h_r, f_s, f_r,
):
    e = lax.axis_index("ep")
    x = lax.axis_index("tp")
    nx = lax.axis_size("tp")
    z, yc = e // YC, e % YC
    y, c = yc // NC, yc % NC
    partner = e + 1 - 2 * c
    zdev = lambda d: ((z + d) % NZ) * YC + yc
    ydev = lambda d: z * YC + ((y + d) % NY) * NC + c
    xdev = lambda d: (x + d) % nx
    seqs, width = tokens.shape
    heads, dk, dv = rec.shape[1:]
    pending = []

    def rcopy(src, dst, ss, rs, ep, tp):
        cp = pltpu.make_async_remote_copy(
            src_ref=src, dst_ref=dst, send_sem=ss, recv_sem=rs, device_id=(ep, tp), device_id_type=MESH
        )
        cp.start()
        pending.append(cp)
        return cp

    barrier = pltpu.get_barrier_semaphore()

    def greet(d, carry):
        pl.semaphore_signal(barrier, inc=1, device_id=((e + d) % EP, x), device_id_type=MESH)
        return carry

    lax.fori_loop(1, EP, greet, 0)
    for d in range(1, nx):
        pl.semaphore_signal(barrier, inc=1, device_id=(e, xdev(d)), device_id_type=MESH)

    count = [0]

    def load(src, dst):
        cp = pltpu.make_async_copy(src, dst, load_sem.at[count[0]])
        count[0] += 1
        cp.start()
        return cp

    first = [load(tokens_h, tokens), load(norm_gain_h, norm_gain)]
    wloads = []
    at = 0
    for w in (wq, wk, wv, wg):
        n = w.shape[1]
        wloads.append(load(w, wbuf.at[yc, :, at : at + n]))
        at += n
    oload = load(ow_h, obuf.at[e])
    qc = width // nx
    edloads = [load(ed_h.at[0, :, q * qc : (q + 1) * qc], dsrc.at[q]) for q in range(nx)]
    small = [
        load(a, b)
        for a, b in (
            (bw_h, bw), (dw_h, dw), (rate_h, rate), (bias_h, bias), (head_gain_h, head_gain),
            (ffn_gain_h, ffn_gain), (routes_h, routes), (rweight_h, rweight), (branch_h, branch_gate),
        )
    ]
    hs = sg_h.shape[1]
    sloads = [
        load(a, sbuf.at[e, :, i * hs : (i + 1) * hs]) for i, a in enumerate((sg_h, su_h, sd_h))
    ]
    load_state = load(rec, state)
    he = eg_h.shape[2]
    eloads = [load(eg_h.at[0], egu.at[:, 0:he]), load(eu_h.at[0], egu.at[:, he : 2 * he])]

    for l in first:
        l.wait()
    normed = rms(tokens[...].astype(F32), norm_gain[...].reshape(1, width).astype(F32)).astype(BF)
    kz = tokbuf.shape[2]
    for i in range(NZ):
        tok_src[i] = normed[:, i * kz : (i + 1) * kz]
    for l in wloads + [oload] + edloads:
        l.wait()
    pl.semaphore_wait(barrier, (EP - 1) + (nx - 1))

    toks = [
        rcopy(tok_src.at[(z + d) % NZ], tokbuf.at[d], t_s.at[d], t_r.at[d], zdev(d), x)
        for d in range(1, NZ)
    ]
    ws = [rcopy(wbuf.at[yc], wbuf.at[yc], w_s.at[d], w_r.at[d], ydev(d), x) for d in range(1, NY)]
    fwd = [rcopy(wbuf.at[yc], wbuf.at[yc], wf_s.at[0], wf_r.at[0], partner, x)]

    def spread_z(buf, ss, rs):
        return [rcopy(buf.at[e], buf.at[e], ss.at[d], rs.at[d], zdev(d), x) for d in range(1, NZ)]

    def spread_y(buf, before, ss, rs, fs, fr):
        over_y, over_c = [], []
        for d in range(NZ):
            if d:
                before[d - 1].wait_recv()
            j = ((z + NZ - d) % NZ) * YC + yc
            for dy in range(1, NY):
                over_y.append((dy, d, rcopy(buf.at[j], buf.at[j], ss.at[dy, d], rs.at[dy, d], ydev(dy), x)))
            over_c.append(rcopy(buf.at[j], buf.at[j], fs.at[0, d], fr.at[0, d], partner, x))
        return over_y, over_c

    def spread_c(buf, over_y, fs, fr):
        over_c = []
        for dy, d, cp in over_y:
            cp.wait_recv()
            j = ((z + NZ - d) % NZ) * YC + ((y + NY - dy) % NY) * NC + c
            over_c.append(rcopy(buf.at[j], buf.at[j], fs.at[dy, d], fr.at[dy, d], partner, x))
        return over_c

    o1 = spread_z(obuf, o1_s, o1_r)
    downs = [
        rcopy(dsrc.at[xdev(d)], dbuf.at[d], ed_s.at[d], ed_r.at[d], e, xdev(d)) for d in range(1, nx)
    ]
    tokbuf[0] = tok_src[z]

    for l in small:
        l.wait()
    bl = nt_dot(normed, bw[...])
    dl = nt_dot(normed, dw[...])
    lanes = iota(bl.shape, 1)
    retain, strength = [], []
    for h in range(heads):
        mine = lanes == x * heads + h
        b = jnp.sum(jnp.where(mine, bl, 0.0), axis=1, keepdims=True)
        g = jnp.sum(jnp.where(mine, dl, 0.0), axis=1, keepdims=True) + bias[h]
        soft = jnp.maximum(g, 0.0) + jnp.log1p(jnp.exp(-jnp.abs(g)))
        strength.append(sigmoid(b))
        retain.append(jnp.exp(-rate[h] * soft))
    lane = iota(rs_ref.shape, 1)
    packed = jnp.zeros(rs_ref.shape, F32)
    for h in range(heads):
        packed = jnp.where(lane == h, retain[h], packed)
        packed = jnp.where(lane == heads + h, strength[h], packed)

    for d in range(1, NY):
        ws[d - 1].wait_recv()
        j = ((y + NY - d) % NY) * NC + c
        fwd.append(rcopy(wbuf.at[j], wbuf.at[j], wf_s.at[d], wf_r.at[d], partner, x))
    for cp in toks + fwd:
        cp.wait_recv()
    cols = wbuf.shape[2]
    partial = jnp.dot(
        tokbuf[...].reshape(NZ * seqs, kz), wbuf[...].reshape(kz, cols), preferred_element_type=F32
    ).astype(BF)
    psend[...] = partial.reshape(NZ, seqs, cols)
    sums = [
        rcopy(psend.at[d], prec.at[d], p_s.at[d], p_r.at[d], zdev(NZ - d), x)
        for d in (4, 3, 5, 2, 6, 1, 7)
    ]
    o2, o3 = spread_y(obuf, o1, o2_s, o2_r, o3_s, o3_r)
    for l in sloads:
        l.wait()
    s1 = spread_z(sbuf, s1_s, s1_r)

    topk = routes.shape[0]
    rrow = [routes[k : k + 1, :] for k in range(topk)]
    square = (seqs, seqs)
    diag = iota(square, 0) == iota(square, 1)
    upright = lambda row, zero: jnp.sum(
        jnp.where(diag, jnp.broadcast_to(row, square), zero), axis=1, keepdims=True
    )
    rcol = [upright(r.astype(F32), 0.0) for r in rrow]
    rrow = [r.astype(F32) for r in rrow]
    before_c = iota(square, 1) < iota(square, 0)
    before_r = iota(square, 0) < iota(square, 1)
    tcol, trow = [], []
    for k in range(topk):
        hits_c = jnp.zeros(square, F32)
        hits_r = jnp.zeros(square, F32)
        for k2 in range(topk):
            hits_c += jnp.where(before_c & (rcol[k] == rrow[k2]), 1.0, 0.0)
            hits_r += jnp.where(before_r & (rrow[k] == rcol[k2]), 1.0, 0.0)
        tcol.append(rcol[k] * SLOTS + jnp.sum(hits_c, axis=1, keepdims=True))
        trow.append(rrow[k] * SLOTS + jnp.sum(hits_r, axis=0, keepdims=True))
    ch = qc // LANES
    wide = ch * seqs
    spreadm = (iota((seqs, wide), 1) % seqs == iota((seqs, wide), 0)).astype(BF)
    rows_all = EP * SLOTS * ch
    rid = iota((rows_all, wide), 0)
    okc = rid % ch == iota((rows_all, wide), 1) // seqs
    ridf = (rid // ch).astype(F32)
    place = jnp.zeros((rows_all, wide), F32)
    for k in range(topk):
        tw = jnp.dot(
            jnp.broadcast_to(trow[k], (8, seqs)).astype(BF), spreadm, preferred_element_type=F32
        )[0:1, :]
        place = jnp.where(okc & (ridf == tw), 1.0, place)
    place = place.astype(BF)
    rw = [rweight[k : k + 1, :] for k in range(topk)]
    rsum = rw[0]
    for k in range(1, topk):
        rsum = rsum + rw[k]
    scol = [upright(rw[k] / rsum * ROUTED_SCALE, 0.0) for k in range(topk)]
    pick_col = jnp.concatenate([tcol[k] * ch + cc for k in range(topk) for cc in range(ch)], axis=0)
    scale_col = jnp.concatenate([scol[k] for k in range(topk) for cc in range(ch)], axis=0)
    pick = (
        jnp.broadcast_to(pick_col, (topk * wide, rows_all))
        == iota((topk * wide, rows_all), 1).astype(F32)
    ).astype(BF)

    for cp in sums:
        cp.wait_recv()
    total = psend[0].astype(F32)
    for d in range(1, NZ):
        total = total + prec[d].astype(F32)
    proj = total.astype(BF).astype(F32)
    o3 += spread_c(obuf, o2, o3_s, o3_r)

    khs = wq.shape[1] // dk
    per = heads // khs
    kq = []
    for i in range(khs):
        q = unit(silu(proj[:, i * dk : (i + 1) * dk])) * dk ** (-0.5)
        k = unit(silu(proj[:, (khs + i) * dk : (khs + i + 1) * dk]))
        keys_out[:, i * dk : (i + 1) * dk] = k
        kt[i] = k.T
        qt[i] = q.T
        kq.append(jnp.sum(k * q, axis=1, keepdims=True))
    for i in range(khs):
        packed = jnp.where(lane == 2 * heads + i, kq[i], packed)
    rs_ref[...] = packed
    retain_out[...] = packed
    vbase = 2 * khs * dk
    for h in range(heads):
        vals[h] = silu(proj[:, vbase + h * dv : vbase + (h + 1) * dv])
    gate = proj[:, vbase + heads * dv :]
    load_state.wait()

    def column(ref, i, s):
        t = ref[i]
        return jnp.sum(jnp.where(iota(t.shape, 1) == s, t, 0.0), axis=1, keepdims=True)

    def read_one(s, carry):
        rowrs = rs_ref[pl.ds(s, 1), :]
        for i in range(khs):
            kcol = column(kt, i, s)
            qcol = column(qt, i, s)
            dotkq = rowrs[:, 2 * heads + i : 2 * heads + i + 1]
            for h in range(i * per, (i + 1) * per):
                st = state[s, h]
                ret = rowrs[:, h : h + 1]
                pred = jnp.sum(st * kcol, axis=0, keepdims=True) * ret
                base = jnp.sum(st * qcol, axis=0, keepdims=True) * ret
                cor = rowrs[:, heads + h : heads + h + 1] * (vals[h, pl.ds(s, 1), :] - pred)
                corr_out[h, pl.ds(s, 1), :] = cor
                ro[h, pl.ds(s, 1), :] = base + dotkq * cor
        return carry

    lax.fori_loop(0, seqs, read_one, 0)

    s2, s3 = spread_y(sbuf, s1, s2_s, s2_r, s3_s, s3_r)
    hg = head_gain[...].reshape(1, dv).astype(F32)
    parts = [rms(ro[h], hg) * silu(gate[:, h * dv : (h + 1) * dv]) for h in range(heads)]
    heads_out = jnp.concatenate(parts, axis=1).astype(BF)
    for cp in o3:
        cp.wait_recv()
    mix_send[...] = nt_dot(heads_out, obuf[...].reshape(width, heads * dv)).astype(BF)
    mixes = [
        rcopy(mix_send, mix_rec.at[d], m_s.at[d], m_r.at[d], e, xdev(d)) for d in range(1, nx)
    ]
    for l in eloads:
        l.wait()
    mixed = mix_send[...].astype(F32)
    for d in range(1, nx):
        mixes[d - 1].wait_recv()
        mixed = mixed + mix_rec[d].astype(F32)
    residual = (tokens[...].astype(F32) + mixed).astype(BF)
    ffn_in = rms(residual.astype(F32), ffn_gain[...].reshape(1, width).astype(F32)).astype(BF)
    for i in range(nx * ch):
        chunks[i] = ffn_in[:, i * LANES : (i + 1) * LANES]
        res_chunks[i] = residual[:, i * LANES : (i + 1) * LANES]

    mine = chunks[pl.ds(x * ch, ch)].reshape(wide, LANES)
    msg = SLOTS * ch
    dsend[...] = (
        jnp.dot(place, mine, preferred_element_type=F32).astype(BF).reshape(EP, msg, LANES)
    )

    def exchange(src, dst, ss, rs):
        def one(i, carry):
            dz, d = i // YC, i % YC
            to = ((z + dz) % NZ) * YC + (yc + d) % YC
            cp = pltpu.make_async_remote_copy(
                src_ref=src.at[to], dst_ref=dst.at[e], send_sem=ss, recv_sem=rs.at[dz],
                device_id=(to, x), device_id_type=MESH,
            )
            cp.start()
            return carry

        lax.fori_loop(1, EP, one, 0)

    def group_wait(dst, dz, rs):
        zs = (z + NZ - dz) % NZ
        n = YC - 1 if dz == 0 else YC
        ref = dst.at[pl.ds(0, n)]
        pltpu.make_async_copy(ref, ref, rs.at[dz]).wait()
        return zs

    def sent_wait(src, ss):
        ref = src.at[pl.ds(0, EP - 1)]
        pltpu.make_async_copy(ref, ref, ss).wait()

    exchange(dsend, xrows.at[x], d_s, d_r)
    xrows[x, e] = dsend[e]

    s3 += spread_c(sbuf, s2, s3_s, s3_r)
    xs = []
    for dz in range(NZ):
        zs = group_wait(xrows.at[x], dz, d_r)
        for d in range(1, nx):
            block = xrows.at[x, pl.ds(zs * YC, YC)]
            xs.append(rcopy(block, block, x_s.at[d, dz], x_r.at[d, dz], e, xdev(d)))
    for cp in s3:
        cp.wait_recv()
    sgu = jnp.dot(ffn_in, sbuf[:, :, 0 : 2 * hs].reshape(width, 2 * hs), preferred_element_type=F32)
    sact = (silu(sgu[:, 0:hs]) * sgu[:, hs:]).astype(BF)
    spart = nt_dot(sact, sbuf[:, :, 2 * hs :].reshape(width, hs)).astype(BF)
    for i in range(nx * ch):
        sh_send[i // ch, (i % ch) * seqs : (i % ch + 1) * seqs, :] = spart[:, i * LANES : (i + 1) * LANES]
    shs = [
        rcopy(sh_send.at[xdev(d)], sh_rec.at[d], h_s.at[d], h_r.at[d], e, xdev(d)) for d in range(1, nx)
    ]
    branch = sigmoid(
        jnp.sum(
            ffn_in.astype(F32) * branch_gate[...].reshape(1, width).astype(F32), axis=1, keepdims=True
        )
    )

    for cp in xs:
        cp.wait_recv()
    gu = jnp.zeros((EP * SLOTS, 2 * he), F32)
    for q in range(nx):
        rowsf[q] = xrows[q].reshape(rows_all, LANES).astype(F32)
    for q in range(nx):
        left = jnp.concatenate(
            [rowsf[q, pl.ds(cc, EP * SLOTS, stride=ch), :] for cc in range(ch)], axis=1
        ).astype(BF)
        gu = gu + jnp.dot(left, egu[q * qc : (q + 1) * qc, :], preferred_element_type=F32)
    act_all[0] = (silu(gu[:, 0:he]) * gu[:, he:]).astype(BF)
    acts = [
        rcopy(act_all.at[0], act_all.at[d], a_s.at[d], a_r.at[d], e, xdev(d)) for d in range(1, nx)
    ]
    for cp in downs:
        cp.wait_recv()
    eout = jnp.dot(act_all[0], dsrc[x], preferred_element_type=F32)
    for d in range(1, nx):
        acts[d - 1].wait_recv()
        eout = eout + jnp.dot(act_all[d], dbuf[d], preferred_element_type=F32)
    for cc in range(ch):
        outf[pl.ds(cc, EP * SLOTS, stride=ch), :] = eout[:, cc * LANES : (cc + 1) * LANES]
    rsend[...] = outf[...].astype(BF).reshape(EP, msg, LANES)
    exchange(rsend, rrecv, r_s, r_r)
    rrecv[e] = rsend[e]

    shared = sh_send[x].astype(F32)
    for d in range(1, nx):
        shs[d - 1].wait_recv()
        shared = shared + sh_rec[d].astype(F32)
    base = res_chunks[pl.ds(x * ch, ch)].reshape(wide, LANES).astype(F32)
    base = base + jnp.concatenate([branch] * ch, axis=0) * shared
    for dz in range(NZ):
        group_wait(rrecv, dz, r_r)
    got = jnp.dot(pick, rrecv[...].reshape(rows_all, LANES), preferred_element_type=F32) * scale_col
    for k in range(topk):
        base = base + got[k * wide : (k + 1) * wide]
    fin[x] = base.astype(BF)
    fins = [rcopy(fin.at[x], fin.at[x], f_s.at[d], f_r.at[d], e, xdev(d)) for d in range(1, nx)]
    for cp in fins:
        cp.wait_recv()
    for i in range(nx * ch):
        out_ref[:, i * LANES : (i + 1) * LANES] = fin[i // ch, (i % ch) * seqs : (i % ch + 1) * seqs, :]

    for cp in pending:
        cp.wait_send()
    sent_wait(dsend, d_s)
    sent_wait(rsend, r_s)


def layer(*args):
    (tokens, norm_gain, wq, wk, wv, wg, bw, dw, rate, bias, head_gain, rec, ow, ffn_gain, routes, rweight,
     eg, eu, ed, sg, su, sd, branch_gate) = args
    nx = lax.axis_size("tp")
    seqs, width = tokens.shape
    heads, dk, dv = rec.shape[1:]
    cols = wq.shape[1] + wk.shape[1] + wv.shape[1] + wg.shape[1]
    rows = wq.shape[0]
    kz = rows * YC
    khs = wq.shape[1] // dk
    topk = routes.shape[1]
    qc = width // nx
    ch = qc // LANES
    he = eg.shape[2]
    hs = sg.shape[1]
    msg = SLOTS * ch
    wide = ch * seqs
    hbm = pl.BlockSpec(memory_space=pltpu.HBM)
    vmem = pl.BlockSpec(memory_space=pltpu.VMEM)
    dma = pltpu.SemaphoreType.DMA
    V = pltpu.VMEM
    return pl.pallas_call(
        layer_kernel,
        out_shape=(
            jax.ShapeDtypeStruct((seqs, width), BF),
            jax.ShapeDtypeStruct((seqs, khs * dk), F32),
            jax.ShapeDtypeStruct((heads, seqs, dv), F32),
            jax.ShapeDtypeStruct((seqs, LANES), F32),
        ),
        in_specs=[hbm] * 23,
        out_specs=(vmem,) * 4,
        scratch_shapes=[
            V((seqs, width), BF), V((width,), BF), V(bw.shape[::-1], BF), V(dw.shape[::-1], BF),
            pltpu.SMEM((heads,), F32), pltpu.SMEM((heads,), F32), V((dv,), BF), V((width,), BF),
            V((topk, seqs), I32), V((topk, seqs), F32), V((width,), BF),
            V(rec.shape, F32),
            V((YC, rows, cols), BF), V((NZ, seqs, kz), BF), V((NZ, seqs, kz), BF),
            V((NZ, seqs, cols), BF), V((NZ, seqs, cols), BF),
            V((EP, ow.shape[1], ow.shape[0]), BF), V((EP, sg.shape[0], 3 * hs), BF),
            V((seqs, width), BF), V((nx, seqs, width), BF),
            V((khs, dk, seqs), F32), V((khs, dk, seqs), F32), V((heads, seqs, dv), F32),
            V((seqs, LANES), F32), V((heads, seqs, dv), F32),
            V((width, 2 * he), BF), V((nx, he, qc), BF), V((nx, he, qc), BF),
            V((nx * ch, seqs, LANES), BF), V((nx * ch, seqs, LANES), BF),
            V((EP, msg, LANES), BF), V((nx, EP, msg, LANES), BF), V((nx, EP * msg, LANES), F32),
            V((nx, EP * SLOTS, he), BF), V((EP * msg, LANES), F32),
            V((EP, msg, LANES), BF), V((EP, msg, LANES), BF),
            V((nx, wide, LANES), BF), V((nx, wide, LANES), BF), V((nx, wide, LANES), BF),
            dma((32,)),
            dma((NY,)), dma((NY,)), dma((NY,)), dma((NY,)),
            dma((NZ,)), dma((NZ,)), dma((NZ,)), dma((NZ,)),
            dma((NZ,)), dma((NZ,)), dma((NY, NZ)), dma((NY, NZ)), dma((NY, NZ)), dma((NY, NZ)),
            dma((NZ,)), dma((NZ,)), dma((NY, NZ)), dma((NY, NZ)), dma((NY, NZ)), dma((NY, NZ)),
            dma((nx,)), dma((nx,)), dma((nx,)), dma((nx,)),
            dma, dma((NZ,)), dma((nx, NZ)), dma((nx, NZ)), dma((nx,)), dma((nx,)), dma, dma((NZ,)),
            dma((nx,)), dma((nx,)), dma((nx,)), dma((nx,)),
        ],
        compiler_params=pltpu.CompilerParams(
            collective_id=1, has_side_effects=True, vmem_limit_bytes=67043328
        ),
        name="layer",
    )(
        tokens, norm_gain, wq, wk, wv, wg, bw.T, dw.T, rate, bias, head_gain, rec, ow.T, ffn_gain,
        routes.T, rweight.T, eg, eu, ed, sg, su, sd.T, branch_gate,
    )


def per_device(*args):
    recurrent = args[11]
    seqs, heads, dk, _ = recurrent.shape
    layer_out, keys, corr, packed = layer(*args)
    keys = jnp.repeat(keys.reshape(seqs, -1, dk), heads * dk // keys.shape[1], axis=1)
    retain = packed[:, 0:heads]
    new_state = (
        recurrent * retain[:, :, None, None]
        + keys[:, :, :, None] * jnp.swapaxes(corr, 0, 1)[:, :, None, :]
    )
    return layer_out, new_state


def solution(mesh):
    return jax.shard_map(
        per_device,
        mesh=mesh,
        in_specs=(
            P("ep", None),
            P(),
            P("ep", "tp"),
            P("ep", "tp"),
            P("ep", "tp"),
            P("ep", "tp"),
            P(),
            P(),
            P("tp"),
            P("tp"),
            P(),
            P("ep", "tp", None, None),
            P("tp", "ep"),
            P(),
            P("ep", None),
            P("ep", None),
            P("ep", None, "tp"),
            P("ep", None, "tp"),
            P("ep", "tp", None),
            P("ep", "tp"),
            P("ep", "tp"),
            P("tp", "ep"),
            P(),
        ),
        out_specs=(P("ep", None), P("ep", "tp", None, None)),
        check_vma=False,
    )
```

```python
import jax
import jax.numpy as jnp
from jax import lax
from jax.experimental import pallas as pl
from jax.experimental.pallas import tpu as pltpu
from jax.sharding import PartitionSpec as P

EPS = 1e-06
ROUTED_SCALE = 2.5
NZ, NY, NC = 8, 4, 2
YC = NY * NC
EP = NZ * YC
SLOTS = 2
UNROLL = 4
STATE_COPIES = 4
LAYER_VMEM = 40 * 1024 * 1024
LANES = 128
MESH = pl.DeviceIdType.MESH
BF = jnp.bfloat16
F32 = jnp.float32
I32 = jnp.int32


def silu(v):
    return v / (1.0 + jnp.exp(-v))


def sigmoid(v):
    return 1.0 / (1.0 + jnp.exp(-v))


def rms(values, gain):
    return values * lax.rsqrt(jnp.mean(values * values, axis=-1, keepdims=True) + EPS) * gain


def unit(v):
    return v * lax.rsqrt(jnp.sum(v * v, axis=-1, keepdims=True) + EPS)


def iota(shape, dim):
    return lax.broadcasted_iota(I32, shape, dim)


def nt_dot(a, b):
    return lax.dot_general(a, b, (((1,), (1,)), ((), ())), preferred_element_type=F32)


def layer_kernel(
    tokens_h, norm_gain_h, wq, wk, wv, wg, bw_h, dw_h, rate_h, bias_h, head_gain_h, rec, ow_h, ffn_gain_h,
    routes_h, rweight_h, eg_h, eu_h, ed_h, sg_h, su_h, sd_h, branch_h,
    out_ref, state,
    tokens, norm_gain, bw, dw, rate, bias, head_gain, ffn_gain, routes, rweight, branch_gate,
    wbuf, tok_src, tokbuf, psend, prec, gsend, grec, obuf, sbuf, mix_send, mix_rec,
    kt, qt, vals, rs_ref, ro, corr,
    egu, dsrc, dbuf, chunks, res_chunks, dsend, xrows, rowsf, act_all, outf, rsend, rrecv, sh_send, sh_rec, fin,
    load_sem, w_s, w_r, wf_s, wf_r, t_s, t_r, p_s, p_r, g_s, g_r, o1_s, o1_r, o2_s, o2_r, o3_s, o3_r,
    s1_s, s1_r, s2_s, s2_r, s3_s, s3_r, m_s, m_r, ed_s, ed_r, d_s, d_r, x_s, x_r, a_s, a_r, r_s, r_r,
    h_s, h_r, f_s, f_r,
):
    e = lax.axis_index("ep")
    x = lax.axis_index("tp")
    nx = lax.axis_size("tp")
    z, yc = lax.div(e, YC), lax.rem(e, YC)
    y, c = lax.div(yc, NC), lax.rem(yc, NC)
    partner = e + 1 - 2 * c
    zdev = lambda d: lax.rem(z + d, NZ) * YC + yc
    ydev = lambda d: z * YC + lax.rem(y + d, NY) * NC + c
    xdev = lambda d: lax.rem(x + d, nx)
    seqs, width = tokens.shape
    heads, dk, dv = rec.shape[1:]
    pending = []

    def rcopy(src, dst, ss, rs, ep, tp):
        cp = pltpu.make_async_remote_copy(
            src_ref=src, dst_ref=dst, send_sem=ss, recv_sem=rs, device_id=(ep, tp), device_id_type=MESH
        )
        cp.start()
        pending.append(cp)
        return cp

    count = [0]

    def load(src, dst):
        cp = pltpu.make_async_copy(src, dst, load_sem.at[count[0]])
        count[0] += 1
        cp.start()
        return cp

    first = [load(tokens_h, tokens), load(norm_gain_h, norm_gain)]
    wloads = []
    at = 0
    for w in (wq, wk, wv, wg):
        n = w.shape[1]
        wloads.append(load(w, wbuf.at[yc, :, at : at + n]))
        at += n
    oload = load(ow_h, obuf.at[e])
    qc = width // nx
    edloads = [load(ed_h.at[0, :, q * qc : (q + 1) * qc], dsrc.at[q]) for q in range(nx)]
    small = [
        load(a, b)
        for a, b in (
            (bw_h, bw), (dw_h, dw), (rate_h, rate), (bias_h, bias), (head_gain_h, head_gain),
            (ffn_gain_h, ffn_gain), (routes_h, routes), (rweight_h, rweight), (branch_h, branch_gate),
        )
    ]
    hs = sg_h.shape[1]
    sloads = [
        load(a, sbuf.at[e, :, i * hs : (i + 1) * hs]) for i, a in enumerate((sg_h, su_h, sd_h))
    ]
    load_state = load(rec, state)
    he = eg_h.shape[2]
    eloads = [load(eg_h.at[0], egu.at[:, 0:he]), load(eu_h.at[0], egu.at[:, he : 2 * he])]

    barrier = pltpu.get_barrier_semaphore()
    zbase = [lax.rem(z + d, NZ) * YC for d in range(NZ)]
    ypart = [lax.rem(yc + d, YC) for d in range(YC)]
    far_first = [(dz, d) for dz in (4, 3, 5, 2, 6, 1, 7, 0) for d in range(YC) if dz or d]
    near_first = far_first[::-1]
    for dz, d in far_first:
        pl.semaphore_signal(barrier, inc=1, device_id=(zbase[dz] + ypart[d], x), device_id_type=MESH)
    for d in range(1, nx):
        pl.semaphore_signal(barrier, inc=1, device_id=(e, xdev(d)), device_id_type=MESH)

    for l in first:
        l.wait()
    normed = rms(tokens[...].astype(F32), norm_gain[...].reshape(1, width).astype(F32)).astype(BF)
    kz = tokbuf.shape[2]
    for i in range(NZ):
        tok_src[i] = normed[:, i * kz : (i + 1) * kz]
    for l in wloads + [oload] + edloads:
        l.wait()
    pl.semaphore_wait(barrier, (EP - 1) + (nx - 1))

    toks = [
        rcopy(tok_src.at[lax.rem(z + d, NZ)], tokbuf.at[d], t_s.at[d], t_r.at[d], zdev(d), x)
        for d in range(1, NZ)
    ]
    ws = [rcopy(wbuf.at[yc], wbuf.at[yc], w_s.at[d], w_r.at[d], ydev(d), x) for d in range(1, NY)]
    fwd = [rcopy(wbuf.at[yc], wbuf.at[yc], wf_s.at[0], wf_r.at[0], partner, x)]

    def spread_z(buf, ss, rs):
        return [rcopy(buf.at[e], buf.at[e], ss.at[d], rs.at[d], zdev(d), x) for d in range(1, NZ)]

    def spread_y(buf, before, ss, rs, fs, fr):
        over_y, over_c = [], []
        for d in range(NZ):
            if d:
                before[d - 1].wait_recv()
            j = lax.rem(z + NZ - d, NZ) * YC + yc
            for dy in range(1, NY):
                over_y.append((dy, d, rcopy(buf.at[j], buf.at[j], ss.at[dy, d], rs.at[dy, d], ydev(dy), x)))
            over_c.append(rcopy(buf.at[j], buf.at[j], fs.at[0, d], fr.at[0, d], partner, x))
        return over_y, over_c

    def spread_c(buf, over_y, fs, fr):
        over_c = []
        for dy, d, cp in over_y:
            cp.wait_recv()
            j = lax.rem(z + NZ - d, NZ) * YC + lax.rem(y + NY - dy, NY) * NC + c
            over_c.append(rcopy(buf.at[j], buf.at[j], fs.at[dy, d], fr.at[dy, d], partner, x))
        return over_c

    o1 = spread_z(obuf, o1_s, o1_r)
    downs = [
        rcopy(dsrc.at[xdev(d)], dbuf.at[d], ed_s.at[d], ed_r.at[d], e, xdev(d)) for d in range(1, nx)
    ]
    tokbuf[0] = tok_src[z]

    for l in small:
        l.wait()
    bl = nt_dot(normed, bw[...])
    dl = nt_dot(normed, dw[...])
    lanes = iota(bl.shape, 1)
    retain, strength = [], []
    for h in range(heads):
        mine = lanes == x * heads + h
        b = jnp.sum(jnp.where(mine, bl, 0.0), axis=1, keepdims=True)
        g = jnp.sum(jnp.where(mine, dl, 0.0), axis=1, keepdims=True) + bias[h]
        soft = jnp.maximum(g, 0.0) + jnp.log1p(jnp.exp(-jnp.abs(g)))
        strength.append(sigmoid(b))
        retain.append(jnp.exp(-rate[h] * soft))
    lane = iota(rs_ref.shape, 1)
    packed = jnp.zeros(rs_ref.shape, F32)
    for h in range(heads):
        packed = jnp.where(lane == h, retain[h], packed)
        packed = jnp.where(lane == heads + h, strength[h], packed)

    for d in range(1, NY):
        ws[d - 1].wait_recv()
        j = lax.rem(y + NY - d, NY) * NC + c
        fwd.append(rcopy(wbuf.at[j], wbuf.at[j], wf_s.at[d], wf_r.at[d], partner, x))
    for cp in toks + fwd:
        cp.wait_recv()
    cols = wbuf.shape[2]
    partial = jnp.dot(
        tokbuf[...].reshape(NZ * seqs, kz), wbuf[...].reshape(kz, cols), preferred_element_type=F32
    ).astype(BF)
    gcols = wg.shape[1]
    psend[...] = partial[:, 0 : cols - gcols].reshape(NZ, seqs, cols - gcols)
    gsend[...] = partial[:, cols - gcols :].reshape(NZ, seqs, gcols)
    far = (4, 3, 5, 2, 6, 1, 7)
    sums = [rcopy(psend.at[d], prec.at[d], p_s.at[d], p_r.at[d], zdev(NZ - d), x) for d in far]
    gsums = [rcopy(gsend.at[d], grec.at[d], g_s.at[d], g_r.at[d], zdev(NZ - d), x) for d in far]
    o2, o3 = spread_y(obuf, o1, o2_s, o2_r, o3_s, o3_r)
    for l in sloads:
        l.wait()
    s1 = spread_z(sbuf, s1_s, s1_r)

    topk = routes.shape[0]
    rrow = [routes[k : k + 1, :] for k in range(topk)]
    square = (seqs, seqs)
    diag = iota(square, 0) == iota(square, 1)
    upright = lambda row, zero: jnp.sum(
        jnp.where(diag, jnp.broadcast_to(row, square), zero), axis=1, keepdims=True
    )
    rcol = [upright(r.astype(F32), 0.0) for r in rrow]
    rrow = [r.astype(F32) for r in rrow]
    before_c = iota(square, 1) < iota(square, 0)
    before_r = iota(square, 0) < iota(square, 1)
    tcol, trow = [], []
    for k in range(topk):
        hits_c = jnp.zeros(square, F32)
        hits_r = jnp.zeros(square, F32)
        for k2 in range(topk):
            hits_c += jnp.where(before_c & (rcol[k] == rrow[k2]), 1.0, 0.0)
            hits_r += jnp.where(before_r & (rrow[k] == rcol[k2]), 1.0, 0.0)
        tcol.append(rcol[k] * SLOTS + jnp.sum(hits_c, axis=1, keepdims=True))
        trow.append(rrow[k] * SLOTS + jnp.sum(hits_r, axis=0, keepdims=True))
    ch = qc // LANES
    wide = ch * seqs
    spreadm = (iota((seqs, wide), 1) % seqs == iota((seqs, wide), 0)).astype(BF)
    rows_all = EP * SLOTS * ch
    rid = iota((rows_all, wide), 0)
    okc = rid % ch == iota((rows_all, wide), 1) // seqs
    ridf = (rid // ch).astype(F32)
    place = jnp.zeros((rows_all, wide), F32)
    for k in range(topk):
        tw = jnp.dot(
            jnp.broadcast_to(trow[k], (8, seqs)).astype(BF), spreadm, preferred_element_type=F32
        )[0:1, :]
        place = jnp.where(okc & (ridf == tw), 1.0, place)
    place = place.astype(BF)
    rw = [rweight[k : k + 1, :] for k in range(topk)]
    rsum = rw[0]
    for k in range(1, topk):
        rsum = rsum + rw[k]
    scol = [upright(rw[k] / rsum * ROUTED_SCALE, 0.0) for k in range(topk)]
    pick_col = jnp.concatenate([tcol[k] * ch + cc for k in range(topk) for cc in range(ch)], axis=0)
    scale_col = jnp.concatenate([scol[k] for k in range(topk) for cc in range(ch)], axis=0)
    pick = (
        jnp.broadcast_to(pick_col, (topk * wide, rows_all))
        == iota((topk * wide, rows_all), 1).astype(F32)
    ).astype(BF)

    for cp in sums:
        cp.wait_recv()
    total = psend[0].astype(F32)
    for d in range(1, NZ):
        total = total + prec[d].astype(F32)
    proj = total.astype(BF).astype(F32)
    khs = wq.shape[1] // dk
    per = heads // khs
    kq = []
    for i in range(khs):
        q = unit(silu(proj[:, i * dk : (i + 1) * dk])) * dk ** (-0.5)
        k = unit(silu(proj[:, (khs + i) * dk : (khs + i + 1) * dk]))
        kt[i] = k.T
        qt[i] = q.T
        kq.append(jnp.sum(k * q, axis=1, keepdims=True))
    for i in range(khs):
        packed = jnp.where(lane == 2 * heads + i, kq[i], packed)
    rs_ref[...] = packed
    vbase = 2 * khs * dk
    for h in range(heads):
        vals[h] = silu(proj[:, vbase + h * dv : vbase + (h + 1) * dv])
    load_state.wait()

    def read_one(s, carry):
        rowrs = rs_ref[pl.ds(s, 1), :]
        for i in range(khs):
            kcol = column(kt, i, s)
            qcol = column(qt, i, s)
            dotkq = rowrs[:, 2 * heads + i : 2 * heads + i + 1]
            for h in range(i * per, (i + 1) * per):
                st = state[s, h]
                ret = rowrs[:, h : h + 1]
                pred = jnp.sum(st * kcol, axis=0, keepdims=True) * ret
                base = jnp.sum(st * qcol, axis=0, keepdims=True) * ret
                cor = rowrs[:, heads + h : heads + h + 1] * (vals[h, pl.ds(s, 1), :] - pred)
                corr[h, pl.ds(s, 1), :] = cor
                ro[h, pl.ds(s, 1), :] = base + dotkq * cor
        return carry

    lax.fori_loop(0, seqs, read_one, 0, unroll=UNROLL)

    o3 += spread_c(obuf, o2, o3_s, o3_r)
    for cp in gsums:
        cp.wait_recv()
    total = gsend[0].astype(F32)
    for d in range(1, NZ):
        total = total + grec[d].astype(F32)
    gate = total.astype(BF).astype(F32)
    hg = head_gain[...].reshape(1, dv).astype(F32)
    parts = [rms(ro[h], hg) * silu(gate[:, h * dv : (h + 1) * dv]) for h in range(heads)]
    heads_out = jnp.concatenate(parts, axis=1).astype(BF)
    for cp in o3:
        cp.wait_recv()
    mix_send[...] = nt_dot(heads_out, obuf[...].reshape(width, heads * dv)).astype(BF)
    mixes = [
        rcopy(mix_send, mix_rec.at[d], m_s.at[d], m_r.at[d], e, xdev(d)) for d in range(1, nx)
    ]
    def write_one(s, carry):
        rowrs = rs_ref[pl.ds(s, 1), :]
        for i in range(khs):
            kcol = column(kt, i, s)
            for h in range(i * per, (i + 1) * per):
                state[s, h] = state[s, h] * rowrs[:, h : h + 1] + kcol * corr[h, pl.ds(s, 1), :]
        return carry

    lax.fori_loop(0, seqs, write_one, 0, unroll=UNROLL)
    mixed = mix_send[...].astype(F32)
    for d in range(1, nx):
        mixes[d - 1].wait_recv()
        mixed = mixed + mix_rec[d].astype(F32)
    residual = (tokens[...].astype(F32) + mixed).astype(BF)
    ffn_in = rms(residual.astype(F32), ffn_gain[...].reshape(1, width).astype(F32)).astype(BF)
    for i in range(nx * ch):
        chunks[i] = ffn_in[:, i * LANES : (i + 1) * LANES]
        res_chunks[i] = residual[:, i * LANES : (i + 1) * LANES]

    mine = chunks[pl.ds(x * ch, ch)].reshape(wide, LANES)
    msg = SLOTS * ch
    dsend[...] = (
        jnp.dot(place, mine, preferred_element_type=F32).astype(BF).reshape(EP, msg, LANES)
    )

    def exchange(src, dst, ss, rs, order):
        for dz, d in order:
            to = zbase[dz] + ypart[d]
            pltpu.make_async_remote_copy(
                src_ref=src.at[to], dst_ref=dst.at[e], send_sem=ss, recv_sem=rs.at[dz],
                device_id=(to, x), device_id_type=MESH,
            ).start()

    def group_wait(dst, dz, rs):
        zs = lax.rem(z + NZ - dz, NZ)
        n = YC - 1 if dz == 0 else YC
        ref = dst.at[pl.ds(0, n)]
        pltpu.make_async_copy(ref, ref, rs.at[dz]).wait()
        return zs

    def sent_wait(src, ss):
        ref = src.at[pl.ds(0, EP - 1)]
        pltpu.make_async_copy(ref, ref, ss).wait()

    exchange(dsend, xrows.at[x], d_s, d_r, near_first)
    xrows[x, e] = dsend[e]
    s2, s3 = spread_y(sbuf, s1, s2_s, s2_r, s3_s, s3_r)
    xs = []
    for dz in (0, 7, 1, 6, 2, 5, 3, 4):
        zs = group_wait(xrows.at[x], dz, d_r)
        for d in range(1, nx):
            block = xrows.at[x, pl.ds(zs * YC, YC)]
            xs.append(rcopy(block, block, x_s.at[d, dz], x_r.at[d, dz], e, xdev(d)))
    for l in eloads:
        l.wait()
    for cp in xs:
        cp.wait_recv()
    gu = jnp.zeros((EP * SLOTS, 2 * he), F32)
    for q in range(nx):
        rowsf[q] = xrows[q].reshape(rows_all, LANES).astype(F32)
    for q in range(nx):
        left = jnp.concatenate(
            [rowsf[q, pl.ds(cc, EP * SLOTS, stride=ch), :] for cc in range(ch)], axis=1
        ).astype(BF)
        gu = gu + jnp.dot(left, egu[q * qc : (q + 1) * qc, :], preferred_element_type=F32)
    act_all[0] = (silu(gu[:, 0:he]) * gu[:, he:]).astype(BF)
    acts = [
        rcopy(act_all.at[0], act_all.at[d], a_s.at[d], a_r.at[d], e, xdev(d)) for d in range(1, nx)
    ]
    s3 += spread_c(sbuf, s2, s3_s, s3_r)
    for cp in downs:
        cp.wait_recv()
    eout = jnp.dot(act_all[0], dsrc[x], preferred_element_type=F32)
    for d in range(1, nx):
        acts[d - 1].wait_recv()
        eout = eout + jnp.dot(act_all[d], dbuf[d], preferred_element_type=F32)
    for cc in range(ch):
        outf[pl.ds(cc, EP * SLOTS, stride=ch), :] = eout[:, cc * LANES : (cc + 1) * LANES]
    rsend[...] = outf[...].astype(BF).reshape(EP, msg, LANES)
    exchange(rsend, rrecv, r_s, r_r, far_first)
    rrecv[e] = rsend[e]
    for cp in s3:
        cp.wait_recv()
    sgu = jnp.dot(ffn_in, sbuf[:, :, 0 : 2 * hs].reshape(width, 2 * hs), preferred_element_type=F32)
    sact = (silu(sgu[:, 0:hs]) * sgu[:, hs:]).astype(BF)
    spart = nt_dot(sact, sbuf[:, :, 2 * hs :].reshape(width, hs)).astype(BF)
    for i in range(nx * ch):
        sh_send[i // ch, (i % ch) * seqs : (i % ch + 1) * seqs, :] = spart[:, i * LANES : (i + 1) * LANES]
    shs = [
        rcopy(sh_send.at[xdev(d)], sh_rec.at[d], h_s.at[d], h_r.at[d], e, xdev(d)) for d in range(1, nx)
    ]
    branch = sigmoid(
        jnp.sum(
            ffn_in.astype(F32) * branch_gate[...].reshape(1, width).astype(F32), axis=1, keepdims=True
        )
    )


    shared = sh_send[x].astype(F32)
    for d in range(1, nx):
        shs[d - 1].wait_recv()
        shared = shared + sh_rec[d].astype(F32)
    base = res_chunks[pl.ds(x * ch, ch)].reshape(wide, LANES).astype(F32)
    base = base + jnp.concatenate([branch] * ch, axis=0) * shared
    for dz in range(NZ):
        group_wait(rrecv, dz, r_r)
    got = jnp.dot(pick, rrecv[...].reshape(rows_all, LANES), preferred_element_type=F32) * scale_col
    for k in range(topk):
        base = base + got[k * wide : (k + 1) * wide]
    fin[x] = base.astype(BF)
    fins = [rcopy(fin.at[x], fin.at[x], f_s.at[d], f_r.at[d], e, xdev(d)) for d in range(1, nx)]
    for cp in fins:
        cp.wait_recv()
    for i in range(nx * ch):
        out_ref[:, i * LANES : (i + 1) * LANES] = fin[i // ch, (i % ch) * seqs : (i % ch + 1) * seqs, :]

    for cp in pending:
        cp.wait_send()
    sent_wait(dsend, d_s)
    sent_wait(rsend, r_s)


def layer(*args):
    (tokens, norm_gain, wq, wk, wv, wg, bw, dw, rate, bias, head_gain, rec, ow, ffn_gain, routes, rweight,
     eg, eu, ed, sg, su, sd, branch_gate) = args
    nx = lax.axis_size("tp")
    seqs, width = tokens.shape
    heads, dk, dv = rec.shape[1:]
    cols = wq.shape[1] + wk.shape[1] + wv.shape[1] + wg.shape[1]
    rows = wq.shape[0]
    kz = rows * YC
    khs = wq.shape[1] // dk
    topk = routes.shape[1]
    qc = width // nx
    ch = qc // LANES
    he = eg.shape[2]
    hs = sg.shape[1]
    msg = SLOTS * ch
    wide = ch * seqs
    hbm = pl.BlockSpec(memory_space=pltpu.HBM)
    vmem = pl.BlockSpec(memory_space=pltpu.VMEM)
    dma = pltpu.SemaphoreType.DMA
    V = pltpu.VMEM
    return pl.pallas_call(
        layer_kernel,
        out_shape=(
            jax.ShapeDtypeStruct((seqs, width), BF),
            pltpu.VMEM(rec.shape, F32),
        ),
        in_specs=[hbm] * 23,
        out_specs=(vmem,) * 2,
        scratch_shapes=[
            V((seqs, width), BF), V((width,), BF), V(bw.shape[::-1], BF), V(dw.shape[::-1], BF),
            pltpu.SMEM((heads,), F32), pltpu.SMEM((heads,), F32), V((dv,), BF), V((width,), BF),
            V((topk, seqs), I32), V((topk, seqs), F32), V((width,), BF),
            V((YC, rows, cols), BF), V((NZ, seqs, kz), BF), V((NZ, seqs, kz), BF),
            V((NZ, seqs, cols - wg.shape[1]), BF), V((NZ, seqs, cols - wg.shape[1]), BF),
            V((NZ, seqs, wg.shape[1]), BF), V((NZ, seqs, wg.shape[1]), BF),
            V((EP, ow.shape[1], ow.shape[0]), BF), V((EP, sg.shape[0], 3 * hs), BF),
            V((seqs, width), BF), V((nx, seqs, width), BF),
            V((khs, dk, seqs), F32), V((khs, dk, seqs), F32), V((heads, seqs, dv), F32),
            V((seqs, LANES), F32), V((heads, seqs, dv), F32), V((heads, seqs, dv), F32),
            V((width, 2 * he), BF), V((nx, he, qc), BF), V((nx, he, qc), BF),
            V((nx * ch, seqs, LANES), BF), V((nx * ch, seqs, LANES), BF),
            V((EP, msg, LANES), BF), V((nx, EP, msg, LANES), BF), V((nx, EP * msg, LANES), F32),
            V((nx, EP * SLOTS, he), BF), V((EP * msg, LANES), F32),
            V((EP, msg, LANES), BF), V((EP, msg, LANES), BF),
            V((nx, wide, LANES), BF), V((nx, wide, LANES), BF), V((nx, wide, LANES), BF),
            dma((32,)),
            dma((NY,)), dma((NY,)), dma((NY,)), dma((NY,)),
            dma((NZ,)), dma((NZ,)), dma((NZ,)), dma((NZ,)), dma((NZ,)), dma((NZ,)),
            dma((NZ,)), dma((NZ,)), dma((NY, NZ)), dma((NY, NZ)), dma((NY, NZ)), dma((NY, NZ)),
            dma((NZ,)), dma((NZ,)), dma((NY, NZ)), dma((NY, NZ)), dma((NY, NZ)), dma((NY, NZ)),
            dma((nx,)), dma((nx,)), dma((nx,)), dma((nx,)),
            dma, dma((NZ,)), dma((nx, NZ)), dma((nx, NZ)), dma((nx,)), dma((nx,)), dma, dma((NZ,)),
            dma((nx,)), dma((nx,)), dma((nx,)), dma((nx,)),
        ],
        compiler_params=pltpu.CompilerParams(
            collective_id=1, has_side_effects=True, vmem_limit_bytes=LAYER_VMEM
        ),
        name="layer",
    )(
        *(
            pltpu.with_memory_space_constraint(a, pltpu.HBM)
            for a in (
                tokens, norm_gain, wq, wk, wv, wg, bw.T, dw.T, rate, bias, head_gain, rec, ow.T, ffn_gain,
                routes.T, rweight.T, eg, eu, ed, sg, su, sd.T, branch_gate,
            )
        )
    )


def column(ref, i, s):
    t = ref[i]
    return jnp.sum(jnp.where(iota(t.shape, 1) == s, t, 0.0), axis=1, keepdims=True)


def store_kernel(layer_in, state, layer_out, new, sems):
    n = state.shape[0] // STATE_COPIES
    copies = [
        pltpu.make_async_copy(
            state.at[pl.ds(i * n, n)], new.at[pl.ds(i * n, n)], sems.at[i]
        )
        for i in range(STATE_COPIES)
    ]
    copies.append(pltpu.make_async_copy(layer_in, layer_out, sems.at[STATE_COPIES]))
    for cp in copies:
        cp.start()
    for cp in copies:
        cp.wait()


def per_device(*args):
    layer_out, state = layer(*args)
    hbm = pl.BlockSpec(memory_space=pltpu.HBM)
    vmem = pl.BlockSpec(memory_space=pltpu.VMEM)
    return pl.pallas_call(
        store_kernel,
        out_shape=(
            jax.ShapeDtypeStruct(layer_out.shape, BF),
            jax.ShapeDtypeStruct(state.shape, F32),
        ),
        in_specs=[vmem, vmem],
        out_specs=(hbm, hbm),
        scratch_shapes=[pltpu.SemaphoreType.DMA((STATE_COPIES + 1,))],
        compiler_params=pltpu.CompilerParams(vmem_limit_bytes=8 * 1024 * 1024),
        name="store",
    )(layer_out, pltpu.with_memory_space_constraint(state, pltpu.VMEM))


def solution(mesh):
    return jax.shard_map(
        per_device,
        mesh=mesh,
        in_specs=(
            P("ep", None),
            P(),
            P("ep", "tp"),
            P("ep", "tp"),
            P("ep", "tp"),
            P("ep", "tp"),
            P(),
            P(),
            P("tp"),
            P("tp"),
            P(),
            P("ep", "tp", None, None),
            P("tp", "ep"),
            P(),
            P("ep", None),
            P("ep", None),
            P("ep", None, "tp"),
            P("ep", None, "tp"),
            P("ep", "tp", None),
            P("ep", "tp"),
            P("ep", "tp"),
            P("tp", "ep"),
            P(),
        ),
        out_specs=(P("ep", None), P("ep", "tp", None, None)),
        check_vma=False,
    )
```

```python
import jax
import jax.numpy as jnp
from jax import lax
from jax.experimental import pallas as pl
from jax.experimental.pallas import tpu as pltpu
from jax.sharding import PartitionSpec as P

EPS = 1e-06
ROUTED_SCALE = 2.5
NZ, NY, NC = 8, 4, 2
YC = NY * NC
EP = NZ * YC
SLOTS = 2
UNROLL = 2
STATE_COPIES = 4
MIX_CHUNKS = 4
FAR = (4, 3, 5, 2, 6, 1, 7)
NEAR = (1, 7, 2, 6, 3, 5, 4)
GROUPS = ((0,), (1, 7), (2, 6), (3, 5, 4))
GROUP = {d: i for i, g in enumerate(GROUPS) for d in g}
LAYER_VMEM = 40 * 1024 * 1024
LANES = 128
MESH = pl.DeviceIdType.MESH
BF = jnp.bfloat16
F32 = jnp.float32
I32 = jnp.int32


def silu(v):
    return v / (1.0 + jnp.exp(-v))


def sigmoid(v):
    return 1.0 / (1.0 + jnp.exp(-v))


def rms(values, gain):
    return values * lax.rsqrt(jnp.mean(values * values, axis=-1, keepdims=True) + EPS) * gain


def unit(v):
    return v * lax.rsqrt(jnp.sum(v * v, axis=-1, keepdims=True) + EPS)


def iota(shape, dim):
    return lax.broadcasted_iota(I32, shape, dim)


def nt_dot(a, b):
    return lax.dot_general(a, b, (((1,), (1,)), ((), ())), preferred_element_type=F32)


def layer_kernel(
    tokens_h, norm_gain_h, wq, wk, wv, wg, bw_h, dw_h, rate_h, bias_h, head_gain_h, rec, ow_h, ffn_gain_h,
    routes_h, rweight_h, eg_h, eu_h, ed_h, sg_h, su_h, sd_h, branch_h,
    out_ref, state,
    tokens, norm_gain, bw, dw, rate, bias, head_gain, ffn_gain, routes, rweight, branch_gate,
    wbuf, gbuf, tok_src, tokbuf, psend, prec, gsend, grec, obuf, sbuf, mix_send, mix_rec,
    kqt, vals, rs_ref, ro, corr,
    egu, dsrc, dbuf, chunks, res_chunks, dsend, xrows, rowsf, act_all, outf, rsend, rrecv, sh_send, sh_rec, fin,
    load_sem, w_r, gw_r, o1_r, o2_r, s1_r, s2_r, d_r,
    t_r, wf_r, gf_r, p_r, g_r, o3_r, s3_r, m_r, ed_r, x_r, a_r, r_r, h_r, f_r,
    t_s, w_s, gw_s, p_s, g_s, o_s, s_s, m_s, ed_s, d_s, x_s, a_s, r_s, h_s, f_s,
):
    e = lax.axis_index("ep")
    x = lax.axis_index("tp")
    nx = lax.axis_size("tp")
    z, yc = lax.div(e, YC), lax.rem(e, YC)
    y, c = lax.div(yc, NC), lax.rem(yc, NC)
    partner = e + 1 - 2 * c
    zdev = lambda d: lax.rem(z + d, NZ) * YC + yc
    ydev = lambda d: z * YC + lax.rem(y + d, NY) * NC + c
    xdev = lambda d: lax.rem(x + d, nx)
    seqs, width = tokens.shape
    heads, dk, dv = rec.shape[1:]

    def wait_all(ref, sem):
        pltpu.make_async_copy(ref, ref, sem).wait()

    def rcopy(src, dst, ss, rs, ep, tp):
        cp = pltpu.make_async_remote_copy(
            src_ref=src, dst_ref=dst, send_sem=ss, recv_sem=rs, device_id=(ep, tp), device_id_type=MESH
        )
        cp.start()
        return cp

    count = [0]

    def load(src, dst):
        cp = pltpu.make_async_copy(src, dst, load_sem.at[count[0]])
        count[0] += 1
        cp.start()
        return cp

    first = [load(tokens_h, tokens), load(norm_gain_h, norm_gain)]
    wloads = []
    at = 0
    for w in (wq, wk, wv):
        n = w.shape[1]
        wloads.append(load(w, wbuf.at[yc, :, at : at + n]))
        at += n
    wloads.append(load(wg, gbuf.at[yc]))
    oload = load(ow_h, obuf.at[e])
    qc = width // nx
    edloads = [load(ed_h.at[0, :, q * qc : (q + 1) * qc], dsrc.at[q]) for q in range(nx)]
    small = [
        load(a, b)
        for a, b in (
            (bw_h, bw), (dw_h, dw), (rate_h, rate), (bias_h, bias), (head_gain_h, head_gain),
            (ffn_gain_h, ffn_gain), (routes_h, routes), (rweight_h, rweight), (branch_h, branch_gate),
        )
    ]
    hs = sg_h.shape[1]
    sloads = [
        load(a, sbuf.at[e, :, i * hs : (i + 1) * hs]) for i, a in enumerate((sg_h, su_h, sd_h))
    ]
    load_state = load(rec, state)
    he = eg_h.shape[2]
    eloads = [load(eg_h.at[0], egu.at[:, 0:he]), load(eu_h.at[0], egu.at[:, he : 2 * he])]

    barrier = pltpu.get_barrier_semaphore()
    zbase = [lax.rem(z + d, NZ) * YC for d in range(NZ)]
    ypart = [lax.rem(yc + d, YC) for d in range(YC)]
    far_first = [(dz, d) for dz in (4, 3, 5, 2, 6, 1, 7, 0) for d in range(YC) if dz or d]
    near_first = far_first[::-1]
    for dz in (4, 3, 5, 2, 6, 1, 7):
        pl.semaphore_signal(barrier, inc=1, device_id=(zbase[dz] + yc, x), device_id_type=MESH)
    for d in range(1, YC):
        pl.semaphore_signal(barrier, inc=1, device_id=(zbase[0] + ypart[d], x), device_id_type=MESH)
    for d in range(1, nx):
        pl.semaphore_signal(barrier, inc=1, device_id=(e, xdev(d)), device_id_type=MESH)

    for l in first:
        l.wait()
    normed = rms(tokens[...].astype(F32), norm_gain[...].reshape(1, width).astype(F32)).astype(BF)
    kz = tokbuf.shape[2]
    for i in range(NZ):
        tok_src[i] = normed[:, i * kz : (i + 1) * kz]
    for l in wloads + [oload] + edloads:
        l.wait()
    pl.semaphore_wait(barrier, (NZ - 1) + (YC - 1) + (nx - 1))

    for d in FAR:
        rcopy(tok_src.at[lax.rem(z + d, NZ)], tokbuf.at[d], t_s, t_r, zdev(d), x)

    def rows_y(buf, ss, rs, fr):
        rcopies = [rcopy(buf.at[yc], buf.at[yc], ss, rs.at[d], ydev(d), x) for d in range(1, NY)]
        rcopy(buf.at[yc], buf.at[yc], ss, fr, partner, x)
        return rcopies

    def rows_c(buf, over_y, ss, fr, which):
        for d in which:
            over_y[d - 1].wait_recv()
            j = lax.rem(y + NY - d, NY) * NC + c
            rcopy(buf.at[j], buf.at[j], ss, fr, partner, x)

    ws = rows_y(wbuf, w_s, w_r, wf_r)
    gws = rows_y(gbuf, gw_s, gw_r, gf_r)

    def spread_z(buf, ss, rs):
        for d in NEAR:
            rcopy(buf.at[e], buf.at[e], ss, rs.at[GROUP[d]], zdev(d), x)

    def z_blocks(which):
        return [lax.rem(z + NZ - d, NZ) * YC for d in which]

    def spread_y(buf, group, ss, rs, fr):
        for zb in z_blocks(GROUPS[group]):
            j = zb + yc
            for dy in range(1, NY):
                rcopy(buf.at[j], buf.at[j], ss, rs.at[group], ydev(dy), x)
            rcopy(buf.at[j], buf.at[j], ss, fr, partner, x)

    def spread_c(buf, group, ss, rs, fr):
        wait_all(buf.at[pl.ds(0, len(GROUPS[group]) * (NY - 1))], rs.at[group])
        for zb in z_blocks(GROUPS[group]):
            for dy in range(1, NY):
                j = zb + lax.rem(y + NY - dy, NY) * NC + c
                rcopy(buf.at[j], buf.at[j], ss, fr, partner, x)

    spread_z(obuf, o_s, o1_r)
    spread_y(obuf, 0, o_s, o2_r, o3_r)
    for d in range(1, nx):
        rcopy(dsrc.at[xdev(d)], dbuf.at[d], ed_s, ed_r, e, xdev(d))
    tokbuf[0] = tok_src[z]

    for l in small:
        l.wait()
    bl = nt_dot(normed, bw[...])
    dl = nt_dot(normed, dw[...])
    lanes = iota(bl.shape, 1)
    retain, strength = [], []
    for h in range(heads):
        mine = lanes == x * heads + h
        b = jnp.sum(jnp.where(mine, bl, 0.0), axis=1, keepdims=True)
        g = jnp.sum(jnp.where(mine, dl, 0.0), axis=1, keepdims=True) + bias[h]
        soft = jnp.maximum(g, 0.0) + jnp.log1p(jnp.exp(-jnp.abs(g)))
        strength.append(sigmoid(b))
        retain.append(jnp.exp(-rate[h] * soft))
    lane = iota(rs_ref.shape, 1)
    packed = jnp.zeros(rs_ref.shape, F32)
    for h in range(heads):
        packed = jnp.where(lane == h, retain[h], packed)
        packed = jnp.where(lane == heads + h, strength[h], packed)

    rows_c(wbuf, ws, w_s, wf_r, (1, 3))
    wait_all(obuf.at[pl.ds(0, len(GROUPS[1]))], o1_r.at[1])
    spread_y(obuf, 1, o_s, o2_r, o3_r)
    rows_c(wbuf, ws, w_s, wf_r, (2,))
    wait_all(tokbuf.at[pl.ds(1, NZ - 1)], t_r)
    wait_all(wbuf.at[pl.ds(0, NY)], wf_r)
    toks_all = tokbuf[...].reshape(NZ * seqs, kz)

    def project(buf, sent, got, ss, rs):
        n = buf.shape[2]
        sent[...] = (
            jnp.dot(toks_all, buf[...].reshape(kz, n), preferred_element_type=F32)
            .astype(BF)
            .reshape(NZ, seqs, n)
        )
        for d in FAR:
            rcopy(sent.at[d], got.at[d], ss, rs, zdev(NZ - d), x)

    def collected(sent, got, rs):
        wait_all(got.at[pl.ds(1, NZ - 1)], rs)
        total = sent[0].astype(F32)
        for d in range(1, NZ):
            total = total + got[d].astype(F32)
        return total.astype(BF).astype(F32)

    project(wbuf, psend, prec, p_s, p_r)
    rows_c(gbuf, gws, gw_s, gf_r, (1, 3, 2))
    wait_all(obuf.at[pl.ds(0, len(GROUPS[2]))], o1_r.at[2])
    spread_y(obuf, 2, o_s, o2_r, o3_r)
    wait_all(gbuf.at[pl.ds(0, NY)], gf_r)
    project(gbuf, gsend, grec, g_s, g_r)
    wait_all(obuf.at[pl.ds(0, len(GROUPS[3]))], o1_r.at[3])
    spread_y(obuf, 3, o_s, o2_r, o3_r)
    for l in sloads:
        l.wait()
    spread_z(sbuf, s_s, s1_r)

    topk = routes.shape[0]
    rrow = [routes[k : k + 1, :] for k in range(topk)]
    square = (seqs, seqs)
    diag = iota(square, 0) == iota(square, 1)
    upright = lambda row, zero: jnp.sum(
        jnp.where(diag, jnp.broadcast_to(row, square), zero), axis=1, keepdims=True
    )
    rcol = [upright(r.astype(F32), 0.0) for r in rrow]
    rrow = [r.astype(F32) for r in rrow]
    before_c = iota(square, 1) < iota(square, 0)
    before_r = iota(square, 0) < iota(square, 1)
    tcol, trow = [], []
    for k in range(topk):
        hits_c = jnp.zeros(square, F32)
        hits_r = jnp.zeros(square, F32)
        for k2 in range(topk):
            hits_c += jnp.where(before_c & (rcol[k] == rrow[k2]), 1.0, 0.0)
            hits_r += jnp.where(before_r & (rrow[k] == rcol[k2]), 1.0, 0.0)
        tcol.append(rcol[k] * SLOTS + jnp.sum(hits_c, axis=1, keepdims=True))
        trow.append(rrow[k] * SLOTS + jnp.sum(hits_r, axis=0, keepdims=True))
    ch = qc // LANES
    wide = ch * seqs
    spreadm = (iota((seqs, wide), 1) % seqs == iota((seqs, wide), 0)).astype(BF)
    rows_all = EP * SLOTS * ch
    rid = iota((rows_all, wide), 0)
    okc = rid % ch == iota((rows_all, wide), 1) // seqs
    ridf = (rid // ch).astype(F32)
    place = jnp.zeros((rows_all, wide), F32)
    for k in range(topk):
        tw = jnp.dot(
            jnp.broadcast_to(trow[k], (8, seqs)).astype(BF), spreadm, preferred_element_type=F32
        )[0:1, :]
        place = jnp.where(okc & (ridf == tw), 1.0, place)
    place = place.astype(BF)
    rw = [rweight[k : k + 1, :] for k in range(topk)]
    rsum = rw[0]
    for k in range(1, topk):
        rsum = rsum + rw[k]
    scol = [upright(rw[k] / rsum * ROUTED_SCALE, 0.0) for k in range(topk)]
    pick_col = jnp.concatenate([tcol[k] * ch + cc for k in range(topk) for cc in range(ch)], axis=0)
    scale_col = jnp.concatenate([scol[k] for k in range(topk) for cc in range(ch)], axis=0)
    pick = (
        jnp.broadcast_to(pick_col, (topk * wide, rows_all))
        == iota((topk * wide, rows_all), 1).astype(F32)
    ).astype(BF)

    proj = collected(psend, prec, p_r)
    for group in range(3):
        spread_c(obuf, group, o_s, o2_r, o3_r)
    khs = wq.shape[1] // dk
    per = heads // khs
    kq = []

    def split(i, t):
        hi = t.astype(BF)
        mid = (t - hi.astype(F32)).astype(BF)
        lo = (t - hi.astype(F32) - mid.astype(F32)).astype(BF)
        kqt[i * dk : (i + 1) * dk, :] = jnp.concatenate([hi, mid, lo], axis=1)

    for i in range(khs):
        q = unit(silu(proj[:, i * dk : (i + 1) * dk])) * dk ** (-0.5)
        k = unit(silu(proj[:, (khs + i) * dk : (khs + i + 1) * dk]))
        split(i, k.T)
        split(khs + i, q.T)
        kq.append(jnp.sum(k * q, axis=1, keepdims=True))
    for i in range(khs):
        packed = jnp.where(lane == 2 * heads + i, kq[i], packed)
    rs_ref[...] = packed
    vbase = 2 * khs * dk
    for h in range(heads):
        vals[h] = silu(proj[:, vbase + h * dv : vbase + (h + 1) * dv])
    load_state.wait()

    span = 2 * dv

    def spread_columns(first, rows):
        shape = (kqt.shape[1], span)
        hot = (lax.rem(iota(shape, 0), seqs) == first + iota(shape, 1) // dv).astype(BF)
        return jnp.dot(kqt[0:rows, :], hot, preferred_element_type=F32)

    def read_pair(p, carry):
        both = spread_columns(2 * p, 2 * khs * dk)
        for j in range(2):
            s = 2 * p + j
            wide_cols = both[:, j * dv : (j + 1) * dv]
            rowrs = rs_ref[pl.ds(s, 1), :]
            for i in range(khs):
                kcol = wide_cols[i * dk : (i + 1) * dk]
                qcol = wide_cols[(khs + i) * dk : (khs + i + 1) * dk]
                dotkq = rowrs[:, 2 * heads + i : 2 * heads + i + 1]
                for h in range(i * per, (i + 1) * per):
                    st = state[s, h]
                    ret = rowrs[:, h : h + 1]
                    pred = jnp.sum(st * kcol, axis=0, keepdims=True) * ret
                    base = jnp.sum(st * qcol, axis=0, keepdims=True) * ret
                    cor = rowrs[:, heads + h : heads + h + 1] * (vals[h, pl.ds(s, 1), :] - pred)
                    corr[h, pl.ds(s, 1), :] = cor
                    ro[h, pl.ds(s, 1), :] = base + dotkq * cor
        return carry

    lax.fori_loop(0, seqs // 2, read_pair, 0, unroll=UNROLL)

    spread_c(obuf, 3, o_s, o2_r, o3_r)
    gate = collected(gsend, grec, g_r)
    hg = head_gain[...].reshape(1, dv).astype(F32)
    parts = [rms(ro[h], hg) * silu(gate[:, h * dv : (h + 1) * dv]) for h in range(heads)]
    heads_out = jnp.concatenate(parts, axis=1).astype(BF)
    wait_all(obuf.at[pl.ds(0, EP // NC)], o3_r)
    per_chunk = EP // MIX_CHUNKS
    for i in range(MIX_CHUNKS):
        n = width // MIX_CHUNKS
        mix_send[i] = nt_dot(
            heads_out, obuf[i * per_chunk : (i + 1) * per_chunk].reshape(n, heads * dv)
        ).astype(BF)
        for d in range(1, nx):
            rcopy(mix_send.at[i], mix_rec.at[d, i], m_s, m_r, e, xdev(d))
    def write_pair(p, carry):
        both = spread_columns(2 * p, khs * dk)
        for j in range(2):
            s = 2 * p + j
            rowrs = rs_ref[pl.ds(s, 1), :]
            for i in range(khs):
                kcol = both[i * dk : (i + 1) * dk, j * dv : (j + 1) * dv]
                for h in range(i * per, (i + 1) * per):
                    state[s, h] = state[s, h] * rowrs[:, h : h + 1] + kcol * corr[h, pl.ds(s, 1), :]
        return carry

    lax.fori_loop(0, seqs // 2, write_pair, 0, unroll=UNROLL)
    wait_all(mix_rec.at[pl.ds(1, nx - 1)], m_r)
    mixed = []
    for i in range(MIX_CHUNKS):
        part = mix_send[i].astype(F32)
        for d in range(1, nx):
            part = part + mix_rec[d, i].astype(F32)
        mixed.append(part)
    mixed = jnp.concatenate(mixed, axis=1)
    residual = (tokens[...].astype(F32) + mixed).astype(BF)
    ffn_in = rms(residual.astype(F32), ffn_gain[...].reshape(1, width).astype(F32)).astype(BF)
    for i in range(nx * ch):
        chunks[i] = ffn_in[:, i * LANES : (i + 1) * LANES]
        res_chunks[i] = residual[:, i * LANES : (i + 1) * LANES]

    mine = chunks[pl.ds(x * ch, ch)].reshape(wide, LANES)
    msg = SLOTS * ch
    dsend[...] = (
        jnp.dot(place, mine, preferred_element_type=F32).astype(BF).reshape(EP, msg, LANES)
    )

    def exchange(src, dst, ss, rs, order):
        for dz, d in order:
            to = zbase[dz] + ypart[d]
            pltpu.make_async_remote_copy(
                src_ref=src.at[to], dst_ref=dst.at[e], send_sem=ss, recv_sem=rs(dz),
                device_id=(to, x), device_id_type=MESH,
            ).start()

    def group_wait(dst, dz, rs):
        zs = lax.rem(z + NZ - dz, NZ)
        n = YC - 1 if dz == 0 else YC
        ref = dst.at[pl.ds(0, n)]
        pltpu.make_async_copy(ref, ref, rs.at[dz]).wait()
        return zs

    exchange(dsend, xrows.at[x], d_s, lambda dz: d_r.at[dz], near_first)
    xrows[x, e] = dsend[e]
    for dz in (0, 7, 1, 6, 2, 5, 3, 4):
        zs = group_wait(xrows.at[x], dz, d_r)
        for d in range(1, nx):
            block = xrows.at[x, pl.ds(zs * YC, YC)]
            rcopy(block, block, x_s, x_r, e, xdev(d))
    for l in eloads:
        l.wait()
    for group in range(4):
        if group:
            wait_all(sbuf.at[pl.ds(0, len(GROUPS[group]))], s1_r.at[group])
        spread_y(sbuf, group, s_s, s2_r, s3_r)
    wait_all(xrows.at[pl.ds(1, nx - 1)], x_r)
    gu = jnp.zeros((EP * SLOTS, 2 * he), F32)
    for q in range(nx):
        rowsf[q] = xrows[q].reshape(rows_all, LANES).astype(F32)
    for q in range(nx):
        left = jnp.concatenate(
            [rowsf[q, pl.ds(cc, EP * SLOTS, stride=ch), :] for cc in range(ch)], axis=1
        ).astype(BF)
        gu = gu + jnp.dot(left, egu[q * qc : (q + 1) * qc, :], preferred_element_type=F32)
    act_all[0] = (silu(gu[:, 0:he]) * gu[:, he:]).astype(BF)
    for d in range(1, nx):
        rcopy(act_all.at[0], act_all.at[d], a_s, a_r, e, xdev(d))
    wait_all(dbuf.at[pl.ds(1, nx - 1)], ed_r)
    eout = jnp.dot(act_all[0], dsrc[x], preferred_element_type=F32)
    wait_all(act_all.at[pl.ds(1, nx - 1)], a_r)
    for d in range(1, nx):
        eout = eout + jnp.dot(act_all[d], dbuf[d], preferred_element_type=F32)
    for cc in range(ch):
        outf[pl.ds(cc, EP * SLOTS, stride=ch), :] = eout[:, cc * LANES : (cc + 1) * LANES]
    rsend[...] = outf[...].astype(BF).reshape(EP, msg, LANES)
    exchange(rsend, rrecv, r_s, lambda dz: r_r, far_first)
    rrecv[e] = rsend[e]
    for group in range(4):
        spread_c(sbuf, group, s_s, s2_r, s3_r)
    wait_all(sbuf.at[pl.ds(0, EP // NC)], s3_r)
    sgu = jnp.dot(ffn_in, sbuf[:, :, 0 : 2 * hs].reshape(width, 2 * hs), preferred_element_type=F32)
    sact = (silu(sgu[:, 0:hs]) * sgu[:, hs:]).astype(BF)
    spart = nt_dot(sact, sbuf[:, :, 2 * hs :].reshape(width, hs)).astype(BF)
    for i in range(nx * ch):
        sh_send[i // ch, (i % ch) * seqs : (i % ch + 1) * seqs, :] = spart[:, i * LANES : (i + 1) * LANES]
    for d in range(1, nx):
        rcopy(sh_send.at[xdev(d)], sh_rec.at[d], h_s, h_r, e, xdev(d))
    branch = sigmoid(
        jnp.sum(
            ffn_in.astype(F32) * branch_gate[...].reshape(1, width).astype(F32), axis=1, keepdims=True
        )
    )


    shared = sh_send[x].astype(F32)
    wait_all(sh_rec.at[pl.ds(1, nx - 1)], h_r)
    for d in range(1, nx):
        shared = shared + sh_rec[d].astype(F32)
    base = res_chunks[pl.ds(x * ch, ch)].reshape(wide, LANES).astype(F32)
    base = base + jnp.concatenate([branch] * ch, axis=0) * shared
    wait_all(rrecv.at[pl.ds(0, EP - 1)], r_r)
    got = jnp.dot(pick, rrecv[...].reshape(rows_all, LANES), preferred_element_type=F32) * scale_col
    for k in range(topk):
        base = base + got[k * wide : (k + 1) * wide]
    fin[x] = base.astype(BF)
    for d in range(1, nx):
        rcopy(fin.at[x], fin.at[x], f_s, f_r, e, xdev(d))
    wait_all(fin.at[pl.ds(0, nx - 1)], f_r)
    for i in range(nx * ch):
        out_ref[:, i * LANES : (i + 1) * LANES] = fin[i // ch, (i % ch) * seqs : (i % ch + 1) * seqs, :]

    some = lambda ref, n: ref.at[pl.ds(0, n)]
    for ref, sem in (
        (some(tokbuf, NZ - 1), t_s), (some(wbuf, 2 * NY - 1), w_s), (some(gbuf, 2 * NY - 1), gw_s),
        (some(psend, NZ - 1), p_s), (some(gsend, NZ - 1), g_s), (some(obuf, EP - 1), o_s),
        (some(sbuf, EP - 1), s_s), (some(mix_rec, nx - 1), m_s), (some(dsrc, nx - 1), ed_s),
        (some(dsend, EP - 1), d_s), (some(xrows, nx - 1), x_s), (some(act_all, nx - 1), a_s),
        (some(rsend, EP - 1), r_s), (some(sh_send, nx - 1), h_s), (some(fin, nx - 1), f_s),
    ):
        wait_all(ref, sem)


def layer(*args):
    (tokens, norm_gain, wq, wk, wv, wg, bw, dw, rate, bias, head_gain, rec, ow, ffn_gain, routes, rweight,
     eg, eu, ed, sg, su, sd, branch_gate) = args
    nx = lax.axis_size("tp")
    seqs, width = tokens.shape
    heads, dk, dv = rec.shape[1:]
    cols = wq.shape[1] + wk.shape[1] + wv.shape[1] + wg.shape[1]
    rows = wq.shape[0]
    kz = rows * YC
    khs = wq.shape[1] // dk
    topk = routes.shape[1]
    qc = width // nx
    ch = qc // LANES
    he = eg.shape[2]
    hs = sg.shape[1]
    msg = SLOTS * ch
    wide = ch * seqs
    hbm = pl.BlockSpec(memory_space=pltpu.HBM)
    vmem = pl.BlockSpec(memory_space=pltpu.VMEM)
    dma = pltpu.SemaphoreType.DMA
    V = pltpu.VMEM
    return pl.pallas_call(
        layer_kernel,
        out_shape=(
            jax.ShapeDtypeStruct((seqs, width), BF),
            pltpu.VMEM(rec.shape, F32),
        ),
        in_specs=[hbm] * 23,
        out_specs=(vmem,) * 2,
        scratch_shapes=[
            V((seqs, width), BF), V((width,), BF), V(bw.shape[::-1], BF), V(dw.shape[::-1], BF),
            pltpu.SMEM((heads,), F32), pltpu.SMEM((heads,), F32), V((dv,), BF), V((width,), BF),
            V((topk, seqs), I32), V((topk, seqs), F32), V((width,), BF),
            V((YC, rows, cols - wg.shape[1]), BF), V((YC, rows, wg.shape[1]), BF), V((NZ, seqs, kz), BF), V((NZ, seqs, kz), BF),
            V((NZ, seqs, cols - wg.shape[1]), BF), V((NZ, seqs, cols - wg.shape[1]), BF),
            V((NZ, seqs, wg.shape[1]), BF), V((NZ, seqs, wg.shape[1]), BF),
            V((EP, ow.shape[1], ow.shape[0]), BF), V((EP, sg.shape[0], 3 * hs), BF),
            V((MIX_CHUNKS, seqs, width // MIX_CHUNKS), BF), V((nx, MIX_CHUNKS, seqs, width // MIX_CHUNKS), BF),
            V((2 * khs * dk, 3 * seqs), BF), V((heads, seqs, dv), F32),
            V((seqs, LANES), F32), V((heads, seqs, dv), F32), V((heads, seqs, dv), F32),
            V((width, 2 * he), BF), V((nx, he, qc), BF), V((nx, he, qc), BF),
            V((nx * ch, seqs, LANES), BF), V((nx * ch, seqs, LANES), BF),
            V((EP, msg, LANES), BF), V((nx, EP, msg, LANES), BF), V((nx, EP * msg, LANES), F32),
            V((nx, EP * SLOTS, he), BF), V((EP * msg, LANES), F32),
            V((EP, msg, LANES), BF), V((EP, msg, LANES), BF),
            V((nx, wide, LANES), BF), V((nx, wide, LANES), BF), V((nx, wide, LANES), BF),
            dma((26,)), dma((NY,)), dma((NY,)), dma((4,)), dma((4,)), dma((4,)), dma((4,)), dma((NZ,)),
            *[dma] * 29,
        ],
        compiler_params=pltpu.CompilerParams(
            collective_id=1, has_side_effects=True, vmem_limit_bytes=LAYER_VMEM
        ),
        name="layer",
    )(
        *(
            pltpu.with_memory_space_constraint(a, pltpu.HBM)
            for a in (
                tokens, norm_gain, wq, wk, wv, wg, bw.T, dw.T, rate, bias, head_gain, rec, ow.T, ffn_gain,
                routes.T, rweight.T, eg, eu, ed, sg, su, sd.T, branch_gate,
            )
        )
    )


def store_kernel(layer_in, state, layer_out, new, sems):
    n = state.shape[0] // STATE_COPIES
    copies = [
        pltpu.make_async_copy(
            state.at[pl.ds(i * n, n)], new.at[pl.ds(i * n, n)], sems.at[i]
        )
        for i in range(STATE_COPIES)
    ]
    copies.append(pltpu.make_async_copy(layer_in, layer_out, sems.at[STATE_COPIES]))
    for cp in copies:
        cp.start()
    for cp in copies:
        cp.wait()


def per_device(*args):
    layer_out, state = layer(*args)
    hbm = pl.BlockSpec(memory_space=pltpu.HBM)
    vmem = pl.BlockSpec(memory_space=pltpu.VMEM)
    return pl.pallas_call(
        store_kernel,
        out_shape=(
            jax.ShapeDtypeStruct(layer_out.shape, BF),
            jax.ShapeDtypeStruct(state.shape, F32),
        ),
        in_specs=[vmem, vmem],
        out_specs=(hbm, hbm),
        scratch_shapes=[pltpu.SemaphoreType.DMA((STATE_COPIES + 1,))],
        compiler_params=pltpu.CompilerParams(vmem_limit_bytes=8 * 1024 * 1024),
        name="store",
    )(layer_out, pltpu.with_memory_space_constraint(state, pltpu.VMEM))


def solution(mesh):
    return jax.shard_map(
        per_device,
        mesh=mesh,
        in_specs=(
            P("ep", None),
            P(),
            P("ep", "tp"),
            P("ep", "tp"),
            P("ep", "tp"),
            P("ep", "tp"),
            P(),
            P(),
            P("tp"),
            P("tp"),
            P(),
            P("ep", "tp", None, None),
            P("tp", "ep"),
            P(),
            P("ep", None),
            P("ep", None),
            P("ep", None, "tp"),
            P("ep", None, "tp"),
            P("ep", "tp", None),
            P("ep", "tp"),
            P("ep", "tp"),
            P("tp", "ep"),
            P(),
        ),
        out_specs=(P("ep", None), P("ep", "tp", None, None)),
        check_vma=False,
    )
```

```python
import jax
import jax.numpy as jnp
from jax import lax
from jax.experimental import pallas as pl
from jax.experimental.pallas import tpu as pltpu
from jax.sharding import PartitionSpec as P

EPS = 1e-06
ROUTED_SCALE = 2.5
NZ, NY, NC = 8, 4, 2
YC = NY * NC
EP = NZ * YC
SLOTS = 2
UNROLL = 2
STATE_COPIES = 4
FAR = (4, 3, 5, 2, 6, 1, 7)
NEAR = (1, 7, 2, 6, 3, 5, 4)
GROUPS = ((0,), (1, 7), (2, 6), (3, 5, 4))
SEND_ORDER = (0, 7, 1, 6, 2, 5, 3, 4)
ARRIVAL = (0, 7, 1, 6, 2, 5, 3, 4)
GROUP = {d: i for i, g in enumerate(GROUPS) for d in g}
LAYER_VMEM = 40 * 1024 * 1024
LANES = 128
MESH = pl.DeviceIdType.MESH
BF = jnp.bfloat16
F32 = jnp.float32
I32 = jnp.int32


def silu(v):
    return v / (1.0 + jnp.exp(-v))


def sigmoid(v):
    return 1.0 / (1.0 + jnp.exp(-v))


def rms(values, gain):
    return values * lax.rsqrt(jnp.mean(values * values, axis=-1, keepdims=True) + EPS) * gain


def unit(v):
    return v * lax.rsqrt(jnp.sum(v * v, axis=-1, keepdims=True) + EPS)


def iota(shape, dim):
    return lax.broadcasted_iota(I32, shape, dim)


def nt_dot(a, b):
    return lax.dot_general(a, b, (((1,), (1,)), ((), ())), preferred_element_type=F32)


def layer_kernel(
    tokens_h, norm_gain_h, wq, wk, wv, wg, bw_h, dw_h, rate_h, bias_h, head_gain_h, rec, ow_h, ffn_gain_h,
    routes_h, rweight_h, eg_h, eu_h, ed_h, sg_h, su_h, sd_h, branch_h,
    out_ref, state,
    tokens, norm_gain, bw, dw, rate, bias, head_gain, ffn_gain, routes, rweight, branch_gate,
    wbuf, gbuf, tok_src, tokbuf, psend, prec, gsend, grec, obuf, sbuf, mix_send, mix_rec,
    kqt, vals, rs_ref, ro, corr,
    egu, dsrc, dbuf, tok_chunks, res_all, dsend, xrows, rowsf, act_all, outf, rsend, rrecv, sh_send, sh_rec, fin,
    load_sem, w_r, gw_r, o1_r, o2_r, s1_r, s2_r, d_r,
    x_r, a_r, t_r, wf_r, gf_r, p_r, g_r, o3_r, s3_r, m_r, ed_r, r_r, h_r, f_r, n_r,
    t_s, w_s, gw_s, p_s, g_s, o_s, s_s, m_s, ed_s, d_s, x_s, a_s, r_s, h_s, f_s, n_s,
):
    e = lax.axis_index("ep")
    x = lax.axis_index("tp")
    nx = lax.axis_size("tp")
    z, yc = lax.div(e, YC), lax.rem(e, YC)
    y, c = lax.div(yc, NC), lax.rem(yc, NC)
    partner = e + 1 - 2 * c
    zdev = lambda d: lax.rem(z + d, NZ) * YC + yc
    ydev = lambda d: z * YC + lax.rem(y + d, NY) * NC + c
    xdev = lambda d: lax.rem(x + d, nx)
    peers = sorted(range(1, nx), key=lambda d: -min(d, nx - d))
    ypeers = sorted(range(1, NY), key=lambda d: -min(d, NY - d))
    seqs, width = tokens.shape
    heads, dk, dv = rec.shape[1:]

    def wait_all(ref, sem):
        pltpu.make_async_copy(ref, ref, sem).wait()

    def rcopy(src, dst, ss, rs, ep, tp):
        cp = pltpu.make_async_remote_copy(
            src_ref=src, dst_ref=dst, send_sem=ss, recv_sem=rs, device_id=(ep, tp), device_id_type=MESH
        )
        cp.start()
        return cp

    count = [0]

    def load(*pairs):
        sem = load_sem.at[count[0]]
        count[0] += 1
        for src, dst in pairs:
            pltpu.make_async_copy(src, dst, sem).start()
        return sem

    cuts = [0]
    for w in (wq, wk, wv):
        cuts.append(cuts[-1] + w.shape[1])
    w_load = load(*((w, wbuf.at[yc, :, cuts[i] : cuts[i + 1]]) for i, w in enumerate((wq, wk, wv))))
    first = [(a, load((b, a))) for a, b in ((tokens, tokens_h), (norm_gain, norm_gain_h))]
    g_load = load((wg, gbuf.at[yc]))
    o_load = load((ow_h, obuf.at[e]))
    qc = width // nx
    ed_load = load(*((ed_h.at[0, :, q * qc : (q + 1) * qc], dsrc.at[q]) for q in range(nx)))
    small = [
        (b, load((a, b)))
        for a, b in (
            (bw_h, bw), (dw_h, dw), (rate_h, rate), (bias_h, bias), (head_gain_h, head_gain),
            (ffn_gain_h, ffn_gain), (routes_h, routes), (rweight_h, rweight), (branch_h, branch_gate),
        )
    ]
    hs = sg_h.shape[1]
    s_load = load(
        *((a, sbuf.at[e, :, i * hs : (i + 1) * hs]) for i, a in enumerate((sg_h, su_h, sd_h)))
    )
    state_load = load((rec, state))
    he = eg_h.shape[2]
    e_load = load((eg_h.at[0], egu.at[:, 0:he]), (eu_h.at[0], egu.at[:, he : 2 * he]))

    barrier = pltpu.get_barrier_semaphore()
    zbase = [lax.rem(z + d, NZ) * YC for d in range(NZ)]
    ypart = [lax.rem(yc + d, YC) for d in range(YC)]
    for dz in (4, 3, 5, 2, 6, 1, 7):
        pl.semaphore_signal(barrier, inc=1, device_id=(zbase[dz] + yc, x), device_id_type=MESH)
    for d in range(1, YC):
        pl.semaphore_signal(barrier, inc=1, device_id=(zbase[0] + ypart[d], x), device_id_type=MESH)
    for d in range(1, nx):
        pl.semaphore_signal(barrier, inc=1, device_id=(e, xdev(d)), device_id_type=MESH)

    def rows_y(buf, ss, rs, fr):
        rcopies = [rcopy(buf.at[yc], buf.at[yc], ss, rs.at[d], ydev(d), x) for d in ypeers]
        rcopy(buf.at[yc], buf.at[yc], ss, fr, partner, x)
        return dict(zip(ypeers, rcopies))

    def rows_c(buf, over_y, ss, fr, which):
        for d in which:
            over_y[d].wait_recv()
            j = lax.rem(y + NY - d, NY) * NC + c
            rcopy(buf.at[j], buf.at[j], ss, fr, partner, x)

    wait_all(wbuf.at[yc], w_load)
    pl.semaphore_wait(barrier, (NZ - 1) + (YC - 1) + (nx - 1))
    ws = rows_y(wbuf, w_s, w_r, wf_r)
    for ref, sem in first:
        wait_all(ref, sem)
    normed = rms(tokens[...].astype(F32), norm_gain[...].reshape(1, width).astype(F32)).astype(BF)
    kz = tokbuf.shape[2]
    for i in range(NZ):
        tok_src[i] = normed[:, i * kz : (i + 1) * kz]
    for d in FAR:
        rcopy(tok_src.at[lax.rem(z + d, NZ)], tokbuf.at[d], t_s, t_r, zdev(d), x)
    wait_all(gbuf.at[yc], g_load)
    gws = rows_y(gbuf, gw_s, gw_r, gf_r)
    wait_all(obuf.at[e], o_load)
    wait_all(dsrc, ed_load)

    def spread_z(buf, ss, rs):
        for d in NEAR:
            rcopy(buf.at[e], buf.at[e], ss, rs.at[GROUP[d]], zdev(d), x)

    def z_blocks(which):
        return [lax.rem(z + NZ - d, NZ) * YC for d in which]

    def spread_y(buf, group, ss, rs, fr):
        for zb in z_blocks(GROUPS[group]):
            j = zb + yc
            for dy in ypeers:
                rcopy(buf.at[j], buf.at[j], ss, rs.at[group], ydev(dy), x)
            rcopy(buf.at[j], buf.at[j], ss, fr, partner, x)

    def spread_c(buf, group, ss, rs, fr):
        wait_all(buf.at[pl.ds(0, len(GROUPS[group]) * (NY - 1))], rs.at[group])
        for zb in z_blocks(GROUPS[group]):
            for dy in range(1, NY):
                j = zb + lax.rem(y + NY - dy, NY) * NC + c
                rcopy(buf.at[j], buf.at[j], ss, fr, partner, x)

    spread_z(obuf, o_s, o1_r)
    spread_y(obuf, 0, o_s, o2_r, o3_r)
    for d in peers:
        rcopy(dsrc.at[xdev(d)], dbuf.at[d], ed_s, ed_r, e, xdev(d))
    tokbuf[0] = tok_src[z]

    for ref, sem in small:
        wait_all(ref, sem)
    bl = nt_dot(normed, bw[...])
    dl = nt_dot(normed, dw[...])
    lanes = iota(bl.shape, 1)
    retain, strength = [], []
    for h in range(heads):
        mine = lanes == x * heads + h
        b = jnp.sum(jnp.where(mine, bl, 0.0), axis=1, keepdims=True)
        g = jnp.sum(jnp.where(mine, dl, 0.0), axis=1, keepdims=True) + bias[h]
        soft = jnp.maximum(g, 0.0) + jnp.log1p(jnp.exp(-jnp.abs(g)))
        strength.append(sigmoid(b))
        retain.append(jnp.exp(-rate[h] * soft))
    lane = iota(rs_ref.shape, 1)
    packed = jnp.zeros(rs_ref.shape, F32)
    for h in range(heads):
        packed = jnp.where(lane == h, retain[h], packed)
        packed = jnp.where(lane == heads + h, strength[h], packed)

    rows_c(wbuf, ws, w_s, wf_r, (1, 3))
    wait_all(obuf.at[pl.ds(0, len(GROUPS[1]))], o1_r.at[1])
    spread_y(obuf, 1, o_s, o2_r, o3_r)
    rows_c(wbuf, ws, w_s, wf_r, (2,))
    wait_all(tokbuf.at[pl.ds(1, NZ - 1)], t_r)
    wait_all(wbuf.at[pl.ds(0, NY)], wf_r)
    toks_all = tokbuf[...].reshape(NZ * seqs, kz)

    def project(buf, sent, got, ss, rs):
        n = buf.shape[2]
        sent[...] = (
            jnp.dot(toks_all, buf[...].reshape(kz, n), preferred_element_type=F32)
            .astype(BF)
            .reshape(NZ, seqs, n)
        )
        for d in FAR:
            rcopy(sent.at[d], got.at[d], ss, rs, zdev(NZ - d), x)

    def collected(sent, got, rs):
        wait_all(got.at[pl.ds(1, NZ - 1)], rs)
        total = sent[0].astype(F32)
        for d in range(1, NZ):
            total = total + got[d].astype(F32)
        return total.astype(BF).astype(F32)

    project(wbuf, psend, prec, p_s, p_r)
    rows_c(gbuf, gws, gw_s, gf_r, (1, 3, 2))
    wait_all(obuf.at[pl.ds(0, len(GROUPS[2]))], o1_r.at[2])
    spread_y(obuf, 2, o_s, o2_r, o3_r)
    wait_all(gbuf.at[pl.ds(0, NY)], gf_r)
    project(gbuf, gsend, grec, g_s, g_r)
    wait_all(obuf.at[pl.ds(0, len(GROUPS[3]))], o1_r.at[3])
    spread_y(obuf, 3, o_s, o2_r, o3_r)
    wait_all(sbuf.at[e], s_load)
    spread_z(sbuf, s_s, s1_r)

    def s_relay(group):
        if group:
            wait_all(sbuf.at[pl.ds(0, len(GROUPS[group]))], s1_r.at[group])
        spread_y(sbuf, group, s_s, s2_r, s3_r)


    ch = qc // LANES
    for i in range(nx * ch):
        tok_chunks[i] = tokens[:, i * LANES : (i + 1) * LANES]
    topk = routes.shape[0]
    rrow = [routes[k : k + 1, :] for k in range(topk)]
    square = (seqs, seqs)
    diag = iota(square, 0) == iota(square, 1)
    upright = lambda row, zero: jnp.sum(
        jnp.where(diag, jnp.broadcast_to(row, square), zero), axis=1, keepdims=True
    )
    rcol = [upright(r.astype(F32), 0.0) for r in rrow]
    rrow = [r.astype(F32) for r in rrow]
    before_c = iota(square, 1) < iota(square, 0)
    before_r = iota(square, 0) < iota(square, 1)
    tcol, trow = [], []
    for k in range(topk):
        hits_c = jnp.zeros(square, F32)
        hits_r = jnp.zeros(square, F32)
        for k2 in range(topk):
            hits_c += jnp.where(before_c & (rcol[k] == rrow[k2]), 1.0, 0.0)
            hits_r += jnp.where(before_r & (rrow[k] == rcol[k2]), 1.0, 0.0)
        tcol.append(rcol[k] * SLOTS + jnp.sum(hits_c, axis=1, keepdims=True))
        trow.append(rrow[k] * SLOTS + jnp.sum(hits_r, axis=0, keepdims=True))
    wide = ch * seqs
    spreadm = (iota((seqs, wide), 1) % seqs == iota((seqs, wide), 0)).astype(BF)
    rows_all = EP * SLOTS * ch
    rid = iota((rows_all, wide), 0)
    okc = rid % ch == iota((rows_all, wide), 1) // seqs
    ridf = (rid // ch).astype(F32)
    place = jnp.zeros((rows_all, wide), F32)
    for k in range(topk):
        tw = jnp.dot(
            jnp.broadcast_to(trow[k], (8, seqs)).astype(BF), spreadm, preferred_element_type=F32
        )[0:1, :]
        place = jnp.where(okc & (ridf == tw), 1.0, place)
    place = place.astype(BF)
    rw = [rweight[k : k + 1, :] for k in range(topk)]
    rsum = rw[0]
    for k in range(1, topk):
        rsum = rsum + rw[k]
    scol = [upright(rw[k] / rsum * ROUTED_SCALE, 0.0) for k in range(topk)]
    pick_col = jnp.concatenate([tcol[k] * ch + cc for k in range(topk) for cc in range(ch)], axis=0)
    scale_col = jnp.concatenate([scol[k] for k in range(topk) for cc in range(ch)], axis=0)
    pick = (
        jnp.broadcast_to(pick_col, (topk * wide, rows_all))
        == iota((topk * wide, rows_all), 1).astype(F32)
    ).astype(BF)

    proj = collected(psend, prec, p_r)
    for group in range(3):
        spread_c(obuf, group, o_s, o2_r, o3_r)
    khs = wq.shape[1] // dk
    per = heads // khs
    kq = []

    def split(i, t):
        hi = t.astype(BF)
        mid = (t - hi.astype(F32)).astype(BF)
        lo = (t - hi.astype(F32) - mid.astype(F32)).astype(BF)
        kqt[i * dk : (i + 1) * dk, :] = jnp.concatenate([hi, mid, lo], axis=1)

    for i in range(khs):
        q = unit(silu(proj[:, i * dk : (i + 1) * dk])) * dk ** (-0.5)
        k = unit(silu(proj[:, (khs + i) * dk : (khs + i + 1) * dk]))
        split(i, k.T)
        split(khs + i, q.T)
        kq.append(jnp.sum(k * q, axis=1, keepdims=True))
    for i in range(khs):
        packed = jnp.where(lane == 2 * heads + i, kq[i], packed)
    rs_ref[...] = packed
    vbase = 2 * khs * dk
    for h in range(heads):
        vals[h] = silu(proj[:, vbase + h * dv : vbase + (h + 1) * dv])
    wait_all(state, state_load)

    span = 2 * dv

    def spread_columns(first, rows):
        shape = (kqt.shape[1], span)
        hot = (lax.rem(iota(shape, 0), seqs) == first + iota(shape, 1) // dv).astype(BF)
        return jnp.dot(kqt[0:rows, :], hot, preferred_element_type=F32)

    def read_pair(p, carry):
        both = spread_columns(2 * p, 2 * khs * dk)
        for j in range(2):
            s = 2 * p + j
            wide_cols = both[:, j * dv : (j + 1) * dv]
            rowrs = rs_ref[pl.ds(s, 1), :]
            for i in range(khs):
                kcol = wide_cols[i * dk : (i + 1) * dk]
                qcol = wide_cols[(khs + i) * dk : (khs + i + 1) * dk]
                dotkq = rowrs[:, 2 * heads + i : 2 * heads + i + 1]
                for h in range(i * per, (i + 1) * per):
                    st = state[s, h]
                    ret = rowrs[:, h : h + 1]
                    pred = jnp.sum(st * kcol, axis=0, keepdims=True) * ret
                    base = jnp.sum(st * qcol, axis=0, keepdims=True) * ret
                    cor = rowrs[:, heads + h : heads + h + 1] * (vals[h, pl.ds(s, 1), :] - pred)
                    corr[h, pl.ds(s, 1), :] = cor
                    ro[h, pl.ds(s, 1), :] = base + dotkq * cor
        return carry

    lax.fori_loop(0, seqs // 2, read_pair, 0, unroll=UNROLL)

    spread_c(obuf, 3, o_s, o2_r, o3_r)
    gate = collected(gsend, grec, g_r)
    hg = head_gain[...].reshape(1, dv).astype(F32)
    parts = [rms(ro[h], hg) * silu(gate[:, h * dv : (h + 1) * dv]) for h in range(heads)]
    heads_out = jnp.concatenate(parts, axis=1).astype(BF)
    wait_all(obuf.at[pl.ds(0, EP // NC)], o3_r)
    mix = nt_dot(heads_out, obuf[...].reshape(width, heads * dv)).astype(BF)
    for q in range(nx):
        mix_send[q] = mix[:, q * qc : (q + 1) * qc]
    for d in peers:
        rcopy(mix_send.at[xdev(d)], mix_rec.at[d], m_s, m_r, e, xdev(d))
    def write_pair(p, carry):
        both = spread_columns(2 * p, khs * dk)
        for j in range(2):
            s = 2 * p + j
            rowrs = rs_ref[pl.ds(s, 1), :]
            for i in range(khs):
                kcol = both[i * dk : (i + 1) * dk, j * dv : (j + 1) * dv]
                for h in range(i * per, (i + 1) * per):
                    state[s, h] = state[s, h] * rowrs[:, h : h + 1] + kcol * corr[h, pl.ds(s, 1), :]
        return carry

    lax.fori_loop(0, seqs // 2, write_pair, 0, unroll=UNROLL)
    s_relay(0)
    s_relay(1)
    wait_all(mix_rec.at[pl.ds(1, nx - 1)], m_r)
    mixed = mix_send[x].astype(F32)
    for d in range(1, nx):
        mixed = mixed + mix_rec[d].astype(F32)
    own = tok_chunks[pl.ds(x * ch, ch)].astype(F32)
    mine = jnp.concatenate(
        [own[cc] + mixed[:, cc * LANES : (cc + 1) * LANES] for cc in range(ch)], axis=0
    ).astype(BF)
    res_all[x] = mine
    msg = SLOTS * ch
    dsend[...] = (
        jnp.dot(place, mine, preferred_element_type=F32).astype(BF).reshape(EP, msg, LANES)
    )

    zback = [lax.rem(z + NZ - d, NZ) * YC for d in range(NZ)]
    yback = [lax.rem(yc + YC - d, YC) for d in range(YC)]
    place_of = {dz: i * YC for i, dz in enumerate(ARRIVAL)}
    half = EP // 2
    part_of = lambda dz: place_of[dz] // half
    for dz in SEND_ORDER:
        for d in range(YC):
            if dz or d:
                to = zbase[dz] + ypart[d]
                rcopy(dsend.at[to], xrows.at[x, place_of[dz] + d], d_s, d_r.at[dz], to, x)
    xrows[x, 0] = dsend[e]
    for d in peers:
        rcopy(res_all.at[x], res_all.at[x], n_s, n_r, e, xdev(d))
    for dz in ARRIVAL:
        n = YC if dz else YC - 1
        wait_all(xrows.at[x, pl.ds(place_of[dz], n)], d_r.at[dz])
        block = xrows.at[x, pl.ds(place_of[dz], YC)]
        for d in peers:
            rcopy(block, block, x_s, x_r.at[part_of(dz)], e, xdev(d))
    s_relay(2)
    s_relay(3)
    wait_all(egu, e_load)
    fgain = ffn_gain[...].reshape(1, width).astype(F32)
    nrows = half * SLOTS

    def dense_branch():
        for group in range(4):
            spread_c(sbuf, group, s_s, s2_r, s3_r)
        wait_all(sbuf.at[pl.ds(0, EP // NC)], s3_r)
        wait_all(res_all.at[pl.ds(0, nx - 1)], n_r)
        residual = jnp.concatenate(
            [res_all[i // ch, (i % ch) * seqs : (i % ch + 1) * seqs, :] for i in range(nx * ch)], axis=1
        ).astype(F32)
        ffn_in = rms(residual, fgain).astype(BF)
        sgu = jnp.dot(ffn_in, sbuf[:, :, 0 : 2 * hs].reshape(width, 2 * hs), preferred_element_type=F32)
        sact = (silu(sgu[:, 0:hs]) * sgu[:, hs:]).astype(BF)
        spart = nt_dot(sact, sbuf[:, :, 2 * hs :].reshape(width, hs)).astype(BF)
        for i in range(nx * ch):
            sh_send[i // ch, (i % ch) * seqs : (i % ch + 1) * seqs, :] = spart[:, i * LANES : (i + 1) * LANES]
        for d in peers:
            rcopy(sh_send.at[xdev(d)], sh_rec.at[d], h_s, h_r, e, xdev(d))
        branch = sigmoid(
            jnp.sum(
                ffn_in.astype(F32) * branch_gate[...].reshape(1, width).astype(F32), axis=1, keepdims=True
            )
        )
        return branch

    for p in range(2):
        wait_all(xrows.at[pl.ds(1, nx - 1), pl.ds(p * half, half)], x_r.at[p])
        for q in range(nx):
            rowsf[q] = xrows[q, p * half : (p + 1) * half].reshape(half * msg, LANES).astype(F32)
        piece = lambda q, cc: rowsf[q, pl.ds(cc, nrows, stride=ch), :]
        squares = jnp.zeros((nrows, LANES), F32)
        for q in range(nx):
            for cc in range(ch):
                v = piece(q, cc)
                squares = squares + v * v
        inv = lax.rsqrt(jnp.sum(squares, axis=1, keepdims=True) / width + EPS)
        gu = jnp.zeros((nrows, 2 * he), F32)
        for q in range(nx):
            left = jnp.concatenate(
                [
                    piece(q, cc) * inv * fgain[:, q * qc + cc * LANES : q * qc + (cc + 1) * LANES]
                    for cc in range(ch)
                ],
                axis=1,
            ).astype(BF)
            gu = gu + jnp.dot(left, egu[q * qc : (q + 1) * qc, :], preferred_element_type=F32)
        act_all[p, 0] = (silu(gu[:, 0:he]) * gu[:, he:]).astype(BF)
        for d in peers:
            rcopy(act_all.at[p, 0], act_all.at[p, d], a_s, a_r.at[p], e, xdev(d))

    wait_all(dbuf.at[pl.ds(1, nx - 1)], ed_r)
    for p in range(2):
        eout = jnp.dot(act_all[p, 0], dsrc[x], preferred_element_type=F32)
        wait_all(act_all.at[p, pl.ds(1, nx - 1)], a_r.at[p])
        for d in range(1, nx):
            eout = eout + jnp.dot(act_all[p, d], dbuf[d], preferred_element_type=F32)
        for cc in range(ch):
            outf[pl.ds(cc, nrows, stride=ch), :] = eout[:, cc * LANES : (cc + 1) * LANES]
        rsend[p * half : (p + 1) * half] = outf[...].astype(BF).reshape(half, msg, LANES)
        for dz in ARRIVAL[::-1]:
            for d in range(YC):
                if part_of(dz) == p and (dz or d):
                    rcopy(rsend.at[place_of[dz] + d], rrecv.at[e], r_s, r_r, zback[dz] + yback[d], x)
    rrecv[e] = rsend[0]
    branch = dense_branch()
    shared = sh_send[x].astype(F32)
    wait_all(sh_rec.at[pl.ds(1, nx - 1)], h_r)
    for d in range(1, nx):
        shared = shared + sh_rec[d].astype(F32)
    base = mine.astype(F32)
    base = base + jnp.concatenate([branch] * ch, axis=0) * shared
    wait_all(rrecv.at[pl.ds(0, EP - 1)], r_r)
    got = jnp.dot(pick, rrecv[...].reshape(rows_all, LANES), preferred_element_type=F32) * scale_col
    for k in range(topk):
        base = base + got[k * wide : (k + 1) * wide]
    fin[x] = base.astype(BF)
    for d in peers:
        rcopy(fin.at[x], fin.at[x], f_s, f_r, e, xdev(d))
    wait_all(fin.at[pl.ds(0, nx - 1)], f_r)
    for i in range(nx * ch):
        out_ref[:, i * LANES : (i + 1) * LANES] = fin[i // ch, (i % ch) * seqs : (i % ch + 1) * seqs, :]

    some = lambda ref, n: ref.at[pl.ds(0, n)]
    for ref, sem in (
        (some(tokbuf, NZ - 1), t_s), (some(wbuf, 2 * NY - 1), w_s), (some(gbuf, 2 * NY - 1), gw_s),
        (some(psend, NZ - 1), p_s), (some(gsend, NZ - 1), g_s), (some(obuf, EP - 1), o_s),
        (some(sbuf, EP - 1), s_s), (some(mix_rec, nx - 1), m_s), (some(dsrc, nx - 1), ed_s),
        (some(dsend, EP - 1), d_s), (some(xrows, nx - 1), x_s), (act_all.at[:, pl.ds(1, nx - 1)], a_s),
        (some(rsend, EP - 1), r_s), (some(sh_send, nx - 1), h_s), (some(fin, nx - 1), f_s), (some(res_all, nx - 1), n_s),
    ):
        wait_all(ref, sem)


def layer(*args):
    (tokens, norm_gain, wq, wk, wv, wg, bw, dw, rate, bias, head_gain, rec, ow, ffn_gain, routes, rweight,
     eg, eu, ed, sg, su, sd, branch_gate) = args
    nx = lax.axis_size("tp")
    seqs, width = tokens.shape
    heads, dk, dv = rec.shape[1:]
    cols = wq.shape[1] + wk.shape[1] + wv.shape[1] + wg.shape[1]
    rows = wq.shape[0]
    kz = rows * YC
    khs = wq.shape[1] // dk
    topk = routes.shape[1]
    qc = width // nx
    ch = qc // LANES
    he = eg.shape[2]
    hs = sg.shape[1]
    msg = SLOTS * ch
    wide = ch * seqs
    hbm = pl.BlockSpec(memory_space=pltpu.HBM)
    vmem = pl.BlockSpec(memory_space=pltpu.VMEM)
    dma = pltpu.SemaphoreType.DMA
    V = pltpu.VMEM
    return pl.pallas_call(
        layer_kernel,
        out_shape=(
            jax.ShapeDtypeStruct((seqs, width), BF),
            pltpu.VMEM(rec.shape, F32),
        ),
        in_specs=[hbm] * 23,
        out_specs=(vmem,) * 2,
        scratch_shapes=[
            V((seqs, width), BF), V((width,), BF), V(bw.shape[::-1], BF), V(dw.shape[::-1], BF),
            pltpu.SMEM((heads,), F32), pltpu.SMEM((heads,), F32), V((dv,), BF), V((width,), BF),
            V((topk, seqs), I32), V((topk, seqs), F32), V((width,), BF),
            V((YC, rows, cols - wg.shape[1]), BF), V((YC, rows, wg.shape[1]), BF), V((NZ, seqs, kz), BF), V((NZ, seqs, kz), BF),
            V((NZ, seqs, cols - wg.shape[1]), BF), V((NZ, seqs, cols - wg.shape[1]), BF),
            V((NZ, seqs, wg.shape[1]), BF), V((NZ, seqs, wg.shape[1]), BF),
            V((EP, ow.shape[1], ow.shape[0]), BF), V((EP, sg.shape[0], 3 * hs), BF),
            V((nx, seqs, qc), BF), V((nx, seqs, qc), BF),
            V((2 * khs * dk, 3 * seqs), BF), V((heads, seqs, dv), F32),
            V((seqs, LANES), F32), V((heads, seqs, dv), F32), V((heads, seqs, dv), F32),
            V((width, 2 * he), BF), V((nx, he, qc), BF), V((nx, he, qc), BF),
            V((nx * ch, seqs, LANES), BF), V((nx, wide, LANES), BF),
            V((EP, msg, LANES), BF), V((nx, EP, msg, LANES), BF), V((nx, EP * msg // 2, LANES), F32),
            V((2, nx, EP * SLOTS // 2, he), BF), V((EP * msg // 2, LANES), F32),
            V((EP, msg, LANES), BF), V((EP, msg, LANES), BF),
            V((nx, wide, LANES), BF), V((nx, wide, LANES), BF), V((nx, wide, LANES), BF),
            dma((18,)), dma((NY,)), dma((NY,)), dma((4,)), dma((4,)), dma((4,)), dma((4,)), dma((NZ,)),
            dma((2,)), dma((2,)), *[dma] * 29,
        ],
        compiler_params=pltpu.CompilerParams(
            collective_id=1, has_side_effects=True, vmem_limit_bytes=LAYER_VMEM
        ),
        name="layer",
    )(
        *(
            pltpu.with_memory_space_constraint(a, pltpu.HBM)
            for a in (
                tokens, norm_gain, wq, wk, wv, wg, bw.T, dw.T, rate, bias, head_gain, rec, ow.T, ffn_gain,
                routes.T, rweight.T, eg, eu, ed, sg, su, sd.T, branch_gate,
            )
        )
    )


def store_kernel(layer_in, state, layer_out, new, sems):
    n = state.shape[0] // STATE_COPIES
    copies = [
        pltpu.make_async_copy(
            state.at[pl.ds(i * n, n)], new.at[pl.ds(i * n, n)], sems.at[i]
        )
        for i in range(STATE_COPIES)
    ]
    copies.append(pltpu.make_async_copy(layer_in, layer_out, sems.at[STATE_COPIES]))
    for cp in copies:
        cp.start()
    for cp in copies:
        cp.wait()


def per_device(*args):
    layer_out, state = layer(*args)
    hbm = pl.BlockSpec(memory_space=pltpu.HBM)
    vmem = pl.BlockSpec(memory_space=pltpu.VMEM)
    return pl.pallas_call(
        store_kernel,
        out_shape=(
            jax.ShapeDtypeStruct(layer_out.shape, BF),
            jax.ShapeDtypeStruct(state.shape, F32),
        ),
        in_specs=[vmem, vmem],
        out_specs=(hbm, hbm),
        scratch_shapes=[pltpu.SemaphoreType.DMA((STATE_COPIES + 1,))],
        compiler_params=pltpu.CompilerParams(vmem_limit_bytes=8 * 1024 * 1024),
        name="store",
    )(layer_out, pltpu.with_memory_space_constraint(state, pltpu.VMEM))


def solution(mesh):
    return jax.shard_map(
        per_device,
        mesh=mesh,
        in_specs=(
            P("ep", None),
            P(),
            P("ep", "tp"),
            P("ep", "tp"),
            P("ep", "tp"),
            P("ep", "tp"),
            P(),
            P(),
            P("tp"),
            P("tp"),
            P(),
            P("ep", "tp", None, None),
            P("tp", "ep"),
            P(),
            P("ep", None),
            P("ep", None),
            P("ep", None, "tp"),
            P("ep", None, "tp"),
            P("ep", "tp", None),
            P("ep", "tp"),
            P("ep", "tp"),
            P("tp", "ep"),
            P(),
        ),
        out_specs=(P("ep", None), P("ep", "tp", None, None)),
        check_vma=False,
    )
```

```python
import jax
import jax.numpy as jnp
from jax import lax
from jax.experimental import pallas as pl
from jax.experimental.pallas import tpu as pltpu
from jax.sharding import PartitionSpec as P

EPS = 1e-06
ROUTED_SCALE = 2.5
NZ, NY, NC = 8, 4, 2
YC = NY * NC
EP = NZ * YC
SLOTS = 2
UNROLL = 2
STATE_COPIES = 8
FAR = (4, 3, 5, 2, 6, 1, 7)
NEAR = (1, 7, 2, 6, 3, 5, 4)
GROUPS = ((0,), (1, 7), (2, 6), (3, 5, 4))
PAIRS = ((0,), (7, 1), (6,), (2, 5), (3, 4))
ARRIVAL = tuple(d for g in PAIRS for d in g)
PAIR = {d: i for i, g in enumerate(PAIRS) for d in g}
NEAR_Z = 5
GROUP = {d: i for i, g in enumerate(GROUPS) for d in g}
LAYER_VMEM = 40 * 1024 * 1024
LANES = 128
MESH = pl.DeviceIdType.MESH
BF = jnp.bfloat16
F32 = jnp.float32
I32 = jnp.int32


def silu(v):
    return v / (1.0 + jnp.exp(-v))


def sigmoid(v):
    return 1.0 / (1.0 + jnp.exp(-v))


def rms(values, gain):
    return values * lax.rsqrt(jnp.mean(values * values, axis=-1, keepdims=True) + EPS) * gain


def unit(v):
    return v * lax.rsqrt(jnp.sum(v * v, axis=-1, keepdims=True) + EPS)


def iota(shape, dim):
    return lax.broadcasted_iota(I32, shape, dim)


def nt_dot(a, b):
    return lax.dot_general(a, b, (((1,), (1,)), ((), ())), preferred_element_type=F32)


def layer_kernel(
    tokens_h, norm_gain_h, wq, wk, wv, wg, bw_h, dw_h, rate_h, bias_h, head_gain_h, rec, ow_h, ffn_gain_h,
    routes_h, rweight_h, eg_h, eu_h, ed_h, sg_h, su_h, sd_h, branch_h,
    out_ref, state,
    tokens, norm_gain, bw, dw, rate, bias, head_gain, ffn_gain, routes, rweight, branch_gate,
    wbuf, gbuf, tok_src, tokbuf, psend, prec, gsend, grec, obuf, sbuf, mix_send, mix_rec,
    kqt, vals, rs_ref, ro, corr,
    egu, dsrc, dbuf, tok_chunks, res_all, dsend, xrows, rowsf, act_all, outf, rsend, rrecv, sh_send, sh_rec, fin,
    load_sem, o1_r, o2_r, s1_r, s2_r, o3_r, d_r,
    x_r, a_r, t_r, wf_r, gf_r, p_r, g_r, w_r, gw_r, s3_r, m_r, ed_r, r_r, h_r, f_r, n_r,
    t_s, w_s, gw_s, p_s, g_s, o_s, s_s, m_s, ed_s, d_s, x_s, a_s, r_s, h_s, f_s, n_s,
):
    e = lax.axis_index("ep")
    x = lax.axis_index("tp")
    nx = lax.axis_size("tp")
    z, yc = lax.div(e, YC), lax.rem(e, YC)
    y, c = lax.div(yc, NC), lax.rem(yc, NC)
    partner = e + 1 - 2 * c
    zdev = lambda d: lax.rem(z + d, NZ) * YC + yc
    ydev = lambda d: z * YC + lax.rem(y + d, NY) * NC + c
    xdev = lambda d: lax.rem(x + d, nx)
    peers = sorted(range(1, nx), key=lambda d: -min(d, nx - d))
    ypeers = sorted(range(1, NY), key=lambda d: -min(d, NY - d))
    seqs, width = tokens.shape
    heads, dk, dv = rec.shape[1:]

    def wait_all(ref, sem):
        pltpu.make_async_copy(ref, ref, sem).wait()

    def rcopy(src, dst, ss, rs, ep, tp):
        cp = pltpu.make_async_remote_copy(
            src_ref=src, dst_ref=dst, send_sem=ss, recv_sem=rs, device_id=(ep, tp), device_id_type=MESH
        )
        cp.start()
        return cp

    count = [0]

    def load(*pairs):
        sem = load_sem.at[count[0]]
        count[0] += 1
        for src, dst in pairs:
            pltpu.make_async_copy(src, dst, sem).start()
        return sem

    cuts = [0]
    for w in (wq, wk, wv):
        cuts.append(cuts[-1] + w.shape[1])
    w_load = load(*((w, wbuf.at[yc, :, cuts[i] : cuts[i + 1]]) for i, w in enumerate((wq, wk, wv))))
    first = [(a, load((b, a))) for a, b in ((tokens, tokens_h), (norm_gain, norm_gain_h))]
    g_load = load((wg, gbuf.at[yc]))
    o_load = load((ow_h, obuf.at[e]))
    qc = width // nx
    ed_load = load(*((ed_h.at[0, :, q * qc : (q + 1) * qc], dsrc.at[q]) for q in range(nx)))
    small = [
        (b, load((a, b)))
        for a, b in (
            (bw_h, bw), (dw_h, dw), (rate_h, rate), (bias_h, bias), (head_gain_h, head_gain),
            (ffn_gain_h, ffn_gain), (routes_h, routes), (rweight_h, rweight), (branch_h, branch_gate),
        )
    ]
    hs = sg_h.shape[1]
    s_load = load(
        *((a, sbuf.at[e, :, i * hs : (i + 1) * hs]) for i, a in enumerate((sg_h, su_h, sd_h)))
    )
    state_load = load((rec, state))
    he = eg_h.shape[2]
    e_load = load((eg_h.at[0], egu.at[:, 0:he]), (eu_h.at[0], egu.at[:, he : 2 * he]))

    barrier = pltpu.get_barrier_semaphore()
    zbase = [lax.rem(z + d, NZ) * YC for d in range(NZ)]
    ypart = [lax.rem(yc + d, YC) for d in range(YC)]
    for dz in (4, 3, 5, 2, 6, 1, 7):
        pl.semaphore_signal(barrier, inc=1, device_id=(zbase[dz] + yc, x), device_id_type=MESH)
    for d in range(1, YC):
        pl.semaphore_signal(barrier, inc=1, device_id=(zbase[0] + ypart[d], x), device_id_type=MESH)
    for d in range(1, nx):
        pl.semaphore_signal(barrier, inc=1, device_id=(e, xdev(d)), device_id_type=MESH)

    def rows_y(buf, ss, rs, fr):
        for d in ypeers:
            rcopy(buf.at[yc], buf.at[yc], ss, rs, ydev(d), x)
        rcopy(buf.at[yc], buf.at[yc], ss, fr, partner, x)

    def rows_c(buf, ss, rs, fr):
        wait_all(buf.at[pl.ds(0, NY - 1)], rs)
        for d in range(1, NY):
            j = lax.rem(y + NY - d, NY) * NC + c
            rcopy(buf.at[j], buf.at[j], ss, fr, partner, x)

    wait_all(wbuf.at[yc], w_load)
    pl.semaphore_wait(barrier, (NZ - 1) + (YC - 1) + (nx - 1))
    rows_y(wbuf, w_s, w_r, wf_r)
    for ref, sem in first:
        wait_all(ref, sem)
    normed = rms(tokens[...].astype(F32), norm_gain[...].reshape(1, width).astype(F32)).astype(BF)
    kz = tokbuf.shape[2]
    for i in range(NZ):
        tok_src[i] = normed[:, i * kz : (i + 1) * kz]
    for d in FAR:
        rcopy(tok_src.at[lax.rem(z + d, NZ)], tokbuf.at[d], t_s, t_r, zdev(d), x)
    wait_all(gbuf.at[yc], g_load)
    rows_y(gbuf, gw_s, gw_r, gf_r)
    wait_all(obuf.at[e], o_load)
    wait_all(dsrc, ed_load)

    def spread_z(buf, ss, rs):
        for d in NEAR:
            rcopy(buf.at[e], buf.at[e], ss, rs.at[GROUP[d]], zdev(d), x)

    def z_blocks(which):
        return [lax.rem(z + NZ - d, NZ) * YC for d in which]

    def spread_y(buf, group, ss, rs, fr):
        for zb in z_blocks(GROUPS[group]):
            j = zb + yc
            for dy in ypeers:
                rcopy(buf.at[j], buf.at[j], ss, rs.at[group], ydev(dy), x)
            rcopy(buf.at[j], buf.at[j], ss, fr(group), partner, x)

    def spread_c(buf, group, ss, rs, fr):
        wait_all(buf.at[pl.ds(0, len(GROUPS[group]) * (NY - 1))], rs.at[group])
        for zb in z_blocks(GROUPS[group]):
            for dy in range(1, NY):
                j = zb + lax.rem(y + NY - dy, NY) * NC + c
                rcopy(buf.at[j], buf.at[j], ss, fr(group), partner, x)

    last_o = lambda group: o3_r.at[1 if group == 3 else 0]
    last_s = lambda group: s3_r
    spread_z(obuf, o_s, o1_r)
    spread_y(obuf, 0, o_s, o2_r, last_o)
    for d in peers:
        rcopy(dsrc.at[xdev(d)], dbuf.at[d], ed_s, ed_r, e, xdev(d))
    tokbuf[0] = tok_src[z]

    for ref, sem in small:
        wait_all(ref, sem)
    bl = nt_dot(normed, bw[...])
    dl = nt_dot(normed, dw[...])
    lanes = iota(bl.shape, 1)
    retain, strength = [], []
    for h in range(heads):
        mine = lanes == x * heads + h
        b = jnp.sum(jnp.where(mine, bl, 0.0), axis=1, keepdims=True)
        g = jnp.sum(jnp.where(mine, dl, 0.0), axis=1, keepdims=True) + bias[h]
        soft = jnp.maximum(g, 0.0) + jnp.log1p(jnp.exp(-jnp.abs(g)))
        strength.append(sigmoid(b))
        retain.append(jnp.exp(-rate[h] * soft))
    lane = iota(rs_ref.shape, 1)
    packed = jnp.zeros(rs_ref.shape, F32)
    for h in range(heads):
        packed = jnp.where(lane == h, retain[h], packed)
        packed = jnp.where(lane == heads + h, strength[h], packed)

    rows_c(wbuf, w_s, w_r, wf_r)
    wait_all(obuf.at[pl.ds(0, len(GROUPS[1]))], o1_r.at[1])
    spread_y(obuf, 1, o_s, o2_r, last_o)
    wait_all(tokbuf.at[pl.ds(1, NZ - 1)], t_r)
    wait_all(wbuf.at[pl.ds(0, NY)], wf_r)
    toks_all = tokbuf[...].reshape(NZ * seqs, kz)

    def project(buf, sent, got, ss, rs):
        n = buf.shape[2]
        sent[...] = (
            jnp.dot(toks_all, buf[...].reshape(kz, n), preferred_element_type=F32)
            .astype(BF)
            .reshape(NZ, seqs, n)
        )
        for d in FAR:
            rcopy(sent.at[d], got.at[d], ss, rs, zdev(NZ - d), x)

    def collected(sent, got, rs):
        wait_all(got.at[pl.ds(1, NZ - 1)], rs)
        total = sent[0].astype(F32)
        for d in range(1, NZ):
            total = total + got[d].astype(F32)
        return total.astype(BF).astype(F32)

    project(wbuf, psend, prec, p_s, p_r)
    rows_c(gbuf, gw_s, gw_r, gf_r)
    wait_all(obuf.at[pl.ds(0, len(GROUPS[2]))], o1_r.at[2])
    spread_y(obuf, 2, o_s, o2_r, last_o)
    wait_all(gbuf.at[pl.ds(0, NY)], gf_r)
    project(gbuf, gsend, grec, g_s, g_r)
    wait_all(obuf.at[pl.ds(0, len(GROUPS[3]))], o1_r.at[3])
    spread_y(obuf, 3, o_s, o2_r, last_o)
    wait_all(sbuf.at[e], s_load)
    spread_z(sbuf, s_s, s1_r)

    def s_relay(group):
        if group:
            wait_all(sbuf.at[pl.ds(0, len(GROUPS[group]))], s1_r.at[group])
        spread_y(sbuf, group, s_s, s2_r, last_s)


    ch = qc // LANES
    for i in range(nx * ch):
        tok_chunks[i] = tokens[:, i * LANES : (i + 1) * LANES]
    topk = routes.shape[0]
    rrow = [routes[k : k + 1, :] for k in range(topk)]
    square = (seqs, seqs)
    diag = iota(square, 0) == iota(square, 1)
    upright = lambda row, zero: jnp.sum(
        jnp.where(diag, jnp.broadcast_to(row, square), zero), axis=1, keepdims=True
    )
    rcol = [upright(r.astype(F32), 0.0) for r in rrow]
    rrow = [r.astype(F32) for r in rrow]
    before_c = iota(square, 1) < iota(square, 0)
    before_r = iota(square, 0) < iota(square, 1)
    tcol, trow = [], []
    for k in range(topk):
        hits_c = jnp.zeros(square, F32)
        hits_r = jnp.zeros(square, F32)
        for k2 in range(topk):
            hits_c += jnp.where(before_c & (rcol[k] == rrow[k2]), 1.0, 0.0)
            hits_r += jnp.where(before_r & (rrow[k] == rcol[k2]), 1.0, 0.0)
        tcol.append(rcol[k] * SLOTS + jnp.sum(hits_c, axis=1, keepdims=True))
        trow.append(rrow[k] * SLOTS + jnp.sum(hits_r, axis=0, keepdims=True))
    wide = ch * seqs
    spreadm = (iota((seqs, wide), 1) % seqs == iota((seqs, wide), 0)).astype(BF)
    rows_all = EP * SLOTS * ch
    rid = iota((rows_all, wide), 0)
    okc = rid % ch == iota((rows_all, wide), 1) // seqs
    ridf = (rid // ch).astype(F32)
    place = jnp.zeros((rows_all, wide), F32)
    for k in range(topk):
        tw = jnp.dot(
            jnp.broadcast_to(trow[k], (8, seqs)).astype(BF), spreadm, preferred_element_type=F32
        )[0:1, :]
        place = jnp.where(okc & (ridf == tw), 1.0, place)
    place = place.astype(BF)
    rw = [rweight[k : k + 1, :] for k in range(topk)]
    rsum = rw[0]
    for k in range(1, topk):
        rsum = rsum + rw[k]
    scol = [upright(rw[k] / rsum * ROUTED_SCALE, 0.0) for k in range(topk)]
    pick_col = jnp.concatenate([tcol[k] * ch + cc for k in range(topk) for cc in range(ch)], axis=0)
    scale_col = jnp.concatenate([scol[k] for k in range(topk) for cc in range(ch)], axis=0)
    pick = (
        jnp.broadcast_to(pick_col, (topk * wide, rows_all))
        == iota((topk * wide, rows_all), 1).astype(F32)
    ).astype(BF)

    proj = collected(psend, prec, p_r)
    for group in range(3):
        spread_c(obuf, group, o_s, o2_r, last_o)
    khs = wq.shape[1] // dk
    per = heads // khs
    kq = []

    def split(i, t):
        hi = t.astype(BF)
        mid = (t - hi.astype(F32)).astype(BF)
        lo = (t - hi.astype(F32) - mid.astype(F32)).astype(BF)
        kqt[i * dk : (i + 1) * dk, :] = jnp.concatenate([hi, mid, lo], axis=1)

    for i in range(khs):
        q = unit(silu(proj[:, i * dk : (i + 1) * dk])) * dk ** (-0.5)
        k = unit(silu(proj[:, (khs + i) * dk : (khs + i + 1) * dk]))
        split(i, k.T)
        split(khs + i, q.T)
        kq.append(jnp.sum(k * q, axis=1, keepdims=True))
    for i in range(khs):
        packed = jnp.where(lane == 2 * heads + i, kq[i], packed)
    rs_ref[...] = packed
    vbase = 2 * khs * dk
    for h in range(heads):
        vals[h] = silu(proj[:, vbase + h * dv : vbase + (h + 1) * dv])
    wait_all(state, state_load)

    span = 2 * dv

    def spread_columns(first, rows):
        shape = (kqt.shape[1], span)
        hot = (lax.rem(iota(shape, 0), seqs) == first + iota(shape, 1) // dv).astype(BF)
        return jnp.dot(kqt[0:rows, :], hot, preferred_element_type=F32)

    def read_pair(p, carry):
        both = spread_columns(2 * p, 2 * khs * dk)
        for j in range(2):
            s = 2 * p + j
            wide_cols = both[:, j * dv : (j + 1) * dv]
            rowrs = rs_ref[pl.ds(s, 1), :]
            for i in range(khs):
                kcol = wide_cols[i * dk : (i + 1) * dk]
                qcol = wide_cols[(khs + i) * dk : (khs + i + 1) * dk]
                dotkq = rowrs[:, 2 * heads + i : 2 * heads + i + 1]
                for h in range(i * per, (i + 1) * per):
                    st = state[s, h]
                    ret = rowrs[:, h : h + 1]
                    pred = jnp.sum(st * kcol, axis=0, keepdims=True) * ret
                    base = jnp.sum(st * qcol, axis=0, keepdims=True) * ret
                    cor = rowrs[:, heads + h : heads + h + 1] * (vals[h, pl.ds(s, 1), :] - pred)
                    corr[h, pl.ds(s, 1), :] = cor
                    ro[h, pl.ds(s, 1), :] = base + dotkq * cor
        return carry

    lax.fori_loop(0, seqs // 2, read_pair, 0, unroll=UNROLL)

    spread_c(obuf, 3, o_s, o2_r, last_o)
    gate = collected(gsend, grec, g_r)
    hg = head_gain[...].reshape(1, dv).astype(F32)
    parts = [rms(ro[h], hg) * silu(gate[:, h * dv : (h + 1) * dv]) for h in range(heads)]
    heads_out = jnp.concatenate(parts, axis=1).astype(BF)
    def project_out(which):
        for zb in z_blocks(which):
            zi = lax.div(zb, YC)
            mix_send[zi] = nt_dot(
                heads_out, obuf[pl.ds(zb, YC)].reshape(YC * obuf.shape[1], heads * dv)
            ).astype(BF)

    wait_all(obuf.at[pl.ds(0, NEAR_Z * NY)], o3_r.at[0])
    project_out([d for g in GROUPS[:3] for d in g])
    wait_all(obuf.at[pl.ds(0, (NZ - NEAR_Z) * NY)], o3_r.at[1])
    project_out(GROUPS[3])
    zq = NZ // nx
    for d in peers:
        q = xdev(d)
        rcopy(mix_send.at[pl.ds(q * zq, zq)], mix_rec.at[d], m_s, m_r, e, q)
    def write_pair(p, carry):
        both = spread_columns(2 * p, khs * dk)
        for j in range(2):
            s = 2 * p + j
            rowrs = rs_ref[pl.ds(s, 1), :]
            for i in range(khs):
                kcol = both[i * dk : (i + 1) * dk, j * dv : (j + 1) * dv]
                for h in range(i * per, (i + 1) * per):
                    state[s, h] = state[s, h] * rowrs[:, h : h + 1] + kcol * corr[h, pl.ds(s, 1), :]
        return carry

    lax.fori_loop(0, seqs // 2, write_pair, 0, unroll=UNROLL)
    s_relay(0)
    s_relay(1)
    wait_all(mix_rec.at[pl.ds(1, nx - 1)], m_r)
    mixed = mix_send[pl.ds(x * zq, zq)].astype(F32)
    for d in range(1, nx):
        mixed = mixed + mix_rec[d].astype(F32)
    mixed = jnp.concatenate([mixed[i] for i in range(zq)], axis=1)
    own = tok_chunks[pl.ds(x * ch, ch)].astype(F32)
    mine = jnp.concatenate(
        [own[cc] + mixed[:, cc * LANES : (cc + 1) * LANES] for cc in range(ch)], axis=0
    ).astype(BF)
    res_all[x] = mine
    msg = SLOTS * ch
    dsend[...] = (
        jnp.dot(place, mine, preferred_element_type=F32).astype(BF).reshape(EP, msg, LANES)
    )

    zback = [lax.rem(z + NZ - d, NZ) * YC for d in range(NZ)]
    yback = [lax.rem(yc + YC - d, YC) for d in range(YC)]
    place_of = {dz: i * YC for i, dz in enumerate(ARRIVAL)}
    half = EP // 2
    part_of = lambda dz: place_of[dz] // half
    for dz in ARRIVAL:
        for d in range(YC):
            if dz or d:
                to = zbase[dz] + ypart[d]
                rcopy(dsend.at[to], xrows.at[x, place_of[dz] + d], d_s, d_r.at[PAIR[dz]], to, x)
    xrows[x, 0] = dsend[e]
    for d in peers:
        rcopy(res_all.at[x], res_all.at[x], n_s, n_r, e, xdev(d))
    for i, group in enumerate(PAIRS):
        n = len(group) * YC - (0 in group)
        at = pl.ds(place_of[group[0]], len(group) * YC)
        wait_all(xrows.at[x, pl.ds(place_of[group[0]], n)], d_r.at[i])
        for d in peers:
            block = xrows.at[x, at]
            rcopy(block, block, x_s, x_r.at[part_of(group[0])], e, xdev(d))
    s_relay(2)
    s_relay(3)
    for group in (0, 1):
        spread_c(sbuf, group, s_s, s2_r, last_s)
    wait_all(egu, e_load)
    fgain = ffn_gain[...].reshape(1, width).astype(F32)
    nrows = half * SLOTS

    def full_rows():
        wait_all(res_all.at[pl.ds(0, nx - 1)], n_r)
        residual = jnp.concatenate(
            [res_all[i // ch, (i % ch) * seqs : (i % ch + 1) * seqs, :] for i in range(nx * ch)], axis=1
        ).astype(F32)
        ffn_in = rms(residual, fgain).astype(BF)
        branch = sigmoid(
            jnp.sum(
                ffn_in.astype(F32) * branch_gate[...].reshape(1, width).astype(F32), axis=1, keepdims=True
            )
        )
        return ffn_in, branch

    for p in range(2):
        wait_all(xrows.at[pl.ds(1, nx - 1), pl.ds(p * half, half)], x_r.at[p])
        for q in range(nx):
            rowsf[q] = xrows[q, p * half : (p + 1) * half].reshape(half * msg, LANES).astype(F32)
        piece = lambda q, cc: rowsf[q, pl.ds(cc, nrows, stride=ch), :]
        squares = jnp.zeros((nrows, LANES), F32)
        for q in range(nx):
            for cc in range(ch):
                v = piece(q, cc)
                squares = squares + v * v
        inv = lax.rsqrt(jnp.sum(squares, axis=1, keepdims=True) / width + EPS)
        gu = jnp.zeros((nrows, 2 * he), F32)
        for q in range(nx):
            left = jnp.concatenate(
                [
                    piece(q, cc) * inv * fgain[:, q * qc + cc * LANES : q * qc + (cc + 1) * LANES]
                    for cc in range(ch)
                ],
                axis=1,
            ).astype(BF)
            gu = gu + jnp.dot(left, egu[q * qc : (q + 1) * qc, :], preferred_element_type=F32)
        act_all[p, 0] = (silu(gu[:, 0:he]) * gu[:, he:]).astype(BF)
        for d in peers:
            rcopy(act_all.at[p, 0], act_all.at[p, d], a_s, a_r.at[p], e, xdev(d))

    wait_all(dbuf.at[pl.ds(1, nx - 1)], ed_r)
    for p in range(2):
        if p == 1:
            spread_c(sbuf, 2, s_s, s2_r, last_s)
            ffn_in, branch = full_rows()
        eout = jnp.dot(act_all[p, 0], dsrc[x], preferred_element_type=F32)
        wait_all(act_all.at[p, pl.ds(1, nx - 1)], a_r.at[p])
        for d in range(1, nx):
            eout = eout + jnp.dot(act_all[p, d], dbuf[d], preferred_element_type=F32)
        for cc in range(ch):
            outf[pl.ds(cc, nrows, stride=ch), :] = eout[:, cc * LANES : (cc + 1) * LANES]
        rsend[p * half : (p + 1) * half] = outf[...].astype(BF).reshape(half, msg, LANES)
        for dz in ARRIVAL[::-1]:
            for d in range(YC):
                if part_of(dz) == p and (dz or d):
                    rcopy(rsend.at[place_of[dz] + d], rrecv.at[e], r_s, r_r, zback[dz] + yback[d], x)
    rrecv[e] = rsend[0]
    spread_c(sbuf, 3, s_s, s2_r, last_s)
    wait_all(sbuf.at[pl.ds(0, EP // NC)], s3_r)
    sgu = jnp.dot(ffn_in, sbuf[:, :, 0 : 2 * hs].reshape(width, 2 * hs), preferred_element_type=F32)
    sact = (silu(sgu[:, 0:hs]) * sgu[:, hs:]).astype(BF)
    spart = nt_dot(sact, sbuf[:, :, 2 * hs :].reshape(width, hs)).astype(BF)
    for i in range(nx * ch):
        sh_send[i // ch, (i % ch) * seqs : (i % ch + 1) * seqs, :] = spart[:, i * LANES : (i + 1) * LANES]
    for d in peers:
        rcopy(sh_send.at[xdev(d)], sh_rec.at[d], h_s, h_r, e, xdev(d))
    shared = sh_send[x].astype(F32)
    wait_all(sh_rec.at[pl.ds(1, nx - 1)], h_r)
    for d in range(1, nx):
        shared = shared + sh_rec[d].astype(F32)
    base = mine.astype(F32)
    base = base + jnp.concatenate([branch] * ch, axis=0) * shared
    wait_all(rrecv.at[pl.ds(0, EP - 1)], r_r)
    got = jnp.dot(pick, rrecv[...].reshape(rows_all, LANES), preferred_element_type=F32) * scale_col
    for k in range(topk):
        base = base + got[k * wide : (k + 1) * wide]
    fin[x] = base.astype(BF)
    for d in peers:
        rcopy(fin.at[x], fin.at[x], f_s, f_r, e, xdev(d))
    wait_all(fin.at[pl.ds(0, nx - 1)], f_r)
    for i in range(nx * ch):
        out_ref[:, i * LANES : (i + 1) * LANES] = fin[i // ch, (i % ch) * seqs : (i % ch + 1) * seqs, :]

    some = lambda ref, n: ref.at[pl.ds(0, n)]
    for ref, sem in (
        (some(tokbuf, NZ - 1), t_s), (some(wbuf, 2 * NY - 1), w_s), (some(gbuf, 2 * NY - 1), gw_s),
        (some(psend, NZ - 1), p_s), (some(gsend, NZ - 1), g_s), (some(obuf, EP - 1), o_s),
        (some(sbuf, EP - 1), s_s), (some(mix_rec, nx - 1), m_s), (some(dsrc, nx - 1), ed_s),
        (some(dsend, EP - 1), d_s), (some(xrows, nx - 1), x_s), (act_all.at[:, pl.ds(1, nx - 1)], a_s),
        (some(rsend, EP - 1), r_s), (some(sh_send, nx - 1), h_s), (some(fin, nx - 1), f_s), (some(res_all, nx - 1), n_s),
    ):
        wait_all(ref, sem)


def layer(*args):
    (tokens, norm_gain, wq, wk, wv, wg, bw, dw, rate, bias, head_gain, rec, ow, ffn_gain, routes, rweight,
     eg, eu, ed, sg, su, sd, branch_gate) = args
    nx = lax.axis_size("tp")
    seqs, width = tokens.shape
    heads, dk, dv = rec.shape[1:]
    cols = wq.shape[1] + wk.shape[1] + wv.shape[1] + wg.shape[1]
    rows = wq.shape[0]
    kz = rows * YC
    khs = wq.shape[1] // dk
    topk = routes.shape[1]
    qc = width // nx
    ch = qc // LANES
    he = eg.shape[2]
    hs = sg.shape[1]
    msg = SLOTS * ch
    wide = ch * seqs
    hbm = pl.BlockSpec(memory_space=pltpu.HBM)
    vmem = pl.BlockSpec(memory_space=pltpu.VMEM)
    dma = pltpu.SemaphoreType.DMA
    V = pltpu.VMEM
    return pl.pallas_call(
        layer_kernel,
        out_shape=(
            jax.ShapeDtypeStruct((seqs, width), BF),
            pltpu.VMEM(rec.shape, F32),
        ),
        in_specs=[hbm] * 23,
        out_specs=(vmem,) * 2,
        scratch_shapes=[
            V((seqs, width), BF), V((width,), BF), V(bw.shape[::-1], BF), V(dw.shape[::-1], BF),
            pltpu.SMEM((heads,), F32), pltpu.SMEM((heads,), F32), V((dv,), BF), V((width,), BF),
            V((topk, seqs), I32), V((topk, seqs), F32), V((width,), BF),
            V((YC, rows, cols - wg.shape[1]), BF), V((YC, rows, wg.shape[1]), BF), V((NZ, seqs, kz), BF), V((NZ, seqs, kz), BF),
            V((NZ, seqs, cols - wg.shape[1]), BF), V((NZ, seqs, cols - wg.shape[1]), BF),
            V((NZ, seqs, wg.shape[1]), BF), V((NZ, seqs, wg.shape[1]), BF),
            V((EP, ow.shape[1], ow.shape[0]), BF), V((EP, sg.shape[0], 3 * hs), BF),
            V((NZ, seqs, width // NZ), BF), V((nx, NZ // nx, seqs, width // NZ), BF),
            V((2 * khs * dk, 3 * seqs), BF), V((heads, seqs, dv), F32),
            V((seqs, LANES), F32), V((heads, seqs, dv), F32), V((heads, seqs, dv), F32),
            V((width, 2 * he), BF), V((nx, he, qc), BF), V((nx, he, qc), BF),
            V((nx * ch, seqs, LANES), BF), V((nx, wide, LANES), BF),
            V((EP, msg, LANES), BF), V((nx, EP, msg, LANES), BF), V((nx, EP * msg // 2, LANES), F32),
            V((2, nx, EP * SLOTS // 2, he), BF), V((EP * msg // 2, LANES), F32),
            V((EP, msg, LANES), BF), V((EP, msg, LANES), BF),
            V((nx, wide, LANES), BF), V((nx, wide, LANES), BF), V((nx, wide, LANES), BF),
            dma((18,)), dma((4,)), dma((4,)), dma((4,)), dma((4,)), dma((2,)), dma((5,)),
            dma((2,)), dma((2,)), *[dma] * 30,
        ],
        compiler_params=pltpu.CompilerParams(
            collective_id=1, has_side_effects=True, vmem_limit_bytes=LAYER_VMEM
        ),
        name="layer",
    )(
        *(
            pltpu.with_memory_space_constraint(a, pltpu.HBM)
            for a in (
                tokens, norm_gain, wq, wk, wv, wg, bw.T, dw.T, rate, bias, head_gain, rec, ow.T, ffn_gain,
                routes.T, rweight.T, eg, eu, ed, sg, su, sd.T, branch_gate,
            )
        )
    )


def store_kernel(layer_in, state, layer_out, new, sems):
    n = state.shape[0] // STATE_COPIES
    copies = [
        pltpu.make_async_copy(
            state.at[pl.ds(i * n, n)], new.at[pl.ds(i * n, n)], sems.at[i]
        )
        for i in range(STATE_COPIES)
    ]
    copies.append(pltpu.make_async_copy(layer_in, layer_out, sems.at[STATE_COPIES]))
    for cp in copies:
        cp.start()
    for cp in copies:
        cp.wait()


def per_device(*args):
    layer_out, state = layer(*args)
    hbm = pl.BlockSpec(memory_space=pltpu.HBM)
    vmem = pl.BlockSpec(memory_space=pltpu.VMEM)
    return pl.pallas_call(
        store_kernel,
        out_shape=(
            jax.ShapeDtypeStruct(layer_out.shape, BF),
            jax.ShapeDtypeStruct(state.shape, F32),
        ),
        in_specs=[vmem, vmem],
        out_specs=(hbm, hbm),
        scratch_shapes=[pltpu.SemaphoreType.DMA((STATE_COPIES + 1,))],
        compiler_params=pltpu.CompilerParams(vmem_limit_bytes=8 * 1024 * 1024),
        name="store",
    )(layer_out, pltpu.with_memory_space_constraint(state, pltpu.VMEM))


def solution(mesh):
    return jax.shard_map(
        per_device,
        mesh=mesh,
        in_specs=(
            P("ep", None),
            P(),
            P("ep", "tp"),
            P("ep", "tp"),
            P("ep", "tp"),
            P("ep", "tp"),
            P(),
            P(),
            P("tp"),
            P("tp"),
            P(),
            P("ep", "tp", None, None),
            P("tp", "ep"),
            P(),
            P("ep", None),
            P("ep", None),
            P("ep", None, "tp"),
            P("ep", None, "tp"),
            P("ep", "tp", None),
            P("ep", "tp"),
            P("ep", "tp"),
            P("tp", "ep"),
            P(),
        ),
        out_specs=(P("ep", None), P("ep", "tp", None, None)),
        check_vma=False,
    )
```

```python
import jax
import jax.numpy as jnp
from jax import lax
from jax.experimental import pallas as pl
from jax.experimental.pallas import tpu as pltpu
from jax.sharding import PartitionSpec as P

EPS = 1e-06
ROUTED_SCALE = 2.5
NZ, NY, NC = 8, 4, 2
YC = NY * NC
EP = NZ * YC
SLOTS = 2
UNROLL = 2
STATE_COPIES = 8
FAR = (4, 3, 5, 2, 6, 1, 7)
NEAR = (1, 7, 2, 6, 3, 5, 4)
GROUPS = ((0,), (1, 7), (2, 6), (3, 5, 4))
PAIRS = ((0,), (7, 1), (6,), (2, 5), (3, 4))
ARRIVAL = tuple(d for g in PAIRS for d in g)
PAIR = {d: i for i, g in enumerate(PAIRS) for d in g}
NEAR_Z = 5
GROUP = {d: i for i, g in enumerate(GROUPS) for d in g}
LAYER_VMEM = 40 * 1024 * 1024
LANES = 128
MESH = pl.DeviceIdType.MESH
BF = jnp.bfloat16
F32 = jnp.float32
I32 = jnp.int32


def silu(v):
    return v / (1.0 + jnp.exp(-v))


def sigmoid(v):
    return 1.0 / (1.0 + jnp.exp(-v))


def rms(values, gain):
    return values * lax.rsqrt(jnp.mean(values * values, axis=-1, keepdims=True) + EPS) * gain


def unit(v):
    return v * lax.rsqrt(jnp.sum(v * v, axis=-1, keepdims=True) + EPS)


def iota(shape, dim):
    return lax.broadcasted_iota(I32, shape, dim)


def nt_dot(a, b):
    return lax.dot_general(a, b, (((1,), (1,)), ((), ())), preferred_element_type=F32)


def layer_kernel(
    tokens_h, norm_gain_h, wq, wk, wv, wg, bw_h, dw_h, rate_h, bias_h, head_gain_h, rec, ow_h, ffn_gain_h,
    routes_h, rweight_h, eg_h, eu_h, ed_h, sg_h, su_h, sd_h, branch_h,
    out_ref, state,
    tokens, norm_gain, bd, rate, bias, head_gain, ffn_gain, routes, rweight, branch_gate,
    wbuf, gbuf, tok_src, tokbuf, psend, prec, gsend, grec, obuf, sbuf, mix_send, mix_rec,
    kqt, vals, rs_ref, ro, corr,
    egu, dsrc, dbuf, tok_chunks, res_all, dsend, xrows, rowsf, act_all, outf, rsend, rrecv, sh_send, sh_rec, fin,
    load_sem, o1_r, o2_r, s1_r, s2_r, o3_r, d_r,
    x_r, a_r, t_r, wf_r, gf_r, p_r, g_r, w_r, gw_r, s3_r, m_r, ed_r, r_r, h_r, f_r, n_r,
    t_s, w_s, gw_s, p_s, g_s, o_s, s_s, m_s, ed_s, d_s, x_s, a_s, r_s, h_s, f_s, n_s,
):
    e = lax.axis_index("ep")
    x = lax.axis_index("tp")
    nx = lax.axis_size("tp")
    z, yc = lax.div(e, YC), lax.rem(e, YC)
    y, c = lax.div(yc, NC), lax.rem(yc, NC)
    partner = e + 1 - 2 * c
    zdev = lambda d: lax.rem(z + d, NZ) * YC + yc
    ydev = lambda d: z * YC + lax.rem(y + d, NY) * NC + c
    xdev = lambda d: lax.rem(x + d, nx)
    peers = sorted(range(1, nx), key=lambda d: -min(d, nx - d))
    ypeers = sorted(range(1, NY), key=lambda d: -min(d, NY - d))
    seqs, width = tokens.shape
    heads, dk, dv = rec.shape[1:]

    def wait_all(ref, sem):
        pltpu.make_async_copy(ref, ref, sem).wait()

    def rcopy(src, dst, ss, rs, ep, tp):
        cp = pltpu.make_async_remote_copy(
            src_ref=src, dst_ref=dst, send_sem=ss, recv_sem=rs, device_id=(ep, tp), device_id_type=MESH
        )
        cp.start()
        return cp

    barrier = pltpu.get_barrier_semaphore()
    zbase = [lax.rem(z + d, NZ) * YC for d in range(NZ)]
    ypart = [lax.rem(yc + d, YC) for d in range(YC)]
    for dz in (4, 3, 5, 2, 6, 1, 7):
        pl.semaphore_signal(barrier, inc=1, device_id=(zbase[dz] + yc, x), device_id_type=MESH)
    for d in range(1, YC):
        pl.semaphore_signal(barrier, inc=1, device_id=(zbase[0] + ypart[d], x), device_id_type=MESH)
    for d in range(1, nx):
        pl.semaphore_signal(barrier, inc=1, device_id=(e, xdev(d)), device_id_type=MESH)

    count = [0]

    def load(*pairs):
        sem = load_sem.at[count[0]]
        count[0] += 1
        for src, dst in pairs:
            pltpu.make_async_copy(src, dst, sem).start()
        return sem

    cuts = [0]
    for w in (wq, wk, wv):
        cuts.append(cuts[-1] + w.shape[1])
    w_load = load(*((w, wbuf.at[yc, :, cuts[i] : cuts[i + 1]]) for i, w in enumerate((wq, wk, wv))))
    first = [(a, load((b, a))) for a, b in ((tokens, tokens_h), (norm_gain, norm_gain_h))]
    g_load = load((wg, gbuf.at[yc]))
    o_load = load((ow_h, obuf.at[e]))
    qc = width // nx
    ed_load = load(*((ed_h.at[0, :, q * qc : (q + 1) * qc], dsrc.at[q]) for q in range(nx)))
    small = [
        (b, load((a, b)))
        for a, b in (
            (rate_h, rate), (bias_h, bias), (head_gain_h, head_gain),
            (ffn_gain_h, ffn_gain), (routes_h, routes), (rweight_h, rweight), (branch_h, branch_gate),
        )
    ]
    bd_load = load((bw_h, bd.at[0]), (dw_h, bd.at[1]))
    hs = sg_h.shape[1]
    s_load = load(
        *((a, sbuf.at[e, :, i * hs : (i + 1) * hs]) for i, a in enumerate((sg_h, su_h, sd_h)))
    )
    state_load = load((rec, state))
    he = eg_h.shape[2]
    e_load = load((eg_h.at[0], egu.at[:, 0:he]), (eu_h.at[0], egu.at[:, he : 2 * he]))

    def rows_y(buf, ss, rs, fr):
        for d in ypeers:
            rcopy(buf.at[yc], buf.at[yc], ss, rs, ydev(d), x)
        rcopy(buf.at[yc], buf.at[yc], ss, fr, partner, x)

    def rows_c(buf, ss, rs, fr):
        wait_all(buf.at[pl.ds(0, NY - 1)], rs)
        for d in range(1, NY):
            j = lax.rem(y + NY - d, NY) * NC + c
            rcopy(buf.at[j], buf.at[j], ss, fr, partner, x)

    wait_all(wbuf.at[yc], w_load)
    pl.semaphore_wait(barrier, (NZ - 1) + (YC - 1) + (nx - 1))
    rows_y(wbuf, w_s, w_r, wf_r)
    for ref, sem in first:
        wait_all(ref, sem)
    normed = rms(tokens[...].astype(F32), norm_gain[...].reshape(1, width).astype(F32)).astype(BF)
    kz = tokbuf.shape[2]
    for i in range(NZ):
        tok_src[i] = normed[:, i * kz : (i + 1) * kz]
    for d in FAR:
        rcopy(tok_src.at[lax.rem(z + d, NZ)], tokbuf.at[d], t_s, t_r, zdev(d), x)
    wait_all(gbuf.at[yc], g_load)
    rows_y(gbuf, gw_s, gw_r, gf_r)
    wait_all(obuf.at[e], o_load)
    wait_all(dsrc, ed_load)

    def spread_z(buf, ss, rs):
        for d in NEAR:
            rcopy(buf.at[e], buf.at[e], ss, rs.at[GROUP[d]], zdev(d), x)

    def z_blocks(which):
        return [lax.rem(z + NZ - d, NZ) * YC for d in which]

    def spread_y(buf, group, ss, rs, fr):
        for zb in z_blocks(GROUPS[group]):
            j = zb + yc
            for dy in ypeers:
                rcopy(buf.at[j], buf.at[j], ss, rs.at[group], ydev(dy), x)
            rcopy(buf.at[j], buf.at[j], ss, fr(group), partner, x)

    def spread_c(buf, group, ss, rs, fr):
        wait_all(buf.at[pl.ds(0, len(GROUPS[group]) * (NY - 1))], rs.at[group])
        for zb in z_blocks(GROUPS[group]):
            for dy in range(1, NY):
                j = zb + lax.rem(y + NY - dy, NY) * NC + c
                rcopy(buf.at[j], buf.at[j], ss, fr(group), partner, x)

    last_o = lambda group: o3_r.at[1 if group == 3 else 0]
    last_s = lambda group: s3_r
    spread_z(obuf, o_s, o1_r)
    spread_y(obuf, 0, o_s, o2_r, last_o)
    for d in peers:
        rcopy(dsrc.at[xdev(d)], dbuf.at[d], ed_s, ed_r, e, xdev(d))
    tokbuf[0] = tok_src[z]

    for ref, sem in small:
        wait_all(ref, sem)
    wait_all(bd, bd_load)
    bl = nt_dot(normed, bd[0])
    dl = nt_dot(normed, bd[1])
    lanes = iota(bl.shape, 1)
    retain, strength = [], []
    for h in range(heads):
        mine = lanes == x * heads + h
        b = jnp.sum(jnp.where(mine, bl, 0.0), axis=1, keepdims=True)
        g = jnp.sum(jnp.where(mine, dl, 0.0), axis=1, keepdims=True) + bias[h]
        soft = jnp.maximum(g, 0.0) + jnp.log1p(jnp.exp(-jnp.abs(g)))
        strength.append(sigmoid(b))
        retain.append(jnp.exp(-rate[h] * soft))
    lane = iota(rs_ref.shape, 1)
    packed = jnp.zeros(rs_ref.shape, F32)
    for h in range(heads):
        packed = jnp.where(lane == h, retain[h], packed)
        packed = jnp.where(lane == heads + h, strength[h], packed)

    rows_c(wbuf, w_s, w_r, wf_r)
    wait_all(obuf.at[pl.ds(0, len(GROUPS[1]))], o1_r.at[1])
    spread_y(obuf, 1, o_s, o2_r, last_o)
    wait_all(tokbuf.at[pl.ds(1, NZ - 1)], t_r)
    wait_all(wbuf.at[pl.ds(0, NY)], wf_r)
    toks_all = tokbuf[...].reshape(NZ * seqs, kz)

    def project(buf, sent, got, ss, rs):
        n = buf.shape[2]
        sent[...] = (
            jnp.dot(toks_all, buf[...].reshape(kz, n), preferred_element_type=F32)
            .astype(BF)
            .reshape(NZ, seqs, n)
        )
        for d in FAR:
            rcopy(sent.at[d], got.at[d], ss, rs, zdev(NZ - d), x)

    def collected(sent, got, rs):
        wait_all(got.at[pl.ds(1, NZ - 1)], rs)
        total = sent[0].astype(F32)
        for d in range(1, NZ):
            total = total + got[d].astype(F32)
        return total.astype(BF).astype(F32)

    project(wbuf, psend, prec, p_s, p_r)
    rows_c(gbuf, gw_s, gw_r, gf_r)
    wait_all(obuf.at[pl.ds(0, len(GROUPS[2]))], o1_r.at[2])
    spread_y(obuf, 2, o_s, o2_r, last_o)
    wait_all(gbuf.at[pl.ds(0, NY)], gf_r)
    project(gbuf, gsend, grec, g_s, g_r)
    wait_all(obuf.at[pl.ds(0, len(GROUPS[3]))], o1_r.at[3])
    spread_y(obuf, 3, o_s, o2_r, last_o)
    wait_all(sbuf.at[e], s_load)
    spread_z(sbuf, s_s, s1_r)

    def s_relay(group):
        if group:
            wait_all(sbuf.at[pl.ds(0, len(GROUPS[group]))], s1_r.at[group])
        spread_y(sbuf, group, s_s, s2_r, last_s)


    ch = qc // LANES
    for i in range(nx * ch):
        tok_chunks[i] = tokens[:, i * LANES : (i + 1) * LANES]
    topk = routes.shape[0]
    rrow = [routes[k : k + 1, :] for k in range(topk)]
    square = (seqs, seqs)
    diag = iota(square, 0) == iota(square, 1)
    upright = lambda row, zero: jnp.sum(
        jnp.where(diag, jnp.broadcast_to(row, square), zero), axis=1, keepdims=True
    )
    rcol = [upright(r.astype(F32), 0.0) for r in rrow]
    rrow = [r.astype(F32) for r in rrow]
    before_c = iota(square, 1) < iota(square, 0)
    before_r = iota(square, 0) < iota(square, 1)
    tcol, trow = [], []
    for k in range(topk):
        hits_c = jnp.zeros(square, F32)
        hits_r = jnp.zeros(square, F32)
        for k2 in range(topk):
            hits_c += jnp.where(before_c & (rcol[k] == rrow[k2]), 1.0, 0.0)
            hits_r += jnp.where(before_r & (rrow[k] == rcol[k2]), 1.0, 0.0)
        tcol.append(rcol[k] * SLOTS + jnp.sum(hits_c, axis=1, keepdims=True))
        trow.append(rrow[k] * SLOTS + jnp.sum(hits_r, axis=0, keepdims=True))
    wide = ch * seqs
    spreadm = (iota((seqs, wide), 1) % seqs == iota((seqs, wide), 0)).astype(BF)
    rows_all = EP * SLOTS * ch
    rid = iota((rows_all, wide), 0)
    okc = rid % ch == iota((rows_all, wide), 1) // seqs
    ridf = (rid // ch).astype(F32)
    place = jnp.zeros((rows_all, wide), F32)
    for k in range(topk):
        tw = jnp.dot(
            jnp.broadcast_to(trow[k], (8, seqs)).astype(BF), spreadm, preferred_element_type=F32
        )[0:1, :]
        place = jnp.where(okc & (ridf == tw), 1.0, place)
    place = place.astype(BF)
    rw = [rweight[k : k + 1, :] for k in range(topk)]
    rsum = rw[0]
    for k in range(1, topk):
        rsum = rsum + rw[k]
    scol = [upright(rw[k] / rsum * ROUTED_SCALE, 0.0) for k in range(topk)]
    pick_col = jnp.concatenate([tcol[k] * ch + cc for k in range(topk) for cc in range(ch)], axis=0)
    scale_col = jnp.concatenate([scol[k] for k in range(topk) for cc in range(ch)], axis=0)
    pick = (
        jnp.broadcast_to(pick_col, (topk * wide, rows_all))
        == iota((topk * wide, rows_all), 1).astype(F32)
    ).astype(BF)

    proj = collected(psend, prec, p_r)
    for group in range(3):
        spread_c(obuf, group, o_s, o2_r, last_o)
    khs = wq.shape[1] // dk
    per = heads // khs
    kq = []

    def split(i, t):
        hi = t.astype(BF)
        mid = (t - hi.astype(F32)).astype(BF)
        lo = (t - hi.astype(F32) - mid.astype(F32)).astype(BF)
        kqt[i * dk : (i + 1) * dk, :] = jnp.concatenate([hi, mid, lo], axis=1)

    for i in range(khs):
        q = unit(silu(proj[:, i * dk : (i + 1) * dk])) * dk ** (-0.5)
        k = unit(silu(proj[:, (khs + i) * dk : (khs + i + 1) * dk]))
        split(i, k.T)
        split(khs + i, q.T)
        kq.append(jnp.sum(k * q, axis=1, keepdims=True))
    for i in range(khs):
        packed = jnp.where(lane == 2 * heads + i, kq[i], packed)
    rs_ref[...] = packed
    vbase = 2 * khs * dk
    for h in range(heads):
        vals[h] = silu(proj[:, vbase + h * dv : vbase + (h + 1) * dv])
    wait_all(state, state_load)

    span = 2 * dv

    def spread_columns(first, rows):
        shape = (kqt.shape[1], span)
        hot = (lax.rem(iota(shape, 0), seqs) == first + iota(shape, 1) // dv).astype(BF)
        return jnp.dot(kqt[0:rows, :], hot, preferred_element_type=F32)

    def read_pair(p, carry):
        both = spread_columns(2 * p, 2 * khs * dk)
        for j in range(2):
            s = 2 * p + j
            wide_cols = both[:, j * dv : (j + 1) * dv]
            rowrs = rs_ref[pl.ds(s, 1), :]
            for i in range(khs):
                kcol = wide_cols[i * dk : (i + 1) * dk]
                qcol = wide_cols[(khs + i) * dk : (khs + i + 1) * dk]
                dotkq = rowrs[:, 2 * heads + i : 2 * heads + i + 1]
                for h in range(i * per, (i + 1) * per):
                    st = state[s, h]
                    ret = rowrs[:, h : h + 1]
                    pred = jnp.sum(st * kcol, axis=0, keepdims=True) * ret
                    base = jnp.sum(st * qcol, axis=0, keepdims=True) * ret
                    cor = rowrs[:, heads + h : heads + h + 1] * (vals[h, pl.ds(s, 1), :] - pred)
                    corr[h, pl.ds(s, 1), :] = cor
                    ro[h, pl.ds(s, 1), :] = base + dotkq * cor
        return carry

    lax.fori_loop(0, seqs // 2, read_pair, 0, unroll=UNROLL)

    spread_c(obuf, 3, o_s, o2_r, last_o)
    gate = collected(gsend, grec, g_r)
    hg = head_gain[...].reshape(1, dv).astype(F32)
    parts = [rms(ro[h], hg) * silu(gate[:, h * dv : (h + 1) * dv]) for h in range(heads)]
    heads_out = jnp.concatenate(parts, axis=1).astype(BF)
    def project_out(which):
        for zb in z_blocks(which):
            zi = lax.div(zb, YC)
            mix_send[zi] = nt_dot(
                heads_out, obuf[pl.ds(zb, YC)].reshape(YC * obuf.shape[1], heads * dv)
            ).astype(BF)

    wait_all(obuf.at[pl.ds(0, NEAR_Z * NY)], o3_r.at[0])
    project_out([d for g in GROUPS[:3] for d in g])
    wait_all(obuf.at[pl.ds(0, (NZ - NEAR_Z) * NY)], o3_r.at[1])
    project_out(GROUPS[3])
    zq = NZ // nx
    for d in peers:
        q = xdev(d)
        rcopy(mix_send.at[pl.ds(q * zq, zq)], mix_rec.at[d], m_s, m_r, e, q)
    def write_pair(p, carry):
        both = spread_columns(2 * p, khs * dk)
        for j in range(2):
            s = 2 * p + j
            rowrs = rs_ref[pl.ds(s, 1), :]
            for i in range(khs):
                kcol = both[i * dk : (i + 1) * dk, j * dv : (j + 1) * dv]
                for h in range(i * per, (i + 1) * per):
                    state[s, h] = state[s, h] * rowrs[:, h : h + 1] + kcol * corr[h, pl.ds(s, 1), :]
        return carry

    lax.fori_loop(0, seqs // 2, write_pair, 0, unroll=UNROLL)
    s_relay(0)
    s_relay(1)
    wait_all(mix_rec.at[pl.ds(1, nx - 1)], m_r)
    mixed = mix_send[pl.ds(x * zq, zq)].astype(F32)
    for d in range(1, nx):
        mixed = mixed + mix_rec[d].astype(F32)
    mixed = jnp.concatenate([mixed[i] for i in range(zq)], axis=1)
    own = tok_chunks[pl.ds(x * ch, ch)].astype(F32)
    mine = jnp.concatenate(
        [own[cc] + mixed[:, cc * LANES : (cc + 1) * LANES] for cc in range(ch)], axis=0
    ).astype(BF)
    res_all[x] = mine
    msg = SLOTS * ch
    dsend[...] = (
        jnp.dot(place, mine, preferred_element_type=F32).astype(BF).reshape(EP, msg, LANES)
    )

    zback = [lax.rem(z + NZ - d, NZ) * YC for d in range(NZ)]
    yback = [lax.rem(yc + YC - d, YC) for d in range(YC)]
    place_of = {dz: i * YC for i, dz in enumerate(ARRIVAL)}
    half = EP // 2
    part_of = lambda dz: place_of[dz] // half
    for dz in ARRIVAL:
        for d in range(YC):
            if dz or d:
                to = zbase[dz] + ypart[d]
                rcopy(dsend.at[to], xrows.at[x, place_of[dz] + d], d_s, d_r.at[PAIR[dz]], to, x)
    xrows[x, 0] = dsend[e]
    for d in peers:
        rcopy(res_all.at[x], res_all.at[x], n_s, n_r, e, xdev(d))
    for i, group in enumerate(PAIRS):
        n = len(group) * YC - (0 in group)
        at = pl.ds(place_of[group[0]], len(group) * YC)
        wait_all(xrows.at[x, pl.ds(place_of[group[0]], n)], d_r.at[i])
        for d in peers:
            block = xrows.at[x, at]
            rcopy(block, block, x_s, x_r.at[part_of(group[0])], e, xdev(d))
    s_relay(2)
    s_relay(3)
    for group in (0, 1):
        spread_c(sbuf, group, s_s, s2_r, last_s)
    wait_all(egu, e_load)
    fgain = ffn_gain[...].reshape(1, width).astype(F32)
    nrows = half * SLOTS

    def full_rows():
        wait_all(res_all.at[pl.ds(0, nx - 1)], n_r)
        residual = jnp.concatenate(
            [res_all[i // ch, (i % ch) * seqs : (i % ch + 1) * seqs, :] for i in range(nx * ch)], axis=1
        ).astype(F32)
        ffn_in = rms(residual, fgain).astype(BF)
        branch = sigmoid(
            jnp.sum(
                ffn_in.astype(F32) * branch_gate[...].reshape(1, width).astype(F32), axis=1, keepdims=True
            )
        )
        return ffn_in, branch

    for p in range(2):
        wait_all(xrows.at[pl.ds(1, nx - 1), pl.ds(p * half, half)], x_r.at[p])
        for q in range(nx):
            rowsf[q] = xrows[q, p * half : (p + 1) * half].reshape(half * msg, LANES).astype(F32)
        squares = jnp.zeros((nrows, LANES), F32)
        gu = jnp.zeros((nrows, 2 * he), F32)
        for q in range(nx):
            pieces = [rowsf[q, pl.ds(cc, nrows, stride=ch), :] for cc in range(ch)]
            for v in pieces:
                squares = squares + v * v
            left = (jnp.concatenate(pieces, axis=1) * fgain[:, q * qc : (q + 1) * qc]).astype(BF)
            gu = gu + jnp.dot(left, egu[q * qc : (q + 1) * qc, :], preferred_element_type=F32)
        gu = gu * lax.rsqrt(jnp.sum(squares, axis=1, keepdims=True) / width + EPS)
        act_all[p, 0] = (silu(gu[:, 0:he]) * gu[:, he:]).astype(BF)
        for d in peers:
            rcopy(act_all.at[p, 0], act_all.at[p, d], a_s, a_r.at[p], e, xdev(d))

    wait_all(dbuf.at[pl.ds(1, nx - 1)], ed_r)
    for p in range(2):
        if p == 1:
            spread_c(sbuf, 2, s_s, s2_r, last_s)
            ffn_in, branch = full_rows()
        eout = jnp.dot(act_all[p, 0], dsrc[x], preferred_element_type=F32)
        wait_all(act_all.at[p, pl.ds(1, nx - 1)], a_r.at[p])
        for d in range(1, nx):
            eout = eout + jnp.dot(act_all[p, d], dbuf[d], preferred_element_type=F32)
        for cc in range(ch):
            outf[pl.ds(cc, nrows, stride=ch), :] = eout[:, cc * LANES : (cc + 1) * LANES]
        rsend[p * half : (p + 1) * half] = outf[...].astype(BF).reshape(half, msg, LANES)
        for dz in ARRIVAL[::-1]:
            for d in range(YC):
                if part_of(dz) == p and (dz or d):
                    rcopy(rsend.at[place_of[dz] + d], rrecv.at[e], r_s, r_r, zback[dz] + yback[d], x)
    rrecv[e] = rsend[0]
    spread_c(sbuf, 3, s_s, s2_r, last_s)
    wait_all(sbuf.at[pl.ds(0, EP // NC)], s3_r)
    sgu = jnp.dot(ffn_in, sbuf[:, :, 0 : 2 * hs].reshape(width, 2 * hs), preferred_element_type=F32)
    sact = (silu(sgu[:, 0:hs]) * sgu[:, hs:]).astype(BF)
    spart = nt_dot(sact, sbuf[:, :, 2 * hs :].reshape(width, hs)).astype(BF)
    for i in range(nx * ch):
        sh_send[i // ch, (i % ch) * seqs : (i % ch + 1) * seqs, :] = spart[:, i * LANES : (i + 1) * LANES]
    for d in peers:
        rcopy(sh_send.at[xdev(d)], sh_rec.at[d], h_s, h_r, e, xdev(d))
    shared = sh_send[x].astype(F32)
    wait_all(sh_rec.at[pl.ds(1, nx - 1)], h_r)
    for d in range(1, nx):
        shared = shared + sh_rec[d].astype(F32)
    base = mine.astype(F32)
    base = base + jnp.concatenate([branch] * ch, axis=0) * shared
    wait_all(rrecv.at[pl.ds(0, EP - 1)], r_r)
    got = jnp.dot(pick, rrecv[...].reshape(rows_all, LANES), preferred_element_type=F32) * scale_col
    for k in range(topk):
        base = base + got[k * wide : (k + 1) * wide]
    fin[x] = base.astype(BF)
    for d in peers:
        rcopy(fin.at[x], fin.at[x], f_s, f_r, e, xdev(d))
    wait_all(fin.at[pl.ds(0, nx - 1)], f_r)
    for i in range(nx * ch):
        out_ref[:, i * LANES : (i + 1) * LANES] = fin[i // ch, (i % ch) * seqs : (i % ch + 1) * seqs, :]

    some = lambda ref, n: ref.at[pl.ds(0, n)]
    for ref, sem in (
        (some(tokbuf, NZ - 1), t_s), (some(wbuf, 2 * NY - 1), w_s), (some(gbuf, 2 * NY - 1), gw_s),
        (some(psend, NZ - 1), p_s), (some(gsend, NZ - 1), g_s), (some(obuf, EP - 1), o_s),
        (some(sbuf, EP - 1), s_s), (some(mix_rec, nx - 1), m_s), (some(dsrc, nx - 1), ed_s),
        (some(dsend, EP - 1), d_s), (some(xrows, nx - 1), x_s), (act_all.at[:, pl.ds(1, nx - 1)], a_s),
        (some(rsend, EP - 1), r_s), (some(sh_send, nx - 1), h_s), (some(fin, nx - 1), f_s), (some(res_all, nx - 1), n_s),
    ):
        wait_all(ref, sem)


def layer(*args):
    (tokens, norm_gain, wq, wk, wv, wg, bw, dw, rate, bias, head_gain, rec, ow, ffn_gain, routes, rweight,
     eg, eu, ed, sg, su, sd, branch_gate) = args
    nx = lax.axis_size("tp")
    seqs, width = tokens.shape
    heads, dk, dv = rec.shape[1:]
    cols = wq.shape[1] + wk.shape[1] + wv.shape[1] + wg.shape[1]
    rows = wq.shape[0]
    kz = rows * YC
    khs = wq.shape[1] // dk
    topk = routes.shape[1]
    qc = width // nx
    ch = qc // LANES
    he = eg.shape[2]
    hs = sg.shape[1]
    msg = SLOTS * ch
    wide = ch * seqs
    hbm = pl.BlockSpec(memory_space=pltpu.HBM)
    vmem = pl.BlockSpec(memory_space=pltpu.VMEM)
    dma = pltpu.SemaphoreType.DMA
    V = pltpu.VMEM
    return pl.pallas_call(
        layer_kernel,
        out_shape=(
            jax.ShapeDtypeStruct((seqs, width), BF),
            pltpu.VMEM(rec.shape, F32),
        ),
        in_specs=[hbm] * 23,
        out_specs=(vmem,) * 2,
        scratch_shapes=[
            V((seqs, width), BF), V((width,), BF), V((2, *bw.shape[::-1]), BF),
            pltpu.SMEM((heads,), F32), pltpu.SMEM((heads,), F32), V((dv,), BF), V((width,), BF),
            V((topk, seqs), I32), V((topk, seqs), F32), V((width,), BF),
            V((YC, rows, cols - wg.shape[1]), BF), V((YC, rows, wg.shape[1]), BF), V((NZ, seqs, kz), BF), V((NZ, seqs, kz), BF),
            V((NZ, seqs, cols - wg.shape[1]), BF), V((NZ, seqs, cols - wg.shape[1]), BF),
            V((NZ, seqs, wg.shape[1]), BF), V((NZ, seqs, wg.shape[1]), BF),
            V((EP, ow.shape[1], ow.shape[0]), BF), V((EP, sg.shape[0], 3 * hs), BF),
            V((NZ, seqs, width // NZ), BF), V((nx, NZ // nx, seqs, width // NZ), BF),
            V((2 * khs * dk, 3 * seqs), BF), V((heads, seqs, dv), F32),
            V((seqs, LANES), F32), V((heads, seqs, dv), F32), V((heads, seqs, dv), F32),
            V((width, 2 * he), BF), V((nx, he, qc), BF), V((nx, he, qc), BF),
            V((nx * ch, seqs, LANES), BF), V((nx, wide, LANES), BF),
            V((EP, msg, LANES), BF), V((nx, EP, msg, LANES), BF), V((nx, EP * msg // 2, LANES), F32),
            V((2, nx, EP * SLOTS // 2, he), BF), V((EP * msg // 2, LANES), F32),
            V((EP, msg, LANES), BF), V((EP, msg, LANES), BF),
            V((nx, wide, LANES), BF), V((nx, wide, LANES), BF), V((nx, wide, LANES), BF),
            dma((17,)), dma((4,)), dma((4,)), dma((4,)), dma((4,)), dma((2,)), dma((5,)),
            dma((2,)), dma((2,)), *[dma] * 30,
        ],
        compiler_params=pltpu.CompilerParams(
            collective_id=1, has_side_effects=True, vmem_limit_bytes=LAYER_VMEM
        ),
        name="layer",
    )(
        *(
            pltpu.with_memory_space_constraint(a, pltpu.HBM)
            for a in (
                tokens, norm_gain, wq, wk, wv, wg, bw.T, dw.T, rate, bias, head_gain, rec, ow.T, ffn_gain,
                routes.T, rweight.T, eg, eu, ed, sg, su, sd.T, branch_gate,
            )
        )
    )


def store_kernel(layer_in, state, layer_out, new, sems):
    n = state.shape[0] // STATE_COPIES
    copies = [
        pltpu.make_async_copy(
            state.at[pl.ds(i * n, n)], new.at[pl.ds(i * n, n)], sems.at[i]
        )
        for i in range(STATE_COPIES)
    ]
    copies.append(pltpu.make_async_copy(layer_in, layer_out, sems.at[STATE_COPIES]))
    for cp in copies:
        cp.start()
    for cp in copies:
        cp.wait()


def per_device(*args):
    layer_out, state = layer(*args)
    hbm = pl.BlockSpec(memory_space=pltpu.HBM)
    vmem = pl.BlockSpec(memory_space=pltpu.VMEM)
    return pl.pallas_call(
        store_kernel,
        out_shape=(
            jax.ShapeDtypeStruct(layer_out.shape, BF),
            jax.ShapeDtypeStruct(state.shape, F32),
        ),
        in_specs=[vmem, vmem],
        out_specs=(hbm, hbm),
        scratch_shapes=[pltpu.SemaphoreType.DMA((STATE_COPIES + 1,))],
        compiler_params=pltpu.CompilerParams(vmem_limit_bytes=8 * 1024 * 1024),
        name="store",
    )(layer_out, pltpu.with_memory_space_constraint(state, pltpu.VMEM))


def solution(mesh):
    return jax.shard_map(
        per_device,
        mesh=mesh,
        in_specs=(
            P("ep", None),
            P(),
            P("ep", "tp"),
            P("ep", "tp"),
            P("ep", "tp"),
            P("ep", "tp"),
            P(),
            P(),
            P("tp"),
            P("tp"),
            P(),
            P("ep", "tp", None, None),
            P("tp", "ep"),
            P(),
            P("ep", None),
            P("ep", None),
            P("ep", None, "tp"),
            P("ep", None, "tp"),
            P("ep", "tp", None),
            P("ep", "tp"),
            P("ep", "tp"),
            P("tp", "ep"),
            P(),
        ),
        out_specs=(P("ep", None), P("ep", "tp", None, None)),
        check_vma=False,
    )
```
